32 devices in a mesh: sp: 16 (over z, y, x), tp: 2 (over core).
Axes of the slice: x: 2, y: 2, z: 4, core: 2. Of those that a mesh axis runs over, the one named last changes fastest.
Arguments:
- resid: bfloat16 [3072, 2048], P('sp'), may hold values from -6 to 6
- query: bfloat16 [3072, 2048], P('sp', 'tp'), may hold values from -6 to 6
- key: bfloat16 [3072, 1024], P('sp', 'tp'), may hold values from -6 to 6
- value: bfloat16 [3072, 1024], P('sp', 'tp'), may hold values from -6 to 6
- q_gain: float32 [128], replicated, may hold values from 0.3 to 5, as said below
- k_gain: float32 [128], replicated, may hold values from 0.3 to 5, as said below
- out_weight: bfloat16 [2048, 2048], P('tp'), may hold values from -0.125 to 0.125
- norm_gain: float32 [2048], replicated, may hold values from 0.1 to 1.9
- gate_weight: bfloat16 [2048, 5632], P('sp', 'tp'), may hold values from -0.125 to 0.125
- up_weight: bfloat16 [2048, 5632], P('sp', 'tp'), may hold values from -0.125 to 0.125
- down_weight: bfloat16 [5632, 2048], P('tp', 'sp'), may hold values from -0.078125 to 0.078125
Outputs:
- mixed: bfloat16 [3072, 2048], P(('sp', 'tp'))
The draws below stay inside these ranges and needn't reach their ends.
Inputs may be any that keep to these rules, and one draw needn't show every extreme that they name: `q_gain`: positive gains. `k_gain`: positive gains.
All inputs are finite; a program needn't handle non-finite values.
Results may differ from the reference program's by a relative error of at most 0.012.
The reference program's roundings to bfloat16 on the way count: a program that leaves them out, or rounds other values in their place, can miss the bound.
Values may be sent and summed in bfloat16 or wider, within the bound.
A program may use at most 128 MiB of HBM per device.

```python
import jax
import jax.numpy as jnp
from jax import lax

D = 2048
HEADS = 16
KV_HEADS = 8
HEAD_DIM = 128
FF = 5632
GRID_W = 64
TOK_DEV = 192
TOKENS = 3072
N_TP = 2


def paired_draw(key):
    base = jax.random.fold_in(key, 11)
    key_rows = jnp.clip(jax.random.normal(jax.random.fold_in(base, 1), (TOKENS, KV_HEADS * HEAD_DIM), jnp.float32), -6.0, 6.0)
    query_rows = jnp.clip(jax.random.normal(jax.random.fold_in(base, 2), (TOKENS, HEADS * HEAD_DIM), jnp.float32), -6.0, 6.0)
    return (query_rows, key_rows)


def draw_query(key, part):
    return paired_draw(key)[0].astype(jnp.bfloat16)


def draw_key(key, part):
    return paired_draw(key)[1].astype(jnp.bfloat16)


def gain_draw(key, salt):
    base = jax.random.fold_in(key, salt)
    return jnp.exp(jax.random.uniform(base, (HEAD_DIM,), jnp.float32, jnp.log(0.6), jnp.log(3.0)))


def draw_q_gain(key, part):
    return gain_draw(key, 21)


def draw_k_gain(key, part):
    return gain_draw(key, 22)


def level_of(key, shape, shards, low, high):
    level, own = 1.0, jax.random.fold_in(key, 6)
    for position, shards_of in shards:
        draws = jnp.exp(jax.random.uniform(jax.random.fold_in(own, position), (shards_of,), jnp.float32, low / len(shards), high / len(shards)))
        level = level * jnp.repeat(draws, shape[position] // shards_of).reshape([-1 if axis == position else 1 for axis in range(len(shape))])
    return level


def normal_values(own_key, extent, deviation, reach, shards=(), kind=jnp.bfloat16):
    entries = deviation * jax.random.normal(own_key, extent, jnp.float32)
    if shards:
        entries = entries * level_of(own_key, extent, shards, -0.22, 0.18)
    return jnp.clip(entries, -reach, reach).astype(kind)


def setup_inputs(seed: int = 0) -> dict:
    splits = jax.random.split(jax.random.key(seed), 12)
    return {
        "resid": normal_values(splits[0], (TOKENS, D), 1.0, 6.0, ((0, 16),)),
        "query": draw_query(jax.random.fold_in(splits[11], 71), 0),
        "key": draw_key(jax.random.fold_in(splits[11], 71), 0),
        "value": normal_values(splits[3], (TOKENS, KV_HEADS * HEAD_DIM), 1.0, 6.0, ((0, 16), (1, 2))),
        "q_gain": draw_q_gain(jax.random.fold_in(splits[11], 71), 0),
        "k_gain": draw_k_gain(jax.random.fold_in(splits[11], 71), 0),
        "out_weight": normal_values(splits[6], (HEADS * HEAD_DIM, D), (HEADS * HEAD_DIM) ** -0.5, 0.125, ((0, 2),)),
        "norm_gain": jnp.clip(1.0 + 0.18 * jax.random.normal(splits[7], (D,), jnp.float32), 0.1, 1.9),
        "gate_weight": normal_values(splits[8], (D, FF), D ** -0.5, 0.125, ((0, 16), (1, 2))),
        "up_weight": normal_values(splits[9], (D, FF), D ** -0.5, 0.125, ((0, 16), (1, 2))),
        "down_weight": normal_values(splits[10], (FF, D), FF ** -0.5, 0.078125, ((0, 2), (1, 16))),
    }


EPSILON = 1e-06

def rounded(values):
    return lax.optimization_barrier(values.astype(jnp.bfloat16)).astype(jnp.float32)

def rotate(values, positions):
    dim_size = values.shape[-1]
    half_dim = dim_size // 2
    quarter = half_dim // 2
    inverse = 10000.0 ** (-jnp.arange(quarter, dtype=jnp.float32) / quarter)
    outputs = []
    for axis_pos, coords in enumerate((positions // GRID_W, positions % GRID_W)):
        angles = coords.astype(jnp.float32)[:, None] * inverse[None, :]
        cosine = jnp.cos(angles)[:, None, :]
        sine = jnp.sin(angles)[:, None, :]
        section = values[..., axis_pos * half_dim:(axis_pos + 1) * half_dim]
        first_half = section[..., :quarter]
        second_half = section[..., quarter:]
        outputs += [first_half * cosine - second_half * sine, second_half * cosine + first_half * sine]
    return jnp.concatenate(outputs, axis=-1)

def prepare(projected, gain, positions):
    values = projected.astype(jnp.float32)
    normed = values * lax.rsqrt(lax.optimization_barrier(jnp.mean(values * values, axis=-1, keepdims=True)) + EPSILON) * gain
    return rotate(normed, positions).astype(jnp.bfloat16)

def normalize(stream, gain):
    values = stream.astype(jnp.float32)
    return (values * lax.rsqrt(lax.optimization_barrier(jnp.mean(values * values, axis=-1, keepdims=True)) + EPSILON) * gain).astype(jnp.bfloat16)

def reference(resid, query, key, value, q_gain, k_gain, out_weight, norm_gain, gate_weight, up_weight, down_weight):
    positions = jnp.arange(TOKENS, dtype=jnp.int32)
    q_rot = prepare(query.reshape(TOKENS, HEADS, HEAD_DIM), q_gain, positions)
    k_rot = prepare(key.reshape(TOKENS, KV_HEADS, HEAD_DIM), k_gain, positions)
    key_float = k_rot.astype(jnp.float32)
    val_float = value.reshape(TOKENS, KV_HEADS, HEAD_DIM).astype(jnp.float32)
    group_size = HEADS // KV_HEADS
    query_blocks = q_rot.reshape(TOKENS // TOK_DEV, TOK_DEV, KV_HEADS, group_size, HEAD_DIM)

    def one_block(block):
        scores = jnp.einsum('qkgd,skd->kgqs', block.astype(jnp.float32), key_float) * HEAD_DIM ** (-0.5)
        maxima = lax.optimization_barrier(jnp.max(scores, axis=-1, keepdims=True))
        weights = jnp.exp(scores - maxima)
        totals = lax.optimization_barrier(jnp.sum(weights, axis=-1))
        summed = jnp.einsum('kgqs,skd->kgqd', rounded(weights), val_float)
        output = summed / totals[..., None]
        return jnp.transpose(output, (2, 0, 1, 3)).reshape(TOK_DEV, HEADS * HEAD_DIM).astype(jnp.bfloat16)
    attn = lax.map(one_block, query_blocks).reshape(TOKENS, HEADS * HEAD_DIM)
    head_width = HEADS * HEAD_DIM // N_TP
    proj = jnp.zeros((TOKENS, D), jnp.float32)
    for index in range(N_TP):
        part_rows = slice(index * head_width, (index + 1) * head_width)
        proj = proj + rounded(jnp.dot(attn[:, part_rows], out_weight[part_rows], preferred_element_type=jnp.float32))
    stream = (resid.astype(jnp.float32) + proj).astype(jnp.bfloat16)
    normed = normalize(stream, norm_gain)
    gate = jnp.dot(normed, gate_weight, preferred_element_type=jnp.float32)
    up_part = jnp.dot(normed, up_weight, preferred_element_type=jnp.float32)
    hidden = (jax.nn.silu(gate) * up_part).astype(jnp.bfloat16)
    unit_width = FF // N_TP
    down = jnp.zeros((TOKENS, D), jnp.float32)
    for index in range(N_TP):
        part_rows = slice(index * unit_width, (index + 1) * unit_width)
        down = down + rounded(jnp.dot(hidden[:, part_rows], down_weight[part_rows], preferred_element_type=jnp.float32))
    return (stream.astype(jnp.float32) + 0.5 * down).astype(jnp.bfloat16)
```

```python
import functools
import math

import jax
import jax.numpy as jnp
import numpy as np
from jax import lax
from jax.experimental import pallas as pl
from jax.experimental.pallas import tpu as pltpu
from jax.sharding import PartitionSpec as P

GRID_W = 64


EPSILON = 1e-06


def rotate(values, positions):
    dim_size = values.shape[-1]
    half_dim = dim_size // 2
    quarter = half_dim // 2
    inverse = 10000.0 ** (-jnp.arange(quarter, dtype=jnp.float32) / quarter)
    outputs = []
    for axis_pos, coords in enumerate((positions // GRID_W, positions % GRID_W)):
        angles = coords.astype(jnp.float32)[:, None] * inverse[None, :]
        cosine = jnp.cos(angles)[:, None, :]
        sine = jnp.sin(angles)[:, None, :]
        section = values[..., axis_pos * half_dim : (axis_pos + 1) * half_dim]
        first_half = section[..., :quarter]
        second_half = section[..., quarter:]
        outputs += [
            first_half * cosine - second_half * sine,
            second_half * cosine + first_half * sine,
        ]
    return jnp.concatenate(outputs, axis=-1)


def prepare(projected, gain, positions):
    values = projected.astype(jnp.float32)
    normed = values * lax.rsqrt(jnp.mean(values * values, axis=-1, keepdims=True) + EPSILON) * gain
    return rotate(normed, positions).astype(jnp.bfloat16)


def normalize(stream, gain):
    values = stream.astype(jnp.float32)
    return (
        values * lax.rsqrt(jnp.mean(values * values, axis=-1, keepdims=True) + EPSILON) * gain
    ).astype(jnp.bfloat16)


def whole_body(
    resid,
    query,
    key,
    value,
    q_gain,
    k_gain,
    out_weight,
    norm_gain,
    gate_weight,
    up_weight,
    down_weight,
):
    rows_here = query.shape[0]
    head_dim = q_gain.shape[0]
    heads_here = query.shape[1] // head_dim
    kv_here = key.shape[1] // head_dim
    group_size = heads_here // kv_here
    score_scale = head_dim ** (-0.5)
    positions = lax.axis_index("sp") * rows_here + jnp.arange(rows_here, dtype=jnp.int32)
    q_rot = prepare(query.reshape(rows_here, heads_here, head_dim), q_gain, positions)
    k_rot = prepare(key.reshape(rows_here, kv_here, head_dim), k_gain, positions)
    val_rows = value.reshape(rows_here, kv_here, head_dim)
    grouped = q_rot.reshape(rows_here, kv_here, group_size, head_dim)

    def key_block(carry, block):
        maxima, totals, accum = carry
        block_keys, block_vals = block
        scores = (
            jnp.einsum("qkgd,skd->kgqs", grouped, block_keys, preferred_element_type=jnp.float32)
            * score_scale
        )
        new_max = jnp.maximum(maxima, jnp.max(scores, axis=-1))
        shrink = jnp.exp(maxima - new_max)
        weights = jnp.exp(scores - new_max[..., None])
        totals = totals * shrink + jnp.sum(weights, axis=-1)
        accum = accum * shrink[..., None] + jnp.einsum(
            "kgqs,skd->kgqd",
            weights.astype(jnp.bfloat16),
            block_vals,
            preferred_element_type=jnp.float32,
        )
        return ((new_max, totals, accum), None)

    start_max = jnp.full((kv_here, group_size, rows_here), -1e30, jnp.float32)
    start_total = jnp.zeros((kv_here, group_size, rows_here), jnp.float32)
    start_accum = jnp.zeros((kv_here, group_size, rows_here, head_dim), jnp.float32)
    carry = (start_max, start_total, start_accum)
    key_part = lax.all_gather(k_rot, "sp", axis=0, tiled=True)
    val_part = lax.all_gather(val_rows, "sp", axis=0, tiled=True)
    length = key_part.shape[0]
    factor = 4
    span = rows_here * factor
    turns = length // span
    key_blocks = key_part.reshape(turns, span, kv_here, head_dim)
    val_blocks = val_part.reshape(turns, span, kv_here, head_dim)
    carry, _ = lax.scan(key_block, carry, (key_blocks, val_blocks))
    maxima, totals, accum = carry
    attn = (
        jnp.transpose(accum / totals[..., None], (2, 0, 1, 3))
        .reshape(rows_here, heads_here * head_dim)
        .astype(jnp.bfloat16)
    )
    share = rows_here // lax.axis_size("tp")
    my_first = lax.axis_index("tp") * share
    proj = lax.psum_scatter(
        jnp.dot(attn, out_weight, preferred_element_type=jnp.float32).astype(jnp.bfloat16),
        "tp",
        scatter_dimension=0,
        tiled=True,
    ).astype(jnp.float32)
    my_resid = lax.dynamic_slice_in_dim(resid, my_first, share, 0)
    my_stream = (my_resid.astype(jnp.float32) + proj).astype(jnp.bfloat16)
    mixer_rows = lax.all_gather(normalize(my_stream, norm_gain), "tp", axis=0, tiled=True)

    def add_rows(shard_rows):
        return jnp.dot(mixer_rows, shard_rows, preferred_element_type=jnp.float32)

    gate = add_rows(lax.all_gather(gate_weight, "sp", axis=0, tiled=True))
    up_part = add_rows(lax.all_gather(up_weight, "sp", axis=0, tiled=True))
    hidden = (jax.nn.silu(gate) * up_part).astype(jnp.bfloat16)
    down_whole = lax.all_gather(down_weight, "sp", axis=1, tiled=True)
    down = lax.psum_scatter(
        jnp.dot(hidden, down_whole, preferred_element_type=jnp.float32).astype(jnp.bfloat16),
        "tp",
        scatter_dimension=0,
        tiled=True,
    ).astype(jnp.float32)
    return (my_stream.astype(jnp.float32) + 0.5 * down).astype(jnp.bfloat16)


SPLIT = 4


def fits(n_sp, kv_here, hidden_here):
    return n_sp % SPLIT == 0 and kv_here % SPLIT == 0 and hidden_here % (64 * SPLIT) == 0


def groups_of(n_sp):
    ranks = n_sp // SPLIT
    tokens = [[part * ranks + rank for part in range(SPLIT)] for rank in range(ranks)]
    hidden = [[part * ranks + rank for rank in range(ranks)] for part in range(SPLIT)]
    return tokens, hidden


MESH = pl.DeviceIdType.MESH


def layer_kernel(
    ranks,
    head_dim,
    key_ref,
    value_ref,
    query_ref,
    k_gain_ref,
    q_gain_ref,
    freq_ref,
    gate_hbm,
    up_hbm,
    down_ref,
    ow_hbm,
    resid_ref,
    gain_ref,
    out_ref,
    kvb,
    qb,
    asend,
    ab,
    wgu,
    wdn,
    pj,
    prv,
    nb,
    st,
    hb,
    dsb,
    drv,
    ds2,
    dzb,
    kv_ref,
    q_ref,
    gu_ref,
    gate_ref,
    up_ref,
    ow_ref,
    local_sem,
    kvp_s, kvp_r, q_s, q_r, qz_s, qz_r, at_r, gz_s, gz_r, dz_s, dz_r, np_s, np_r,
    gx_s, gx_r, dx_s, dx_r, gh_s, gh_r, dh_s, dh_r, dp_s, dp_r,
    kvz_s, kvz_r, fz_s, fz_r,
    nz_s, nz_r, at_s, pj_s, pj_r,
):
    sp = lax.axis_index("sp")
    core = lax.axis_index("tp")
    part = sp // ranks
    rank = sp % ranks
    rows = q_ref.shape[1]
    share = rows // 2
    depth = gu_ref.shape[1]
    width = down_ref.shape[0] // SPLIT
    cols = down_ref.shape[1]
    group = q_ref.shape[2] // head_dim
    other = 1 - core
    flips = (1, 2, 3)
    last = SPLIT - 1

    def flip(e):
        x = rank % 2
        y = rank // 2
        nx = 1 - x if e % 2 else x
        ny = 1 - y if e // 2 else y
        return ny * 2 + nx

    def near(e):
        return part * ranks + flip(e)

    def at_part(target):
        return target * ranks + rank

    def dn_own(index):
        return down_ref.at[pl.ds(pl.multiple_of(index * width, 16), width)]

    barrier = pltpu.get_barrier_semaphore()
    for dz in range(1, SPLIT):
        pl.semaphore_signal(barrier, inc=1, device_id=(at_part((part + dz) % SPLIT), core), device_id_type=MESH)
    for e in flips:
        pl.semaphore_signal(barrier, inc=1, device_id=(near(e), core), device_id_type=MESH)
    pl.semaphore_signal(barrier, inc=1, device_id=(sp, other), device_id_type=MESH)

    loads = [
        pltpu.make_async_copy(gate_hbm, gate_ref, local_sem.at[4]),
        pltpu.make_async_copy(up_hbm, up_ref, local_sem.at[5]),
        pltpu.make_async_copy(ow_hbm, ow_ref, local_sem.at[6]),
    ]
    for copy in loads:
        copy.start()

    lane = lax.broadcasted_iota(jnp.int32, (rows, head_dim), 1)
    spot = sp * rows + lax.broadcasted_iota(jnp.int32, (rows, head_dim), 0)
    grid_bits = GRID_W.bit_length() - 1
    coords = jnp.where(lane < head_dim // 2, spot >> grid_bits, spot & (GRID_W - 1))
    angles = coords.astype(jnp.float32) * freq_ref[...]
    first_half = (lane & (head_dim // 2 - 1)) < head_dim // 4
    cosine = jnp.cos(angles)
    sine = jnp.where(first_half, -jnp.sin(angles), jnp.sin(angles))

    def turn(ref, head, gain):
        x = ref[:, head * head_dim : (head + 1) * head_dim].astype(jnp.float32)
        x = x * lax.rsqrt(jnp.mean(x * x, axis=-1, keepdims=True) + EPSILON) * gain[...]
        quarter = head_dim // 4
        mate = jnp.where(first_half, pltpu.roll(x, head_dim - quarter, 1), pltpu.roll(x, quarter, 1))
        return (x * cosine + mate * sine).astype(jnp.bfloat16)

    def send(src, dst, s_sem, r_sem, target):
        copy = pltpu.make_async_remote_copy(
            src_ref=src, dst_ref=dst, send_sem=s_sem, recv_sem=r_sem, device_id=target, device_id_type=MESH
        )
        copy.start()

    def landed(dst, s_sem, r_sem):
        pltpu.make_async_remote_copy(
            src_ref=dst, dst_ref=dst, send_sem=s_sem, recv_sem=r_sem, device_id=(sp, other), device_id_type=MESH
        ).wait_recv()

    def left(src, s_sem, r_sem):
        pltpu.make_async_remote_copy(
            src_ref=src, dst_ref=src, send_sem=s_sem, recv_sem=r_sem, device_id=(sp, other), device_id_type=MESH
        ).wait_send()

    def gu_at(source, first=0, count=None):
        return wgu.at[pl.ds(pl.multiple_of(source * depth + first, 16), depth if count is None else count)]

    def dn_at(source, first=0, count=None):
        return wdn.at[pl.ds(first, width if count is None else count), pl.ds(pl.multiple_of(source * cols, cols), cols)]

    for index in range(SPLIT):
        kv_ref[index, :, 0:head_dim] = turn(key_ref, index, k_gain_ref)
        kv_ref[index, :, head_dim : 2 * head_dim] = value_ref[:, index * head_dim : (index + 1) * head_dim]

    pl.semaphore_wait(barrier, SPLIT - 1 + 3 + 1)

    ways = ((part < last, 1), (part > 0, -1))
    kv_ways = (part < last - 1, part > 1)
    at_end = (part == 0) | (part == last)
    inner = (part > 0) & (part < last)
    inward = jnp.where(part == 0, 1, last - 1)
    outward = jnp.where(part == 1, 0, last)

    def kv_on(way, step, source, piece, src=None):
        slot = kvb.at[source, piece]
        send(
            slot if src is None else src,
            slot,
            kvz_s.at[way, step, piece],
            kvz_r.at[way, step, piece],
            (sp + ranks * ways[way][1], core),
        )

    own_kv = kv_ref.at[rank]
    for e in flips:
        send(kv_ref.at[flip(e)], kvb.at[part, rank], kvp_s.at[e], kvp_r.at[e], (near(e), core))
    for way in (0, 1):

        @pl.when(kv_ways[way])
        def _():
            kv_on(way, 0, part, rank, own_kv)

    locals_ = [
        pltpu.make_async_copy(own_kv, kvb.at[part, rank], local_sem.at[0]),
        pltpu.make_async_copy(dn_own(part), dn_at(sp), local_sem.at[3]),
    ]
    for copy in locals_:
        copy.start()

    for index in range(SPLIT):
        for head in range(group):
            lanes = slice(head * head_dim, (head + 1) * head_dim)
            q_ref[index, :, lanes] = turn(query_ref, index * group + head, q_gain_ref)
    for e in flips:
        send(q_ref.at[flip(e)], qb.at[0, rank], q_s.at[e], q_r.at[e], (near(e), core))
    q_own = pltpu.make_async_copy(q_ref.at[rank], qb.at[0, rank], local_sem.at[1])
    q_own.start()

    loads[0].wait()
    loads[1].wait()
    whole_lanes = width // 128 * 128
    for index in range(SPLIT):
        start = index * width // 128 * 128
        skew = index * width - start
        rests = []
        for which, ref in enumerate((gate_ref, up_ref)):
            block = ref[:, start : start + whole_lanes + 128]
            if skew:
                block = pltpu.roll(block.astype(jnp.float32), whole_lanes + 128 - skew, 1).astype(jnp.bfloat16)
            gu_ref[index, :, which * whole_lanes : (which + 1) * whole_lanes] = block[:, :whole_lanes]
            rests.append(block[:, whole_lanes:].astype(jnp.float32))
        spread = lax.broadcasted_iota(jnp.int32, rests[0].shape, 1)
        tail = jnp.where(spread < width - whole_lanes, rests[0], pltpu.roll(rests[1], width - whole_lanes, 1))
        gu_ref[index, :, 2 * whole_lanes :] = tail.astype(jnp.bfloat16)
    gu_own = pltpu.make_async_copy(gu_ref.at[part], gu_at(sp), local_sem.at[2])
    gu_own.start()
    pad = wdn.shape[0] - width
    wdn[pl.ds(width, pad), :] = jnp.zeros((pad, wdn.shape[1]), wdn.dtype)
    for e in (1, 2):
        send(gu_ref.at[part], gu_at(sp), gx_s.at[part, e], gx_r.at[part, e], (near(e), core))
    for e in (1, 2):
        send(dn_own(part), dn_at(sp), dx_s.at[part, e], dx_r.at[part, e], (near(e), core))

    def gate_to(target):
        @pl.when((target >= 0) & (target < SPLIT))
        def _():
            send(gu_ref.at[target], gu_at(sp), gz_s.at[target], gz_r.at[part], (at_part(target), core))

    def down_to(target):
        @pl.when((target >= 0) & (target < SPLIT))
        def _():
            send(dn_own(target), dn_at(sp), dz_s.at[target], dz_r.at[part], (at_part(target), core))

    def downs_in(stage):
        for way, behind in ((0, part), (1, last - part)):

            @pl.when((behind == stage) & (stage < SPLIT - 2))
            def _():
                for d in flips:
                    down_to(part + d * ways[way][1])

    def gu_pass(source):
        place = gu_at(at_part(source))
        landed(place, gz_s.at[source], gz_r.at[source])
        for e in (1, 2):
            send(place, place, gx_s.at[source, e], gx_r.at[source, e], (near(e), core))

    def dn_pass(source):
        place = dn_at(at_part(source))
        landed(place, dz_s.at[source], dz_r.at[source])
        for e in (1, 2):
            send(place, place, dx_s.at[source, e], dx_r.at[source, e], (near(e), core))

    def gu_halves(source):
        for e in (1, 2):
            origin = source * ranks + flip(e)
            landed(gu_at(origin), gx_s.at[source, e], gx_r.at[source, e])
            half = gu_at(origin, (e - 1) * depth // 2, depth // 2)
            send(half, half, gh_s.at[source, e], gh_r.at[source, e], (near(3 - e), core))

    def dn_halves(source):
        for e in (1, 2):
            origin = source * ranks + flip(e)
            landed(dn_at(origin), dx_s.at[source, e], dx_r.at[source, e])
            half = dn_at(origin, (e - 1) * width // 2, width // 2)
            send(half, half, dh_s.at[source, e], dh_r.at[source, e], (near(3 - e), core))

    def gu_done(source):
        for e in (1, 2):
            origin = source * ranks + flip(3)
            landed(gu_at(origin, (e - 1) * depth // 2, depth // 2), gh_s.at[source, e], gh_r.at[source, e])

    def dn_done(source):
        for e in (1, 2):
            origin = source * ranks + flip(3)
            landed(dn_at(origin, (e - 1) * width // 2, width // 2), dh_s.at[source, e], dh_r.at[source, e])

    high, odd = part // 2, part % 2
    nears = (part + 1 - 2 * odd, 2 - high, 3 - 3 * high)

    def present(way, step):
        source = part - ways[way][1] * (step + 1)
        return source, (source >= 0) & (source < SPLIT)

    def kv_hop(step):
        for way in (0, 1):
            source, there = present(way, step)

            @pl.when(there & inner)
            def _():
                for piece in range(ranks):
                    landed(kvb.at[source, piece], kvz_s.at[way, step, piece], kvz_r.at[way, step, piece])
                    if step == 0:

                        @pl.when(kv_ways[way])
                        def _():
                            kv_on(way, 1, source, piece)

    @pl.when(inner)
    def _():
        gate_to(outward)
        down_to(outward)

    for e in flips:
        landed(kvb.at[part, flip(e)], kvp_s.at[e], kvp_r.at[e])
        for way in (0, 1):

            @pl.when(kv_ways[way])
            def _():
                kv_on(way, 0, part, flip(e))

    locals_[0].wait()
    q_own.wait()
    for e in flips:
        landed(qb.at[0, flip(e)], q_s.at[e], q_r.at[e])

    factor = head_dim ** (-0.5) * math.log2(math.e)
    length = SPLIT * ranks * rows

    def attend(plane, piece, target):
        @pl.loop(0, group)
        def _(head):
            lanes = pl.ds(pl.multiple_of(head * head_dim, head_dim), head_dim)
            q = qb[plane, piece, :, lanes]
            keys = kvb[:, :, :, pl.ds(0, head_dim)].reshape(length, head_dim)
            scores = lax.dot_general(q, keys, (((1,), (1,)), ((), ())), preferred_element_type=jnp.float32)
            peak = jnp.max(scores, axis=-1, keepdims=True)
            weights = jnp.exp2((scores - peak) * factor)
            total = jnp.sum(weights, axis=-1, keepdims=True)
            vals = kvb[:, :, :, pl.ds(head_dim, head_dim)].reshape(length, head_dim)
            summed = jnp.dot(weights.astype(jnp.bfloat16), vals, preferred_element_type=jnp.float32)
            target[:, lanes] = (summed / total).astype(jnp.bfloat16)

    def attend_away(piece):
        attend(1, piece, asend.at[1, piece])
        send(
            asend.at[1, piece],
            ab.at[rank],
            at_s.at[1, piece],
            at_r.at[rank],
            (outward * ranks + piece, core),
        )


    @pl.when(at_end)
    def _():
        for piece in range(ranks):
            slot = qb.at[0, piece]
            send(slot, qb.at[1, piece], qz_s.at[piece], qz_r.at[piece], (at_part(inward), core))
        for d in flips:
            gate_to(part + d * jnp.where(part == 0, 1, -1))
        gu_halves(part)
        dn_halves(part)
        gu_pass(nears[0])
        gu_halves(nears[0])
        gu_pass(nears[1])
        gu_halves(nears[1])

    @pl.when(inner)
    def _():
        kv_hop(0)
        for d in (1, 2):
            gate_to(part + d * jnp.where(part == 1, 1, -1))
        gu_halves(part)
        dn_halves(part)
        kv_hop(1)
        for piece in range(ranks):
            landed(qb.at[1, piece], qz_s.at[piece], qz_r.at[piece])

        @pl.loop(0, 2)
        def _(piece):
            attend_away(piece)

        gu_pass(nears[0])

        @pl.loop(2, 4)
        def _(piece):
            attend_away(piece)

        gu_halves(nears[0])

        @pl.loop(1, 4)
        def _(turn_by):
            piece = (rank + turn_by) % ranks
            attend(0, piece, asend.at[0, piece])
            send(
                asend.at[0, piece],
                ab.at[rank],
                at_s.at[0, piece],
                at_r.at[rank],
                (part * ranks + piece, core),
                )

        attend(0, rank, ab.at[rank])
        gu_pass(nears[1])
        gu_halves(nears[1])

    loads[2].wait()
    for e in flips:
        landed(ab.at[flip(e)], at_s.at[0, flip(e)], at_r.at[flip(e)])

    @pl.when(at_end)
    def _():
        landed(ab.at[rank], at_s.at[0, rank], at_r.at[rank])

    attn = jnp.concatenate([ab[index] for index in range(SPLIT)], axis=1)
    tile = 512
    for first in range(0, ow_ref.shape[1], tile):
        block = jnp.dot(attn, ow_ref[:, first : first + tile], preferred_element_type=jnp.float32)
        pj[:, :, first : first + tile] = block.astype(jnp.bfloat16).reshape(2, share, tile)
    send(pj.at[other], prv, pj_s, pj_r, (sp, other))
    landed(prv, pj_s, pj_r)
    proj = pj[core].astype(jnp.float32) + prv[...].astype(jnp.float32)
    stream = (resid_ref[pl.ds(pl.multiple_of(core * share, 16), share)].astype(jnp.float32) + proj).astype(jnp.bfloat16)
    st[...] = stream
    wide = stream.astype(jnp.float32)
    level = lax.rsqrt(jnp.mean(wide * wide, axis=-1, keepdims=True) + EPSILON)
    nb[part, core] = (wide * level * gain_ref[...]).astype(jnp.bfloat16)

    def step_on(source, step, way):
        slot = nb.at[source, core]

        @pl.when(ways[way][0])
        def _():
            send(slot, slot, nz_s.at[way, step], nz_r.at[way, step], (sp + ranks * ways[way][1], core))

    step_on(part, 0, 0)
    step_on(part, 0, 1)
    downs_in(0)
    mine = nb.at[part, core]
    send(mine, mine, np_s.at[part], np_r.at[part], (sp, other))

    def hop(step):
        for way in (0, 1):
            source, there = present(way, step)

            @pl.when(there)
            def _():
                slot = nb.at[source, core]
                landed(slot, nz_s.at[way, step], nz_r.at[way, step])
                if step < SPLIT - 2:
                    step_on(source, step + 1, way)
                send(slot, slot, np_s.at[source], np_r.at[source], (sp, other))

    hop(0)
    downs_in(1)
    gu_pass(nears[2])
    dn_pass(nears[0])
    hop(1)
    gu_halves(nears[2])
    gu_own.wait()
    gu_done(part)
    for source in nears:
        gu_done(source)

    main = width // 128 * 128
    half_lane = width - main

    def feed(source):
        landed(nb.at[source, other], np_s.at[source], np_r.at[source])
        x = nb[source].reshape(rows, nb.shape[-1])
        gate = jnp.dot(x, wgu[:, pl.ds(0, main)], preferred_element_type=jnp.float32)
        up = jnp.dot(x, wgu[:, pl.ds(main, main)], preferred_element_type=jnp.float32)
        hb[source, :, 0:main] = (gate / (1.0 + jnp.exp(-gate)) * up).astype(jnp.bfloat16)
        rest = jnp.dot(x, wgu[:, pl.ds(2 * main, 128)], preferred_element_type=jnp.float32)
        turned = pltpu.roll(rest, half_lane, 1)
        where = lax.broadcasted_iota(jnp.int32, rest.shape, 1)
        tail = jnp.where(where < half_lane, rest / (1.0 + jnp.exp(-rest)) * turned, 0.0)
        hb[source, :, main : main + 128] = tail.astype(jnp.bfloat16)

    feed(part)
    feed(nears[0])
    dn_halves(nears[0])
    dn_pass(nears[1])
    feed(nears[1])
    dn_halves(nears[1])
    dn_pass(nears[2])
    hop(2)
    feed(nears[2])
    locals_[1].wait()
    dn_done(part)
    dn_done(nears[0])
    dn_done(nears[1])

    order = (3 - 3 * high, 2 - 2 * odd + high, 1 + odd, part)
    wide_cols = ranks * cols

    def pair_sum(b, place):
        landed(drv.at[b, place], dp_s.at[b, place], dp_r.at[b, place])
        return dsb[b, order[place], core].astype(jnp.float32) + drv[b, place].astype(jnp.float32)

    def onward(b, place, first):
        target = order[place]
        way = 1 - (target > part).astype(jnp.int32)
        total = pair_sum(b, place)
        if not first:
            landed(dzb.at[b, way, target], fz_s.at[b, way, target], fz_r.at[b, way, target])
            total = total + dzb[b, way, target].astype(jnp.float32)
        ds2[b, target] = total.astype(jnp.bfloat16)
        send(
            ds2.at[b, target],
            dzb.at[b, way, target],
            fz_s.at[b, way, target],
            fz_r.at[b, way, target],
            (sp + ranks * (1 - 2 * way), core),
        )

    def stage(b):
        for place in range(SPLIT):
            target = order[place]
            block = jnp.dot(hb[target], wdn[:, b * wide_cols : (b + 1) * wide_cols], preferred_element_type=jnp.float32)
            dsb[b, target] = block.astype(jnp.bfloat16).reshape(2, share, wide_cols)
            send(dsb.at[b, target, other], drv.at[b, place], dp_s.at[b, place], dp_r.at[b, place], (sp, other))

        @pl.when(at_end)
        def _():
            for place in range(last):
                onward(b, place, True)

        @pl.when(inner)
        def _():
            for place in range(last):
                onward(b, place, False)

    stage(1)
    stage(2)
    dn_halves(nears[2])
    dn_done(nears[2])
    stage(0)
    stage(3)

    for b in (1, 2, 0, 3):
        lanes = slice(b * wide_cols, (b + 1) * wide_cols)
        acc = pair_sum(b, last)
        base = st[:, lanes].astype(jnp.float32)

        def add(way, value, b=b):
            landed(dzb.at[b, way, part], fz_s.at[b, way, part], fz_r.at[b, way, part])
            return value + dzb[b, way, part].astype(jnp.float32)

        @pl.when(part == 0)
        def _():
            out_ref[:, lanes] = (base + 0.5 * add(1, acc)).astype(jnp.bfloat16)

        @pl.when(part == last)
        def _():
            out_ref[:, lanes] = (base + 0.5 * add(0, acc)).astype(jnp.bfloat16)

        @pl.when(inner)
        def _():
            out_ref[:, lanes] = (base + 0.5 * add(1, add(0, acc))).astype(jnp.bfloat16)

    for e in flips:
        left(kv_ref.at[flip(e)], kvp_s.at[e], kvp_r.at[e])
        left(q_ref.at[flip(e)], q_s.at[e], q_r.at[e])
    for source in range(SPLIT):
        for e in (1, 2):
            place = at_part(source)
            left(gu_at(place), gx_s.at[source, e], gx_r.at[source, e])
            left(dn_at(place), dx_s.at[source, e], dx_r.at[source, e])
            left(gu_at(place, 0, depth // 2), gh_s.at[source, e], gh_r.at[source, e])
            left(dn_at(place, 0, width // 2), dh_s.at[source, e], dh_r.at[source, e])
    left(prv, pj_s, pj_r)
    left(mine, np_s.at[part], np_r.at[part])
    for b in range(SPLIT):
        for place in range(SPLIT):
            left(drv.at[b, place], dp_s.at[b, place], dp_r.at[b, place])
    for dz in range(1, SPLIT):
        target = (part + dz) % SPLIT
        left(gu_ref.at[target], gz_s.at[target], gz_r.at[target])
        left(dn_own(target), dz_s.at[target], dz_r.at[target])
    for way in (0, 1):
        for step in range(SPLIT - 1):
            source, there = present(way, step)

            @pl.when(there)
            def _():
                left(nb.at[source, core], np_s.at[source], np_r.at[source])

        for step in range(SPLIT - 1):
            source, there = present(way, step - 1)

            @pl.when(ways[way][0] & there)
            def _():
                left(nb.at[source, core], nz_s.at[way, step], nz_r.at[way, step])

            if step < 2:

                @pl.when(kv_ways[way] & there)
                def _():
                    for piece in range(ranks):
                        left(kvb.at[source, piece], kvz_s.at[way, step, piece], kvz_r.at[way, step, piece])

    @pl.when(at_end)
    def _():
        for piece in range(ranks):
            left(qb.at[0, piece], qz_s.at[piece], qz_r.at[piece])

    @pl.when(inner)
    def _():
        for piece in range(ranks):
            left(asend.at[1, piece], at_s.at[1, piece], at_r.at[rank])
        for e in flips:
            left(asend.at[0, flip(e)], at_s.at[0, flip(e)], at_r.at[rank])

    for b in range(SPLIT):
        for place in range(last):
            target = order[place]
            way = 1 - (target > part).astype(jnp.int32)
            left(ds2.at[b, target], fz_s.at[b, way, target], fz_r.at[b, way, target])


def run_layer(key, value, query, k_gain, q_gain, gate, up, down, out_weight, resid, gain, ranks):
    rows = query.shape[0]
    share = rows // 2
    model = resid.shape[1]
    width = down.shape[0] // SPLIT
    depth = gate.shape[0]
    head_dim = q_gain.shape[0]
    n_sp = ranks * SPLIT
    quarter = head_dim // 4
    steps = np.tile(np.arange(quarter, dtype=np.float32), 4)
    freq = jnp.asarray((np.float64(10000.0) ** (-steps / quarter)).astype(np.float32))[None, :]
    half = jnp.bfloat16
    dma = pltpu.SemaphoreType.DMA
    padded = -(-width // 128) * 128
    some = model // SPLIT
    anywhere = pl.BlockSpec(memory_space=pl.ANY)
    inside = pl.BlockSpec(memory_space=pltpu.VMEM)
    kv_shape = (SPLIT, rows, 2 * head_dim)
    q_shape = (SPLIT, rows, query.shape[1] // SPLIT)
    return pl.pallas_call(
        functools.partial(layer_kernel, ranks, head_dim),
        out_shape=jax.ShapeDtypeStruct((share, model), half),
        in_specs=[inside] * 6 + [anywhere] * 4 + [inside] * 2,
        out_specs=inside,
        scratch_shapes=[
            pltpu.VMEM((SPLIT, ranks, rows, 2 * head_dim), half),
            pltpu.VMEM((2, *q_shape), half),
            pltpu.VMEM((2, *q_shape), half),
            pltpu.VMEM(q_shape, half),
            pltpu.VMEM((n_sp * depth, 2 * width), half),
            pltpu.VMEM((padded, model), half),
            pltpu.VMEM((2, share, model), half),
            pltpu.VMEM((share, model), half),
            pltpu.VMEM((SPLIT, 2, share, model), half),
            pltpu.VMEM((share, model), half),
            pltpu.VMEM((SPLIT, rows, padded), half),
            pltpu.VMEM((SPLIT, SPLIT, 2, share, some), half),
            pltpu.VMEM((SPLIT, SPLIT, share, some), half),
            pltpu.VMEM((SPLIT, SPLIT, share, some), half),
            pltpu.VMEM((SPLIT, 2, SPLIT, share, some), half),
            pltpu.VMEM(kv_shape, half),
            pltpu.VMEM(q_shape, half),
            pltpu.VMEM((SPLIT, depth, 2 * width), half),
            pltpu.VMEM(gate.shape, half),
            pltpu.VMEM(up.shape, half),
            pltpu.VMEM(out_weight.shape, half),
            dma((7,)),
        ]
        + [dma((SPLIT,))] * 13
        + [dma((SPLIT, SPLIT))] * 10
        + [dma((2, SPLIT, ranks))] * 2
        + [dma((SPLIT, 2, SPLIT))] * 2
        + [dma((2, SPLIT))] * 3
        + [dma, dma],
        compiler_params=pltpu.CompilerParams(
            collective_id=0, has_side_effects=True, vmem_limit_bytes=62 * 1024 * 1024
        ),
    )(
        key, value, query, k_gain[None, :], q_gain[None, :], freq, gate, up, down, out_weight, resid, gain[None, :]
    )


def in_kernel(n_sp, n_tp, kv_here, head_dim, width):
    return n_sp == 4 * SPLIT and n_tp == 2 and kv_here == SPLIT and head_dim == 128 and width % 128 == 64


def body(
    resid,
    query,
    key,
    value,
    q_gain,
    k_gain,
    out_weight,
    norm_gain,
    gate_weight,
    up_weight,
    down_weight,
):
    rows = query.shape[0]
    head_dim = q_gain.shape[0]
    heads_here = query.shape[1] // head_dim
    kv_here = key.shape[1] // head_dim
    n_sp = lax.axis_size("sp")
    if not fits(n_sp, kv_here, gate_weight.shape[1]):
        return whole_body(
            resid, query, key, value, q_gain, k_gain, out_weight, norm_gain, gate_weight, up_weight, down_weight
        )
    hidden_part = gate_weight.shape[1] // SPLIT
    ranks = n_sp // SPLIT
    if in_kernel(n_sp, lax.axis_size("tp"), kv_here, head_dim, hidden_part):
        return run_layer(
            key, value, query, k_gain, q_gain, gate_weight, up_weight, down_weight, out_weight, resid, norm_gain, ranks
        )
    tok_groups, hid_groups = groups_of(n_sp)
    ranks = n_sp // SPLIT
    group_size = heads_here // kv_here
    kv_part = kv_here // SPLIT

    def swap(array):
        return lax.all_to_all(array, "sp", 0, 0, axis_index_groups=tok_groups, tiled=True)

    def spread(array, axis):
        return lax.all_gather(array, "sp", axis=axis, axis_index_groups=hid_groups, tiled=True)

    positions = lax.axis_index("sp") * rows + jnp.arange(rows, dtype=jnp.int32)
    q_rot = prepare(query.reshape(rows, heads_here, head_dim), q_gain, positions)
    k_rot = prepare(key.reshape(rows, kv_here, head_dim), k_gain, positions)
    cut = lambda a: a.reshape(a.shape[0], SPLIT, -1).transpose(1, 0, 2).reshape(SPLIT * a.shape[0], -1)
    k_rot, val = cut(k_rot), cut(value)
    pair = swap(jnp.concatenate([k_rot, val], axis=1))
    pair = spread(pair, 0)
    q_mine = swap(cut(q_rot))
    width = kv_part * head_dim
    keys = pair[:, :width].reshape(-1, kv_part, head_dim)
    vals = pair[:, width:].reshape(-1, kv_part, head_dim)
    grouped = q_mine.reshape(SPLIT * rows, kv_part, group_size, head_dim)
    gate_up = spread(swap(jnp.concatenate([cut(gate_weight), cut(up_weight)], axis=1)), 0)
    depth = gate_weight.shape[0]
    gate_up = gate_up.reshape(ranks, SPLIT, depth, -1).transpose(1, 0, 2, 3).reshape(n_sp * depth, -1)
    down_w = swap(down_weight)
    part = down_weight.shape[0] // SPLIT
    down_w = down_w.reshape(SPLIT, part, -1)
    down_w = lax.all_gather(down_w, "sp", axis=1, axis_index_groups=hid_groups)
    down_w = jnp.transpose(down_w, (2, 0, 1, 3)).reshape(part, -1)
    scores = jnp.einsum("qkgd,skd->kgqs", grouped, keys, preferred_element_type=jnp.float32) * head_dim ** (-0.5)
    weights = jnp.exp(scores - jnp.max(scores, axis=-1, keepdims=True))
    totals = jnp.sum(weights, axis=-1)
    accum = jnp.einsum("kgqs,skd->kgqd", weights.astype(jnp.bfloat16), vals, preferred_element_type=jnp.float32)
    attn = jnp.transpose(accum / totals[..., None], (2, 0, 1, 3)).astype(jnp.bfloat16).reshape(SPLIT * rows, -1)
    attn = swap(attn).reshape(SPLIT, rows, -1).transpose(1, 0, 2).reshape(rows, -1)
    return finish(attn, resid, out_weight, norm_gain, gate_up, down_w, tok_groups)


def finish(attn, resid, out_weight, norm_gain, gate_up, down_w, tok_groups):
    rows = resid.shape[0]
    n_tp = lax.axis_size("tp")
    share = rows // n_tp
    my_first = lax.axis_index("tp") * share
    proj = lax.psum_scatter(
        jnp.dot(attn, out_weight, preferred_element_type=jnp.float32).astype(jnp.bfloat16),
        "tp",
        scatter_dimension=0,
        tiled=True,
    ).astype(jnp.float32)
    my_resid = lax.dynamic_slice_in_dim(resid, my_first, share, 0)
    my_stream = (my_resid.astype(jnp.float32) + proj).astype(jnp.bfloat16)
    normed = normalize(my_stream, norm_gain)
    normed = lax.all_gather(normed, "sp", axis=0, axis_index_groups=tok_groups, tiled=False)
    normed = lax.all_gather(normed, "tp", axis=0, tiled=False)
    normed = normed.reshape(n_tp * SPLIT * share, -1)
    both = jnp.dot(normed, gate_up, preferred_element_type=jnp.float32)
    gate, up_part = jnp.split(both, 2, axis=1)
    hidden = (jax.nn.silu(gate) * up_part).astype(jnp.bfloat16)
    down = jnp.dot(hidden, down_w, preferred_element_type=jnp.float32).astype(jnp.bfloat16)
    down = lax.psum_scatter(down, "tp", scatter_dimension=0, tiled=True)
    down = lax.all_to_all(
        down.reshape(SPLIT, share, -1), "sp", 0, 0, axis_index_groups=tok_groups, tiled=True
    )
    down = jnp.sum(down.astype(jnp.float32), axis=0)
    return (my_stream.astype(jnp.float32) + 0.5 * down).astype(jnp.bfloat16)


def solution(mesh):
    placed = (
        P("sp", None),
        P("sp", "tp"),
        P("sp", "tp"),
        P("sp", "tp"),
        P(),
        P(),
        P("tp", None),
        P(),
        P("sp", "tp"),
        P("sp", "tp"),
        P("tp", "sp"),
    )
    return jax.shard_map(
        body, mesh=mesh, in_specs=placed, out_specs=P(("sp", "tp"), None), check_vma=False
    )
```

```python
import functools
import math

import jax
import jax.numpy as jnp
import numpy as np
from jax import lax
from jax.experimental import pallas as pl
from jax.experimental.pallas import tpu as pltpu
from jax.sharding import PartitionSpec as P

GRID_W = 64


EPSILON = 1e-06


def rotate(values, positions):
    dim_size = values.shape[-1]
    half_dim = dim_size // 2
    quarter = half_dim // 2
    inverse = 10000.0 ** (-jnp.arange(quarter, dtype=jnp.float32) / quarter)
    outputs = []
    for axis_pos, coords in enumerate((positions // GRID_W, positions % GRID_W)):
        angles = coords.astype(jnp.float32)[:, None] * inverse[None, :]
        cosine = jnp.cos(angles)[:, None, :]
        sine = jnp.sin(angles)[:, None, :]
        section = values[..., axis_pos * half_dim : (axis_pos + 1) * half_dim]
        first_half = section[..., :quarter]
        second_half = section[..., quarter:]
        outputs += [
            first_half * cosine - second_half * sine,
            second_half * cosine + first_half * sine,
        ]
    return jnp.concatenate(outputs, axis=-1)


def prepare(projected, gain, positions):
    values = projected.astype(jnp.float32)
    normed = values * lax.rsqrt(jnp.mean(values * values, axis=-1, keepdims=True) + EPSILON) * gain
    return rotate(normed, positions).astype(jnp.bfloat16)


def normalize(stream, gain):
    values = stream.astype(jnp.float32)
    return (
        values * lax.rsqrt(jnp.mean(values * values, axis=-1, keepdims=True) + EPSILON) * gain
    ).astype(jnp.bfloat16)


def whole_body(
    resid,
    query,
    key,
    value,
    q_gain,
    k_gain,
    out_weight,
    norm_gain,
    gate_weight,
    up_weight,
    down_weight,
):
    rows_here = query.shape[0]
    head_dim = q_gain.shape[0]
    heads_here = query.shape[1] // head_dim
    kv_here = key.shape[1] // head_dim
    group_size = heads_here // kv_here
    score_scale = head_dim ** (-0.5)
    positions = lax.axis_index("sp") * rows_here + jnp.arange(rows_here, dtype=jnp.int32)
    q_rot = prepare(query.reshape(rows_here, heads_here, head_dim), q_gain, positions)
    k_rot = prepare(key.reshape(rows_here, kv_here, head_dim), k_gain, positions)
    val_rows = value.reshape(rows_here, kv_here, head_dim)
    grouped = q_rot.reshape(rows_here, kv_here, group_size, head_dim)

    def key_block(carry, block):
        maxima, totals, accum = carry
        block_keys, block_vals = block
        scores = (
            jnp.einsum("qkgd,skd->kgqs", grouped, block_keys, preferred_element_type=jnp.float32)
            * score_scale
        )
        new_max = jnp.maximum(maxima, jnp.max(scores, axis=-1))
        shrink = jnp.exp(maxima - new_max)
        weights = jnp.exp(scores - new_max[..., None])
        totals = totals * shrink + jnp.sum(weights, axis=-1)
        accum = accum * shrink[..., None] + jnp.einsum(
            "kgqs,skd->kgqd",
            weights.astype(jnp.bfloat16),
            block_vals,
            preferred_element_type=jnp.float32,
        )
        return ((new_max, totals, accum), None)

    start_max = jnp.full((kv_here, group_size, rows_here), -1e30, jnp.float32)
    start_total = jnp.zeros((kv_here, group_size, rows_here), jnp.float32)
    start_accum = jnp.zeros((kv_here, group_size, rows_here, head_dim), jnp.float32)
    carry = (start_max, start_total, start_accum)
    key_part = lax.all_gather(k_rot, "sp", axis=0, tiled=True)
    val_part = lax.all_gather(val_rows, "sp", axis=0, tiled=True)
    length = key_part.shape[0]
    factor = 4
    span = rows_here * factor
    turns = length // span
    key_blocks = key_part.reshape(turns, span, kv_here, head_dim)
    val_blocks = val_part.reshape(turns, span, kv_here, head_dim)
    carry, _ = lax.scan(key_block, carry, (key_blocks, val_blocks))
    maxima, totals, accum = carry
    attn = (
        jnp.transpose(accum / totals[..., None], (2, 0, 1, 3))
        .reshape(rows_here, heads_here * head_dim)
        .astype(jnp.bfloat16)
    )
    share = rows_here // lax.axis_size("tp")
    my_first = lax.axis_index("tp") * share
    proj = lax.psum_scatter(
        jnp.dot(attn, out_weight, preferred_element_type=jnp.float32).astype(jnp.bfloat16),
        "tp",
        scatter_dimension=0,
        tiled=True,
    ).astype(jnp.float32)
    my_resid = lax.dynamic_slice_in_dim(resid, my_first, share, 0)
    my_stream = (my_resid.astype(jnp.float32) + proj).astype(jnp.bfloat16)
    mixer_rows = lax.all_gather(normalize(my_stream, norm_gain), "tp", axis=0, tiled=True)

    def add_rows(shard_rows):
        return jnp.dot(mixer_rows, shard_rows, preferred_element_type=jnp.float32)

    gate = add_rows(lax.all_gather(gate_weight, "sp", axis=0, tiled=True))
    up_part = add_rows(lax.all_gather(up_weight, "sp", axis=0, tiled=True))
    hidden = (jax.nn.silu(gate) * up_part).astype(jnp.bfloat16)
    down_whole = lax.all_gather(down_weight, "sp", axis=1, tiled=True)
    down = lax.psum_scatter(
        jnp.dot(hidden, down_whole, preferred_element_type=jnp.float32).astype(jnp.bfloat16),
        "tp",
        scatter_dimension=0,
        tiled=True,
    ).astype(jnp.float32)
    return (my_stream.astype(jnp.float32) + 0.5 * down).astype(jnp.bfloat16)


SPLIT = 4


def fits(n_sp, kv_here, hidden_here):
    return n_sp % SPLIT == 0 and kv_here % SPLIT == 0 and hidden_here % (64 * SPLIT) == 0


def groups_of(n_sp):
    ranks = n_sp // SPLIT
    tokens = [[part * ranks + rank for part in range(SPLIT)] for rank in range(ranks)]
    hidden = [[part * ranks + rank for rank in range(ranks)] for part in range(SPLIT)]
    return tokens, hidden


MESH = pl.DeviceIdType.MESH


def layer_kernel(
    ranks,
    head_dim,
    key_ref,
    value_ref,
    query_ref,
    k_gain_ref,
    q_gain_ref,
    freq_ref,
    gate_hbm,
    up_hbm,
    down_ref,
    ow_hbm,
    resid_ref,
    gain_ref,
    out_hbm,
    out_ref,
    kvb,
    qb,
    asend,
    ab,
    wgu,
    wdn,
    pj,
    prv,
    nb,
    st,
    hb,
    dsb,
    drv,
    ds2,
    dzb,
    kv_ref,
    q_ref,
    gu_ref,
    gate_ref,
    up_ref,
    ow_ref,
    local_sem,
    kvp_s, q_s, qz_s, gz_s, dz_s, np_s, gx_s, dx_s, gh_s, dh_s, dp_s, fz_s, pj_s, pj_r, gh_r,
    kvp_r, q_r, qz_r, at_r, gz_r, dz_r, np_r, dh_r,
    gx_r, dx_r, dp_r, at_s, kvz_s, kvz_r, nz_s, nz_r, fz_r,
):
    sp = lax.axis_index("sp")
    core = lax.axis_index("tp")
    part = sp // ranks
    rank = sp % ranks
    rows = q_ref.shape[1]
    share = rows // 2
    depth = gu_ref.shape[1]
    width = down_ref.shape[0] // SPLIT
    cols = down_ref.shape[1]
    group = q_ref.shape[2] // head_dim
    other = 1 - core
    flips = (1, 2, 3)
    last = SPLIT - 1

    def flip(e):
        x = rank % 2
        y = rank // 2
        nx = 1 - x if e % 2 else x
        ny = 1 - y if e // 2 else y
        return ny * 2 + nx

    def near(e):
        return part * ranks + flip(e)

    def at_part(target):
        return target * ranks + rank

    def dn_own(index):
        return down_ref.at[pl.ds(pl.multiple_of(index * width, 16), width)]

    barrier = pltpu.get_barrier_semaphore()
    for dz in range(1, SPLIT):
        pl.semaphore_signal(barrier, inc=1, device_id=(at_part((part + dz) % SPLIT), core), device_id_type=MESH)
    for e in flips:
        pl.semaphore_signal(barrier, inc=1, device_id=(near(e), core), device_id_type=MESH)
    pl.semaphore_signal(barrier, inc=1, device_id=(sp, other), device_id_type=MESH)

    loads = [
        pltpu.make_async_copy(gate_hbm, gate_ref, local_sem.at[4]),
        pltpu.make_async_copy(up_hbm, up_ref, local_sem.at[5]),
        pltpu.make_async_copy(ow_hbm, ow_ref, local_sem.at[6]),
    ]
    for copy in loads:
        copy.start()

    lane = lax.broadcasted_iota(jnp.int32, (rows, head_dim), 1)
    spot = sp * rows + lax.broadcasted_iota(jnp.int32, (rows, head_dim), 0)
    grid_bits = GRID_W.bit_length() - 1
    coords = jnp.where(lane < head_dim // 2, spot >> grid_bits, spot & (GRID_W - 1))
    angles = coords.astype(jnp.float32) * freq_ref[...]
    first_half = (lane & (head_dim // 2 - 1)) < head_dim // 4
    cosine = jnp.cos(angles)
    sine = jnp.where(first_half, -jnp.sin(angles), jnp.sin(angles))

    def turn(ref, head, gain):
        x = ref[:, head * head_dim : (head + 1) * head_dim].astype(jnp.float32)
        x = x * lax.rsqrt(jnp.mean(x * x, axis=-1, keepdims=True) + EPSILON) * gain[...]
        quarter = head_dim // 4
        mate = jnp.where(first_half, pltpu.roll(x, head_dim - quarter, 1), pltpu.roll(x, quarter, 1))
        return (x * cosine + mate * sine).astype(jnp.bfloat16)

    def send(src, dst, s_sem, r_sem, target):
        copy = pltpu.make_async_remote_copy(
            src_ref=src, dst_ref=dst, send_sem=s_sem, recv_sem=r_sem, device_id=target, device_id_type=MESH
        )
        copy.start()

    def landed(dst, s_sem, r_sem):
        pltpu.make_async_remote_copy(
            src_ref=dst, dst_ref=dst, send_sem=s_sem, recv_sem=r_sem, device_id=(sp, other), device_id_type=MESH
        ).wait_recv()

    def left(src, s_sem, r_sem):
        pltpu.make_async_remote_copy(
            src_ref=src, dst_ref=src, send_sem=s_sem, recv_sem=r_sem, device_id=(sp, other), device_id_type=MESH
        ).wait_send()

    def gu_at(source, first=0, count=None):
        return wgu.at[pl.ds(pl.multiple_of(source * depth + first, 16), depth if count is None else count)]

    def dn_at(source, first=0, count=None):
        return wdn.at[pl.ds(first, width if count is None else count), pl.ds(pl.multiple_of(source * cols, cols), cols)]

    for index in range(SPLIT):
        kv_ref[index, :, 0:head_dim] = turn(key_ref, index, k_gain_ref)
        kv_ref[index, :, head_dim : 2 * head_dim] = value_ref[:, index * head_dim : (index + 1) * head_dim]

    pl.semaphore_wait(barrier, SPLIT - 1 + 3 + 1)

    ways = ((part < last, 1), (part > 0, -1))
    kv_ways = (part < last - 1, part > 1)
    at_end = (part == 0) | (part == last)
    inner = (part > 0) & (part < last)
    inward = jnp.where(part == 0, 1, last - 1)
    outward = jnp.where(part == 1, 0, last)

    def kv_on(way, step, source, piece, src=None):
        slot = kvb.at[source, piece]
        send(
            slot if src is None else src,
            slot,
            kvz_s.at[way, step, piece],
            kvz_r.at[way, step, piece],
            (sp + ranks * ways[way][1], core),
        )

    own_kv = kv_ref.at[rank]
    for e in flips:
        send(kv_ref.at[flip(e)], kvb.at[part, rank], kvp_s, kvp_r.at[e], (near(e), core))
    for way in (0, 1):

        @pl.when(kv_ways[way])
        def _():
            kv_on(way, 0, part, rank, own_kv)

    locals_ = [
        pltpu.make_async_copy(own_kv, kvb.at[part, rank], local_sem.at[0]),
        pltpu.make_async_copy(dn_own(part), dn_at(sp), local_sem.at[3]),
    ]
    for copy in locals_:
        copy.start()

    for index in range(SPLIT):
        for head in range(group):
            lanes = slice(head * head_dim, (head + 1) * head_dim)
            q_ref[index, :, lanes] = turn(query_ref, index * group + head, q_gain_ref)
    for e in flips:
        send(q_ref.at[flip(e)], qb.at[0, rank], q_s, q_r.at[e], (near(e), core))
    q_own = pltpu.make_async_copy(q_ref.at[rank], qb.at[0, rank], local_sem.at[1])
    q_own.start()

    loads[0].wait()
    loads[1].wait()
    whole_lanes = width // 128 * 128
    for index in range(SPLIT):
        start = index * width // 128 * 128
        skew = index * width - start
        rests = []
        for which, ref in enumerate((gate_ref, up_ref)):
            block = ref[:, start : start + whole_lanes + 128]
            if skew:
                block = pltpu.roll(block.astype(jnp.float32), whole_lanes + 128 - skew, 1).astype(jnp.bfloat16)
            gu_ref[index, :, which * whole_lanes : (which + 1) * whole_lanes] = block[:, :whole_lanes]
            rests.append(block[:, whole_lanes:].astype(jnp.float32))
        spread = lax.broadcasted_iota(jnp.int32, rests[0].shape, 1)
        tail = jnp.where(spread < width - whole_lanes, rests[0], pltpu.roll(rests[1], width - whole_lanes, 1))
        gu_ref[index, :, 2 * whole_lanes :] = tail.astype(jnp.bfloat16)
    gu_own = pltpu.make_async_copy(gu_ref.at[part], gu_at(sp), local_sem.at[2])
    gu_own.start()
    pad = wdn.shape[0] - width
    wdn[pl.ds(width, pad), :] = jnp.zeros((pad, wdn.shape[1]), wdn.dtype)
    for e in (1, 2):
        send(gu_ref.at[part], gu_at(sp), gx_s, gx_r.at[part, e - 1], (near(e), core))
    for e in (1, 2):
        send(dn_own(part), dn_at(sp), dx_s, dx_r.at[part, e - 1], (near(e), core))

    def gate_to(target):
        @pl.when((target >= 0) & (target < SPLIT))
        def _():
            send(gu_ref.at[target], gu_at(sp), gz_s, gz_r.at[part], (at_part(target), core))

    def down_to(target):
        @pl.when((target >= 0) & (target < SPLIT))
        def _():
            send(dn_own(target), dn_at(sp), dz_s, dz_r.at[part], (at_part(target), core))

    def gu_pass(source):
        place = gu_at(at_part(source))
        landed(place, gz_s, gz_r.at[source])
        for e in (1, 2):
            send(place, place, gx_s, gx_r.at[source, e - 1], (near(e), core))

    def dn_pass(source):
        place = dn_at(at_part(source))
        landed(place, dz_s, dz_r.at[source])
        for e in (1, 2):
            send(place, place, dx_s, dx_r.at[source, e - 1], (near(e), core))

    def gu_halves(source):
        for e in (1, 2):
            origin = source * ranks + flip(e)
            landed(gu_at(origin), gx_s, gx_r.at[source, e - 1])
            half = gu_at(origin, (e - 1) * depth // 2, depth // 2)
            send(half, half, gh_s, gh_r, (near(3 - e), core))

    def dn_halves(source):
        for e in (1, 2):
            origin = source * ranks + flip(e)
            landed(dn_at(origin), dx_s, dx_r.at[source, e - 1])
            half = dn_at(origin, (e - 1) * width // 2, width // 2)
            send(half, half, dh_s, dh_r.at[source], (near(3 - e), core))

    def dn_done(source):
        landed(dn_at(source * ranks + flip(3)), dh_s, dh_r.at[source])

    high, odd = part // 2, part % 2
    nears = (part + 1 - 2 * odd, 2 - high, 3 - 3 * high)
    second, third = jnp.where(inner, nears[2], nears[1]), jnp.where(inner, nears[1], nears[2])

    def present(way, step):
        source = part - ways[way][1] * (step + 1)
        return source, (source >= 0) & (source < SPLIT)

    def kv_hop(step):
        for way in (0, 1):
            source, there = present(way, step)

            @pl.when(there & inner)
            def _():
                for piece in range(ranks):
                    landed(kvb.at[source, piece], kvz_s.at[way, step, piece], kvz_r.at[way, step, piece])
                    if step == 0:

                        @pl.when(kv_ways[way])
                        def _():
                            kv_on(way, 1, source, piece)

    @pl.when(inner)
    def _():
        gate_to(outward)
        down_to(outward)

    for e in flips:
        landed(kvb.at[part, flip(e)], kvp_s, kvp_r.at[e])
        for way in (0, 1):

            @pl.when(kv_ways[way])
            def _():
                kv_on(way, 0, part, flip(e))

    locals_[0].wait()
    q_own.wait()
    for e in flips:
        landed(qb.at[0, flip(e)], q_s, q_r.at[e])

    factor = head_dim ** (-0.5) * math.log2(math.e)
    length = SPLIT * ranks * rows

    def attend(plane, piece, target):
        @pl.loop(0, group)
        def _(head):
            lanes = pl.ds(pl.multiple_of(head * head_dim, head_dim), head_dim)
            q = qb[plane, piece, :, lanes]
            keys = kvb[:, :, :, pl.ds(0, head_dim)].reshape(length, head_dim)
            scores = lax.dot_general(q, keys, (((1,), (1,)), ((), ())), preferred_element_type=jnp.float32)
            peak = jnp.max(scores, axis=-1, keepdims=True)
            weights = jnp.exp2((scores - peak) * factor)
            total = jnp.sum(weights, axis=-1, keepdims=True)
            vals = kvb[:, :, :, pl.ds(head_dim, head_dim)].reshape(length, head_dim)
            summed = jnp.dot(weights.astype(jnp.bfloat16), vals, preferred_element_type=jnp.float32)
            target[:, lanes] = (summed / total).astype(jnp.bfloat16)

    def attend_away(piece):
        attend(1, piece, asend.at[1, piece])
        send(
            asend.at[1, piece],
            ab.at[rank],
            at_s.at[1, piece],
            at_r.at[rank],
            (outward * ranks + piece, core),
        )


    @pl.when(at_end)
    def _():
        for piece in range(ranks):
            slot = qb.at[0, piece]
            send(slot, qb.at[1, piece], qz_s, qz_r.at[piece], (at_part(inward), core))
        for target in nears:
            gate_to(target)
        down_to(nears[0])
        gu_pass(nears[0])
        gu_halves(part)
        dn_halves(part)
        gu_halves(nears[0])
        dn_pass(nears[0])
        gu_pass(second)

    @pl.when(inner)
    def _():
        kv_hop(0)
        gate_to(nears[2])
        gate_to(nears[1])
        down_to(nears[2])
        down_to(nears[1])
        gu_halves(part)
        dn_halves(part)
        kv_hop(1)
        for piece in range(ranks):
            landed(qb.at[1, piece], qz_s, qz_r.at[piece])
        def attend_near(turn_by):
            piece = (rank + turn_by) % ranks
            attend(0, piece, asend.at[0, piece])
            send(
                asend.at[0, piece],
                ab.at[rank],
                at_s.at[0, piece],
                at_r.at[rank],
                (part * ranks + piece, core),
            )


        @pl.loop(1, 4)
        def _(turn_by):
            attend_near(turn_by)

        gu_pass(nears[0])

        @pl.loop(0, 3)
        def _(piece):
            attend_away(piece)

        gu_pass(second)
        attend_away(3)
        attend(0, rank, ab.at[rank])
        gu_halves(nears[0])

    loads[2].wait()
    for e in flips:
        landed(ab.at[flip(e)], at_s.at[0, flip(e)], at_r.at[flip(e)])

    @pl.when(at_end)
    def _():
        landed(ab.at[rank], at_s.at[0, rank], at_r.at[rank])

    attn = jnp.concatenate([ab[index] for index in range(SPLIT)], axis=1)
    tile = 512
    for first in range(0, ow_ref.shape[1], tile):
        block = jnp.dot(attn, ow_ref[:, first : first + tile], preferred_element_type=jnp.float32)
        pj[:, :, first : first + tile] = block.astype(jnp.bfloat16).reshape(2, share, tile)
    send(pj.at[other], prv, pj_s, pj_r, (sp, other))
    landed(prv, pj_s, pj_r)
    proj = pj[core].astype(jnp.float32) + prv[...].astype(jnp.float32)
    stream = (resid_ref[pl.ds(pl.multiple_of(core * share, 16), share)].astype(jnp.float32) + proj).astype(jnp.bfloat16)
    st[...] = stream
    wide = stream.astype(jnp.float32)
    level = lax.rsqrt(jnp.mean(wide * wide, axis=-1, keepdims=True) + EPSILON)
    nb[part, core] = (wide * level * gain_ref[...]).astype(jnp.bfloat16)

    def step_on(source, step, way):
        slot = nb.at[source, core]

        @pl.when(ways[way][0])
        def _():
            send(slot, slot, nz_s.at[way, step], nz_r.at[way, step], (sp + ranks * ways[way][1], core))

    step_on(part, 0, 0)
    step_on(part, 0, 1)
    mine = nb.at[part, core]
    send(mine, mine, np_s, np_r.at[part], (sp, other))

    def hop(step, chosen=(True, True)):
        for way in (0, 1):
            source, there = present(way, step)

            @pl.when(there & chosen[way])
            def _():
                slot = nb.at[source, core]
                landed(slot, nz_s.at[way, step], nz_r.at[way, step])
                if step < SPLIT - 2:
                    step_on(source, step + 1, way)
                send(slot, slot, np_s, np_r.at[source], (sp, other))

    outer = (at_end | (high == 0), at_end | (high == 1))
    across = (inner & (high == 1), inner & (high == 0))

    main = width // 128 * 128
    half_lane = width - main

    def feed(source):
        landed(nb.at[source, other], np_s, np_r.at[source])
        x = nb[source].reshape(rows, nb.shape[-1])
        gate = jnp.dot(x, wgu[:, pl.ds(0, main)], preferred_element_type=jnp.float32)
        up = jnp.dot(x, wgu[:, pl.ds(main, main)], preferred_element_type=jnp.float32)
        hb[source, :, 0:main] = (gate / (1.0 + jnp.exp(-gate)) * up).astype(jnp.bfloat16)
        rest = jnp.dot(x, wgu[:, pl.ds(2 * main, 128)], preferred_element_type=jnp.float32)
        turned = pltpu.roll(rest, half_lane, 1)
        where = lax.broadcasted_iota(jnp.int32, rest.shape, 1)
        tail = jnp.where(where < half_lane, rest / (1.0 + jnp.exp(-rest)) * turned, 0.0)
        hb[source, :, main : main + 128] = tail.astype(jnp.bfloat16)

    order = nears + (part,)
    wide_cols = ranks * cols
    first_cols, later_cols = (1, 2), (0, 3)

    def pair_sum(b, place):
        landed(drv.at[b, place], dp_s, dp_r.at[b, place])
        return dsb[b, order[place], core].astype(jnp.float32) + drv[b, place].astype(jnp.float32)

    def onward(blocks, place, first):
        target = order[place]
        way = 1 - (target > part).astype(jnp.int32)
        for b in blocks:
            total = pair_sum(b, place)
            if not first:
                landed(dzb.at[b, way, target], fz_s, fz_r.at[b, way, target])
                total = total + dzb[b, way, target].astype(jnp.float32)
            ds2[b, target] = total.astype(jnp.bfloat16)
            send(
                ds2.at[b, target],
                dzb.at[b, way, target],
                fz_s,
                fz_r.at[b, way, target],
                (sp + ranks * (1 - 2 * way), core),
            )

    def stage(blocks, place):
        target = order[place]
        for b in blocks:
            block = jnp.dot(hb[target], wdn[:, b * wide_cols : (b + 1) * wide_cols], preferred_element_type=jnp.float32)
            dsb[b, target] = block.astype(jnp.bfloat16).reshape(2, share, wide_cols)
            send(dsb.at[b, target, other], drv.at[b, place], dp_s, dp_r.at[b, place], (sp, other))

    def ends_on(blocks, place):
        @pl.when(at_end)
        def _():
            onward(blocks, place, True)

    gu_halves(second)
    gu_pass(third)

    @pl.when(inner)
    def _():
        dn_pass(nears[0])

    hop(0, outer)

    @pl.when(at_end)
    def _():
        down_to(nears[1])
        down_to(nears[2])

    gu_halves(third)
    dn_halves(nears[0])
    dn_pass(nears[1])
    gu_own.wait()
    landed(gu_at(0, 0, ranks * depth), gh_s, gh_r)
    feed(nears[0])
    hop(0, across)
    feed(part)
    dn_halves(nears[1])
    locals_[1].wait()
    dn_done(part)
    dn_done(nears[0])
    dn_done(nears[1])
    stage(first_cols, 0)
    stage(first_cols, 3)
    ends_on(first_cols, 0)
    hop(1)
    feed(nears[1])
    stage(first_cols, 1)
    dn_pass(nears[2])
    ends_on(first_cols, 1)
    hop(2)
    feed(nears[2])
    stage(first_cols, 2)
    dn_halves(nears[2])
    ends_on(first_cols, 2)

    @pl.when(inner)
    def _():
        onward(first_cols, 1, False)

    dn_done(nears[2])
    stage(later_cols, 0)
    stage(later_cols, 1)
    ends_on(later_cols, 0)
    stage(later_cols, 2)
    ends_on(later_cols, 1)
    stage(later_cols, 3)
    ends_on(later_cols, 2)

    @pl.when(inner)
    def _():
        for blocks, place in ((first_cols, 2), (first_cols, 0), (later_cols, 1), (later_cols, 2), (later_cols, 0)):
            onward(blocks, place, False)

    for b in first_cols + later_cols:
        lanes = slice(b * wide_cols, (b + 1) * wide_cols)
        acc = pair_sum(b, last)
        base = st[:, lanes].astype(jnp.float32)

        def add(way, value, b=b):
            landed(dzb.at[b, way, part], fz_s, fz_r.at[b, way, part])
            return value + dzb[b, way, part].astype(jnp.float32)

        @pl.when(part == 0)
        def _():
            out_ref[:, lanes] = (base + 0.5 * add(1, acc)).astype(jnp.bfloat16)

        @pl.when(part == last)
        def _():
            out_ref[:, lanes] = (base + 0.5 * add(0, acc)).astype(jnp.bfloat16)

        @pl.when(inner)
        def _():
            out_ref[:, lanes] = (base + 0.5 * add(1, add(0, acc))).astype(jnp.bfloat16)

        pltpu.make_async_copy(out_ref.at[:, lanes], out_hbm.at[:, lanes], local_sem.at[7 + b]).start()

    left(kv_ref.at[pl.ds(0, last)], kvp_s, kvp_r.at[1])
    left(q_ref.at[pl.ds(0, last)], q_s, q_r.at[1])
    left(gu_ref.at[pl.ds(0, last)], gz_s, gz_r.at[0])
    left(down_ref.at[pl.ds(0, last * width)], dz_s, dz_r.at[0])
    left(gu_at(0, 0, 2 * ranks * depth), gx_s, gx_r.at[0, 0])
    left(gu_at(0, 0, ranks * depth), gh_s, gh_r)
    left(wdn.at[pl.ds(0, width), pl.ds(0, 2 * wide_cols)], dx_s, dx_r.at[0, 0])
    left(wdn.at[pl.ds(0, width), pl.ds(0, wide_cols)], dh_s, dh_r.at[0])
    left(prv, pj_s, pj_r)
    left(nb.at[:, 0], np_s, np_r.at[0])
    left(drv, dp_s, dp_r.at[0, 0])
    left(drv.at[pl.ds(0, last)], fz_s, fz_r.at[0, 0, 0])
    for way in (0, 1):
        for step in range(SPLIT - 1):
            source, there = present(way, step - 1)

            @pl.when(ways[way][0] & there)
            def _():
                left(nb.at[source, core], nz_s.at[way, step], nz_r.at[way, step])

            if step < 2:

                @pl.when(kv_ways[way] & there)
                def _():
                    for piece in range(ranks):
                        left(kvb.at[source, piece], kvz_s.at[way, step, piece], kvz_r.at[way, step, piece])

    @pl.when(at_end)
    def _():
        left(qb.at[0], qz_s, qz_r.at[0])

    @pl.when(inner)
    def _():
        for piece in range(ranks):
            left(asend.at[1, piece], at_s.at[1, piece], at_r.at[rank])
        for e in flips:
            left(asend.at[0, flip(e)], at_s.at[0, flip(e)], at_r.at[rank])

    for b in range(SPLIT):
        lanes = slice(b * wide_cols, (b + 1) * wide_cols)
        pltpu.make_async_copy(out_ref.at[:, lanes], out_hbm.at[:, lanes], local_sem.at[7 + b]).wait()


def run_layer(key, value, query, k_gain, q_gain, gate, up, down, out_weight, resid, gain, ranks):
    rows = query.shape[0]
    share = rows // 2
    model = resid.shape[1]
    width = down.shape[0] // SPLIT
    depth = gate.shape[0]
    head_dim = q_gain.shape[0]
    n_sp = ranks * SPLIT
    quarter = head_dim // 4
    steps = np.tile(np.arange(quarter, dtype=np.float32), 4)
    freq = jnp.asarray((np.float64(10000.0) ** (-steps / quarter)).astype(np.float32))[None, :]
    half = jnp.bfloat16
    dma = pltpu.SemaphoreType.DMA
    padded = -(-width // 128) * 128
    some = model // SPLIT
    anywhere = pl.BlockSpec(memory_space=pl.ANY)
    inside = pl.BlockSpec(memory_space=pltpu.VMEM)
    kv_shape = (SPLIT, rows, 2 * head_dim)
    q_shape = (SPLIT, rows, query.shape[1] // SPLIT)
    return pl.pallas_call(
        functools.partial(layer_kernel, ranks, head_dim),
        out_shape=jax.ShapeDtypeStruct((share, model), half),
        in_specs=[inside] * 6 + [anywhere] * 4 + [inside] * 2,
        out_specs=anywhere,
        scratch_shapes=[
            pltpu.VMEM((share, model), half),
            pltpu.VMEM((SPLIT, ranks, rows, 2 * head_dim), half),
            pltpu.VMEM((2, *q_shape), half),
            pltpu.VMEM((2, *q_shape), half),
            pltpu.VMEM(q_shape, half),
            pltpu.VMEM((n_sp * depth, 2 * width), half),
            pltpu.VMEM((padded, model), half),
            pltpu.VMEM((2, share, model), half),
            pltpu.VMEM((share, model), half),
            pltpu.VMEM((SPLIT, 2, share, model), half),
            pltpu.VMEM((share, model), half),
            pltpu.VMEM((SPLIT, rows, padded), half),
            pltpu.VMEM((SPLIT, SPLIT, 2, share, some), half),
            pltpu.VMEM((SPLIT, SPLIT, share, some), half),
            pltpu.VMEM((SPLIT, SPLIT, share, some), half),
            pltpu.VMEM((SPLIT, 2, SPLIT, share, some), half),
            pltpu.VMEM(kv_shape, half),
            pltpu.VMEM(q_shape, half),
            pltpu.VMEM((SPLIT, depth, 2 * width), half),
            pltpu.VMEM(gate.shape, half),
            pltpu.VMEM(up.shape, half),
            pltpu.VMEM(out_weight.shape, half),
            dma((7 + SPLIT,)),
        ]
        + [dma] * 15
        + [dma((SPLIT,))] * 8
        + [dma((SPLIT, 2))] * 2
        + [dma((SPLIT, SPLIT)), dma((2, SPLIT))]
        + [dma((2, 2, ranks))] * 2
        + [dma((2, SPLIT - 1))] * 2
        + [dma((SPLIT, 2, SPLIT))],
        compiler_params=pltpu.CompilerParams(
            collective_id=0, has_side_effects=True, vmem_limit_bytes=62 * 1024 * 1024
        ),
    )(
        key, value, query, k_gain[None, :], q_gain[None, :], freq, gate, up, down, out_weight, resid, gain[None, :]
    )


def in_kernel(n_sp, n_tp, kv_here, head_dim, width):
    return n_sp == 4 * SPLIT and n_tp == 2 and kv_here == SPLIT and head_dim == 128 and width % 128 == 64


def body(
    resid,
    query,
    key,
    value,
    q_gain,
    k_gain,
    out_weight,
    norm_gain,
    gate_weight,
    up_weight,
    down_weight,
):
    rows = query.shape[0]
    head_dim = q_gain.shape[0]
    heads_here = query.shape[1] // head_dim
    kv_here = key.shape[1] // head_dim
    n_sp = lax.axis_size("sp")
    if not fits(n_sp, kv_here, gate_weight.shape[1]):
        return whole_body(
            resid, query, key, value, q_gain, k_gain, out_weight, norm_gain, gate_weight, up_weight, down_weight
        )
    hidden_part = gate_weight.shape[1] // SPLIT
    ranks = n_sp // SPLIT
    if in_kernel(n_sp, lax.axis_size("tp"), kv_here, head_dim, hidden_part):
        return run_layer(
            key, value, query, k_gain, q_gain, gate_weight, up_weight, down_weight, out_weight, resid, norm_gain, ranks
        )
    tok_groups, hid_groups = groups_of(n_sp)
    ranks = n_sp // SPLIT
    group_size = heads_here // kv_here
    kv_part = kv_here // SPLIT

    def swap(array):
        return lax.all_to_all(array, "sp", 0, 0, axis_index_groups=tok_groups, tiled=True)

    def spread(array, axis):
        return lax.all_gather(array, "sp", axis=axis, axis_index_groups=hid_groups, tiled=True)

    positions = lax.axis_index("sp") * rows + jnp.arange(rows, dtype=jnp.int32)
    q_rot = prepare(query.reshape(rows, heads_here, head_dim), q_gain, positions)
    k_rot = prepare(key.reshape(rows, kv_here, head_dim), k_gain, positions)
    cut = lambda a: a.reshape(a.shape[0], SPLIT, -1).transpose(1, 0, 2).reshape(SPLIT * a.shape[0], -1)
    k_rot, val = cut(k_rot), cut(value)
    pair = swap(jnp.concatenate([k_rot, val], axis=1))
    pair = spread(pair, 0)
    q_mine = swap(cut(q_rot))
    width = kv_part * head_dim
    keys = pair[:, :width].reshape(-1, kv_part, head_dim)
    vals = pair[:, width:].reshape(-1, kv_part, head_dim)
    grouped = q_mine.reshape(SPLIT * rows, kv_part, group_size, head_dim)
    gate_up = spread(swap(jnp.concatenate([cut(gate_weight), cut(up_weight)], axis=1)), 0)
    depth = gate_weight.shape[0]
    gate_up = gate_up.reshape(ranks, SPLIT, depth, -1).transpose(1, 0, 2, 3).reshape(n_sp * depth, -1)
    down_w = swap(down_weight)
    part = down_weight.shape[0] // SPLIT
    down_w = down_w.reshape(SPLIT, part, -1)
    down_w = lax.all_gather(down_w, "sp", axis=1, axis_index_groups=hid_groups)
    down_w = jnp.transpose(down_w, (2, 0, 1, 3)).reshape(part, -1)
    scores = jnp.einsum("qkgd,skd->kgqs", grouped, keys, preferred_element_type=jnp.float32) * head_dim ** (-0.5)
    weights = jnp.exp(scores - jnp.max(scores, axis=-1, keepdims=True))
    totals = jnp.sum(weights, axis=-1)
    accum = jnp.einsum("kgqs,skd->kgqd", weights.astype(jnp.bfloat16), vals, preferred_element_type=jnp.float32)
    attn = jnp.transpose(accum / totals[..., None], (2, 0, 1, 3)).astype(jnp.bfloat16).reshape(SPLIT * rows, -1)
    attn = swap(attn).reshape(SPLIT, rows, -1).transpose(1, 0, 2).reshape(rows, -1)
    return finish(attn, resid, out_weight, norm_gain, gate_up, down_w, tok_groups)


def finish(attn, resid, out_weight, norm_gain, gate_up, down_w, tok_groups):
    rows = resid.shape[0]
    n_tp = lax.axis_size("tp")
    share = rows // n_tp
    my_first = lax.axis_index("tp") * share
    proj = lax.psum_scatter(
        jnp.dot(attn, out_weight, preferred_element_type=jnp.float32).astype(jnp.bfloat16),
        "tp",
        scatter_dimension=0,
        tiled=True,
    ).astype(jnp.float32)
    my_resid = lax.dynamic_slice_in_dim(resid, my_first, share, 0)
    my_stream = (my_resid.astype(jnp.float32) + proj).astype(jnp.bfloat16)
    normed = normalize(my_stream, norm_gain)
    normed = lax.all_gather(normed, "sp", axis=0, axis_index_groups=tok_groups, tiled=False)
    normed = lax.all_gather(normed, "tp", axis=0, tiled=False)
    normed = normed.reshape(n_tp * SPLIT * share, -1)
    both = jnp.dot(normed, gate_up, preferred_element_type=jnp.float32)
    gate, up_part = jnp.split(both, 2, axis=1)
    hidden = (jax.nn.silu(gate) * up_part).astype(jnp.bfloat16)
    down = jnp.dot(hidden, down_w, preferred_element_type=jnp.float32).astype(jnp.bfloat16)
    down = lax.psum_scatter(down, "tp", scatter_dimension=0, tiled=True)
    down = lax.all_to_all(
        down.reshape(SPLIT, share, -1), "sp", 0, 0, axis_index_groups=tok_groups, tiled=True
    )
    down = jnp.sum(down.astype(jnp.float32), axis=0)
    return (my_stream.astype(jnp.float32) + 0.5 * down).astype(jnp.bfloat16)


def solution(mesh):
    placed = (
        P("sp", None),
        P("sp", "tp"),
        P("sp", "tp"),
        P("sp", "tp"),
        P(),
        P(),
        P("tp", None),
        P(),
        P("sp", "tp"),
        P("sp", "tp"),
        P("tp", "sp"),
    )
    return jax.shard_map(
        body, mesh=mesh, in_specs=placed, out_specs=P(("sp", "tp"), None), check_vma=False
    )
```

```python
import functools
import math

import jax
import jax.numpy as jnp
import numpy as np
from jax import lax
from jax.experimental import pallas as pl
from jax.experimental.pallas import tpu as pltpu
from jax.sharding import PartitionSpec as P

GRID_W = 64


EPSILON = 1e-06


def rotate(values, positions):
    dim_size = values.shape[-1]
    half_dim = dim_size // 2
    quarter = half_dim // 2
    inverse = 10000.0 ** (-jnp.arange(quarter, dtype=jnp.float32) / quarter)
    outputs = []
    for axis_pos, coords in enumerate((positions // GRID_W, positions % GRID_W)):
        angles = coords.astype(jnp.float32)[:, None] * inverse[None, :]
        cosine = jnp.cos(angles)[:, None, :]
        sine = jnp.sin(angles)[:, None, :]
        section = values[..., axis_pos * half_dim : (axis_pos + 1) * half_dim]
        first_half = section[..., :quarter]
        second_half = section[..., quarter:]
        outputs += [
            first_half * cosine - second_half * sine,
            second_half * cosine + first_half * sine,
        ]
    return jnp.concatenate(outputs, axis=-1)


def prepare(projected, gain, positions):
    values = projected.astype(jnp.float32)
    normed = values * lax.rsqrt(jnp.mean(values * values, axis=-1, keepdims=True) + EPSILON) * gain
    return rotate(normed, positions).astype(jnp.bfloat16)


def normalize(stream, gain):
    values = stream.astype(jnp.float32)
    return (
        values * lax.rsqrt(jnp.mean(values * values, axis=-1, keepdims=True) + EPSILON) * gain
    ).astype(jnp.bfloat16)


def whole_body(
    resid,
    query,
    key,
    value,
    q_gain,
    k_gain,
    out_weight,
    norm_gain,
    gate_weight,
    up_weight,
    down_weight,
):
    rows_here = query.shape[0]
    head_dim = q_gain.shape[0]
    heads_here = query.shape[1] // head_dim
    kv_here = key.shape[1] // head_dim
    group_size = heads_here // kv_here
    score_scale = head_dim ** (-0.5)
    positions = lax.axis_index("sp") * rows_here + jnp.arange(rows_here, dtype=jnp.int32)
    q_rot = prepare(query.reshape(rows_here, heads_here, head_dim), q_gain, positions)
    k_rot = prepare(key.reshape(rows_here, kv_here, head_dim), k_gain, positions)
    val_rows = value.reshape(rows_here, kv_here, head_dim)
    grouped = q_rot.reshape(rows_here, kv_here, group_size, head_dim)

    def key_block(carry, block):
        maxima, totals, accum = carry
        block_keys, block_vals = block
        scores = (
            jnp.einsum("qkgd,skd->kgqs", grouped, block_keys, preferred_element_type=jnp.float32)
            * score_scale
        )
        new_max = jnp.maximum(maxima, jnp.max(scores, axis=-1))
        shrink = jnp.exp(maxima - new_max)
        weights = jnp.exp(scores - new_max[..., None])
        totals = totals * shrink + jnp.sum(weights, axis=-1)
        accum = accum * shrink[..., None] + jnp.einsum(
            "kgqs,skd->kgqd",
            weights.astype(jnp.bfloat16),
            block_vals,
            preferred_element_type=jnp.float32,
        )
        return ((new_max, totals, accum), None)

    start_max = jnp.full((kv_here, group_size, rows_here), -1e30, jnp.float32)
    start_total = jnp.zeros((kv_here, group_size, rows_here), jnp.float32)
    start_accum = jnp.zeros((kv_here, group_size, rows_here, head_dim), jnp.float32)
    carry = (start_max, start_total, start_accum)
    key_part = lax.all_gather(k_rot, "sp", axis=0, tiled=True)
    val_part = lax.all_gather(val_rows, "sp", axis=0, tiled=True)
    length = key_part.shape[0]
    factor = 4
    span = rows_here * factor
    turns = length // span
    key_blocks = key_part.reshape(turns, span, kv_here, head_dim)
    val_blocks = val_part.reshape(turns, span, kv_here, head_dim)
    carry, _ = lax.scan(key_block, carry, (key_blocks, val_blocks))
    maxima, totals, accum = carry
    attn = (
        jnp.transpose(accum / totals[..., None], (2, 0, 1, 3))
        .reshape(rows_here, heads_here * head_dim)
        .astype(jnp.bfloat16)
    )
    share = rows_here // lax.axis_size("tp")
    my_first = lax.axis_index("tp") * share
    proj = lax.psum_scatter(
        jnp.dot(attn, out_weight, preferred_element_type=jnp.float32).astype(jnp.bfloat16),
        "tp",
        scatter_dimension=0,
        tiled=True,
    ).astype(jnp.float32)
    my_resid = lax.dynamic_slice_in_dim(resid, my_first, share, 0)
    my_stream = (my_resid.astype(jnp.float32) + proj).astype(jnp.bfloat16)
    mixer_rows = lax.all_gather(normalize(my_stream, norm_gain), "tp", axis=0, tiled=True)

    def add_rows(shard_rows):
        return jnp.dot(mixer_rows, shard_rows, preferred_element_type=jnp.float32)

    gate = add_rows(lax.all_gather(gate_weight, "sp", axis=0, tiled=True))
    up_part = add_rows(lax.all_gather(up_weight, "sp", axis=0, tiled=True))
    hidden = (jax.nn.silu(gate) * up_part).astype(jnp.bfloat16)
    down_whole = lax.all_gather(down_weight, "sp", axis=1, tiled=True)
    down = lax.psum_scatter(
        jnp.dot(hidden, down_whole, preferred_element_type=jnp.float32).astype(jnp.bfloat16),
        "tp",
        scatter_dimension=0,
        tiled=True,
    ).astype(jnp.float32)
    return (my_stream.astype(jnp.float32) + 0.5 * down).astype(jnp.bfloat16)


SPLIT = 4


def fits(n_sp, kv_here, hidden_here):
    return n_sp % SPLIT == 0 and kv_here % SPLIT == 0 and hidden_here % (64 * SPLIT) == 0


def groups_of(n_sp):
    ranks = n_sp // SPLIT
    tokens = [[part * ranks + rank for part in range(SPLIT)] for rank in range(ranks)]
    hidden = [[part * ranks + rank for rank in range(ranks)] for part in range(SPLIT)]
    return tokens, hidden


MESH = pl.DeviceIdType.MESH


def layer_kernel(
    ranks,
    head_dim,
    key_ref,
    value_ref,
    query_ref,
    k_gain_ref,
    q_gain_ref,
    freq_ref,
    gate_hbm,
    up_hbm,
    down_ref,
    ow_hbm,
    resid_ref,
    gain_ref,
    out_hbm,
    out_ref,
    kvb,
    qb,
    asend,
    ab,
    wgu,
    wdn,
    pj,
    prv,
    nb,
    st,
    hb,
    dsb,
    drv,
    ds2,
    dzb,
    kv_ref,
    q_ref,
    gu_ref,
    gate_ref,
    up_ref,
    ow_ref,
    local_sem,
    kvp_s, q_s, qz_s, gz_s, dz_s, np_s, gx_s, dx_s, gh_s, dh_s, dp_s, fz_s, pj_s, pj_r, gh_r,
    kvp_r, q_r, qz_r, at_r, gz_r, dz_r, np_r, dh_r,
    gx_r, dx_r, dp_r, at_s, kvz_s, kvz_r, nz_s, nz_r, fz_r,
):
    sp = lax.axis_index("sp")
    core = lax.axis_index("tp")
    part = sp // ranks
    rank = sp % ranks
    rows = q_ref.shape[1]
    share = rows // 2
    depth = gu_ref.shape[1]
    width = down_ref.shape[0] // SPLIT
    cols = down_ref.shape[1]
    group = q_ref.shape[2] // head_dim
    other = 1 - core
    flips = (1, 2, 3)
    last = SPLIT - 1

    def flip(e):
        x = rank % 2
        y = rank // 2
        nx = 1 - x if e % 2 else x
        ny = 1 - y if e // 2 else y
        return ny * 2 + nx

    def near(e):
        return part * ranks + flip(e)

    def at_part(target):
        return target * ranks + rank

    def dn_own(index):
        return down_ref.at[pl.ds(pl.multiple_of(index * width, 16), width)]

    barrier = pltpu.get_barrier_semaphore()
    for dz in range(1, SPLIT):
        pl.semaphore_signal(barrier, inc=1, device_id=(at_part((part + dz) % SPLIT), core), device_id_type=MESH)
    for e in flips:
        pl.semaphore_signal(barrier, inc=1, device_id=(near(e), core), device_id_type=MESH)
    pl.semaphore_signal(barrier, inc=1, device_id=(sp, other), device_id_type=MESH)

    loads = [
        pltpu.make_async_copy(gate_hbm, gate_ref, local_sem.at[4]),
        pltpu.make_async_copy(up_hbm, up_ref, local_sem.at[5]),
        pltpu.make_async_copy(ow_hbm, ow_ref, local_sem.at[6]),
    ]
    for copy in loads:
        copy.start()

    lane = lax.broadcasted_iota(jnp.int32, (rows, head_dim), 1)
    spot = sp * rows + lax.broadcasted_iota(jnp.int32, (rows, head_dim), 0)
    grid_bits = GRID_W.bit_length() - 1
    coords = jnp.where(lane < head_dim // 2, spot >> grid_bits, spot & (GRID_W - 1))
    angles = coords.astype(jnp.float32) * freq_ref[...]
    first_half = (lane & (head_dim // 2 - 1)) < head_dim // 4
    cosine = jnp.cos(angles)
    sine = jnp.where(first_half, -jnp.sin(angles), jnp.sin(angles))

    def turn(ref, head, gain):
        x = ref[:, head * head_dim : (head + 1) * head_dim].astype(jnp.float32)
        x = x * lax.rsqrt(jnp.mean(x * x, axis=-1, keepdims=True) + EPSILON) * gain[...]
        quarter = head_dim // 4
        mate = jnp.where(first_half, pltpu.roll(x, head_dim - quarter, 1), pltpu.roll(x, quarter, 1))
        return (x * cosine + mate * sine).astype(jnp.bfloat16)

    def send(src, dst, s_sem, r_sem, target):
        copy = pltpu.make_async_remote_copy(
            src_ref=src, dst_ref=dst, send_sem=s_sem, recv_sem=r_sem, device_id=target, device_id_type=MESH
        )
        copy.start()

    def landed(dst, s_sem, r_sem):
        pltpu.make_async_remote_copy(
            src_ref=dst, dst_ref=dst, send_sem=s_sem, recv_sem=r_sem, device_id=(sp, other), device_id_type=MESH
        ).wait_recv()

    def left(src, s_sem, r_sem):
        pltpu.make_async_remote_copy(
            src_ref=src, dst_ref=src, send_sem=s_sem, recv_sem=r_sem, device_id=(sp, other), device_id_type=MESH
        ).wait_send()

    def gu_at(source, first=0, count=None):
        return wgu.at[pl.ds(pl.multiple_of(source * depth + first, 16), depth if count is None else count)]

    def dn_at(source, first=0, count=None):
        return wdn.at[pl.ds(first, width if count is None else count), pl.ds(pl.multiple_of(source * cols, cols), cols)]

    for index in range(SPLIT):
        kv_ref[index, :, 0:head_dim] = turn(key_ref, index, k_gain_ref)
        kv_ref[index, :, head_dim : 2 * head_dim] = value_ref[:, index * head_dim : (index + 1) * head_dim]

    pl.semaphore_wait(barrier, SPLIT - 1 + 3 + 1)

    ways = ((part < last, 1), (part > 0, -1))
    kv_ways = (part < last - 1, part > 1)
    at_end = (part == 0) | (part == last)
    inner = (part > 0) & (part < last)
    inward = jnp.where(part == 0, 1, last - 1)
    outward = jnp.where(part == 1, 0, last)

    def kv_on(way, step, source, piece, src=None):
        slot = kvb.at[source, piece]
        send(
            slot if src is None else src,
            slot,
            kvz_s.at[way, step, piece],
            kvz_r.at[way, step, piece],
            (sp + ranks * ways[way][1], core),
        )

    own_kv = kv_ref.at[rank]
    for e in flips:
        send(kv_ref.at[flip(e)], kvb.at[part, rank], kvp_s, kvp_r.at[e], (near(e), core))
    for way in (0, 1):

        @pl.when(kv_ways[way])
        def _():
            kv_on(way, 0, part, rank, own_kv)

    locals_ = [
        pltpu.make_async_copy(own_kv, kvb.at[part, rank], local_sem.at[0]),
        pltpu.make_async_copy(dn_own(part), dn_at(sp), local_sem.at[3]),
    ]
    for copy in locals_:
        copy.start()

    for index in range(SPLIT):
        for head in range(group):
            lanes = slice(head * head_dim, (head + 1) * head_dim)
            q_ref[index, :, lanes] = turn(query_ref, index * group + head, q_gain_ref)
    for e in flips:
        send(q_ref.at[flip(e)], qb.at[0, rank], q_s, q_r.at[e], (near(e), core))
    q_own = pltpu.make_async_copy(q_ref.at[rank], qb.at[0, rank], local_sem.at[1])
    q_own.start()

    loads[0].wait()
    loads[1].wait()
    whole_lanes = width // 128 * 128
    for index in range(SPLIT):
        start = index * width // 128 * 128
        skew = index * width - start
        rests = []
        for which, ref in enumerate((gate_ref, up_ref)):
            block = ref[:, start : start + whole_lanes + 128]
            if skew:
                block = pltpu.roll(block.astype(jnp.float32), whole_lanes + 128 - skew, 1).astype(jnp.bfloat16)
            gu_ref[index, :, which * whole_lanes : (which + 1) * whole_lanes] = block[:, :whole_lanes]
            rests.append(block[:, whole_lanes:].astype(jnp.float32))
        spread = lax.broadcasted_iota(jnp.int32, rests[0].shape, 1)
        tail = jnp.where(spread < width - whole_lanes, rests[0], pltpu.roll(rests[1], width - whole_lanes, 1))
        gu_ref[index, :, 2 * whole_lanes :] = tail.astype(jnp.bfloat16)
    gu_own = pltpu.make_async_copy(gu_ref.at[part], gu_at(sp), local_sem.at[2])
    gu_own.start()
    pad = wdn.shape[0] - width
    wdn[pl.ds(width, pad), :] = jnp.zeros((pad, wdn.shape[1]), wdn.dtype)
    for e in (1, 2):
        send(gu_ref.at[part], gu_at(sp), gx_s, gx_r.at[part, e - 1], (near(e), core))

    def own_downs():
        for e in (1, 2):
            send(dn_own(part), dn_at(sp), dx_s, dx_r.at[part, e - 1], (near(e), core))

    @pl.when(inner)
    def _():
        own_downs()


    def gate_to(target):
        @pl.when((target >= 0) & (target < SPLIT))
        def _():
            send(gu_ref.at[target], gu_at(sp), gz_s, gz_r.at[part], (at_part(target), core))

    def down_to(target):
        @pl.when((target >= 0) & (target < SPLIT))
        def _():
            send(dn_own(target), dn_at(sp), dz_s, dz_r.at[part], (at_part(target), core))

    def gu_pass(source):
        place = gu_at(at_part(source))
        landed(place, gz_s, gz_r.at[source])
        for e in (1, 2):
            send(place, place, gx_s, gx_r.at[source, e - 1], (near(e), core))

    def dn_pass(source):
        place = dn_at(at_part(source))
        landed(place, dz_s, dz_r.at[source])
        for e in (1, 2):
            send(place, place, dx_s, dx_r.at[source, e - 1], (near(e), core))

    def gu_halves(source):
        for e in (1, 2):
            origin = source * ranks + flip(e)
            landed(gu_at(origin), gx_s, gx_r.at[source, e - 1])
            half = gu_at(origin, (e - 1) * depth // 2, depth // 2)
            send(half, half, gh_s, gh_r, (near(3 - e), core))

    def dn_halves(source):
        for e in (1, 2):
            origin = source * ranks + flip(e)
            landed(dn_at(origin), dx_s, dx_r.at[source, e - 1])
            half = dn_at(origin, (e - 1) * width // 2, width // 2)
            send(half, half, dh_s, dh_r.at[source], (near(3 - e), core))

    def dn_done(source):
        landed(dn_at(source * ranks + flip(3)), dh_s, dh_r.at[source])

    high, odd = part // 2, part % 2
    nears = (part + 1 - 2 * odd, 2 - high, 3 - 3 * high)
    second, third = jnp.where(inner, nears[2], nears[1]), jnp.where(inner, nears[1], nears[2])

    def present(way, step):
        source = part - ways[way][1] * (step + 1)
        return source, (source >= 0) & (source < SPLIT)

    def kv_hop(step):
        for way in (0, 1):
            source, there = present(way, step)

            @pl.when(there & inner)
            def _():
                for piece in range(ranks):
                    landed(kvb.at[source, piece], kvz_s.at[way, step, piece], kvz_r.at[way, step, piece])
                    if step == 0:

                        @pl.when(kv_ways[way])
                        def _():
                            kv_on(way, 1, source, piece)

    @pl.when(inner)
    def _():
        gate_to(outward)
        down_to(outward)

    for e in flips:
        landed(kvb.at[part, flip(e)], kvp_s, kvp_r.at[e])
        for way in (0, 1):

            @pl.when(kv_ways[way])
            def _():
                kv_on(way, 0, part, flip(e))


    @pl.when(at_end)
    def _():
        gate_to(nears[0])

    locals_[0].wait()
    q_own.wait()
    for e in flips:
        landed(qb.at[0, flip(e)], q_s, q_r.at[e])

    factor = head_dim ** (-0.5) * math.log2(math.e)
    length = SPLIT * ranks * rows

    def attend(plane, piece, target):
        @pl.loop(0, group)
        def _(head):
            lanes = pl.ds(pl.multiple_of(head * head_dim, head_dim), head_dim)
            q = qb[plane, piece, :, lanes]
            keys = kvb[:, :, :, pl.ds(0, head_dim)].reshape(length, head_dim)
            scores = lax.dot_general(q, keys, (((1,), (1,)), ((), ())), preferred_element_type=jnp.float32)
            peak = jnp.max(scores, axis=-1, keepdims=True)
            weights = jnp.exp2((scores - peak) * factor)
            total = jnp.sum(weights, axis=-1, keepdims=True)
            vals = kvb[:, :, :, pl.ds(head_dim, head_dim)].reshape(length, head_dim)
            summed = jnp.dot(weights.astype(jnp.bfloat16), vals, preferred_element_type=jnp.float32)
            target[:, lanes] = (summed / total).astype(jnp.bfloat16)

    def attend_away(piece):
        attend(1, piece, asend.at[1, piece])
        send(
            asend.at[1, piece],
            ab.at[rank],
            at_s.at[1, piece],
            at_r.at[rank],
            (outward * ranks + piece, core),
        )


    @pl.when(at_end)
    def _():
        for piece in range(ranks):
            slot = qb.at[0, piece]
            send(slot, qb.at[1, piece], qz_s, qz_r.at[piece], (at_part(inward), core))
        gate_to(nears[1])
        gate_to(nears[2])
        down_to(nears[0])
        gu_pass(nears[0])
        gu_halves(part)
        gu_halves(nears[0])
        dn_pass(nears[0])
        gu_pass(second)

    @pl.when(inner)
    def _():
        kv_hop(0)
        gate_to(nears[2])
        gu_halves(part)
        dn_halves(part)
        kv_hop(1)
        def attend_near(turn_by):
            piece = (rank + turn_by) % ranks
            attend(0, piece, asend.at[0, piece])
            send(
                asend.at[0, piece],
                ab.at[rank],
                at_s.at[0, piece],
                at_r.at[rank],
                (part * ranks + piece, core),
            )

        gu_pass(nears[0])

        @pl.loop(1, 4)
        def _(turn_by):
            attend_near(turn_by)

        gate_to(nears[1])
        for piece in range(ranks):
            landed(qb.at[1, piece], qz_s, qz_r.at[piece])

        @pl.loop(0, 3)
        def _(piece):
            attend_away(piece)

        gu_halves(nears[0])
        gu_pass(second)
        down_to(nears[2])
        down_to(nears[1])
        attend_away(3)
        attend(0, rank, ab.at[rank])

    loads[2].wait()
    for e in flips:
        landed(ab.at[flip(e)], at_s.at[0, flip(e)], at_r.at[flip(e)])

    @pl.when(at_end)
    def _():
        landed(ab.at[rank], at_s.at[0, rank], at_r.at[rank])

    attn = jnp.concatenate([ab[index] for index in range(SPLIT)], axis=1)
    tile = 512
    for first in range(0, ow_ref.shape[1], tile):
        block = jnp.dot(attn, ow_ref[:, first : first + tile], preferred_element_type=jnp.float32)
        pj[:, :, first : first + tile] = block.astype(jnp.bfloat16).reshape(2, share, tile)
    send(pj.at[other], prv, pj_s, pj_r, (sp, other))
    landed(prv, pj_s, pj_r)
    proj = pj[core].astype(jnp.float32) + prv[...].astype(jnp.float32)
    stream = (resid_ref[pl.ds(pl.multiple_of(core * share, 16), share)].astype(jnp.float32) + proj).astype(jnp.bfloat16)
    st[...] = stream
    wide = stream.astype(jnp.float32)
    level = lax.rsqrt(jnp.mean(wide * wide, axis=-1, keepdims=True) + EPSILON)
    nb[part, core] = (wide * level * gain_ref[...]).astype(jnp.bfloat16)

    def step_on(source, step, way):
        slot = nb.at[source, core]

        @pl.when(ways[way][0])
        def _():
            send(slot, slot, nz_s.at[way, step], nz_r.at[way, step], (sp + ranks * ways[way][1], core))

    step_on(part, 0, 0)
    step_on(part, 0, 1)
    mine = nb.at[part, core]
    send(mine, mine, np_s, np_r.at[part], (sp, other))

    def hop(step, chosen=(True, True)):
        for way in (0, 1):
            source, there = present(way, step)

            @pl.when(there & chosen[way])
            def _():
                slot = nb.at[source, core]
                landed(slot, nz_s.at[way, step], nz_r.at[way, step])
                if step < SPLIT - 2:
                    step_on(source, step + 1, way)
                send(slot, slot, np_s, np_r.at[source], (sp, other))

    outer = (at_end | (high == 0), at_end | (high == 1))
    across = (inner & (high == 1), inner & (high == 0))

    main = width // 128 * 128
    half_lane = width - main

    def feed(source):
        landed(nb.at[source, other], np_s, np_r.at[source])
        x = nb[source].reshape(rows, nb.shape[-1])
        gate = jnp.dot(x, wgu[:, pl.ds(0, main)], preferred_element_type=jnp.float32)
        up = jnp.dot(x, wgu[:, pl.ds(main, main)], preferred_element_type=jnp.float32)
        hb[source, :, 0:main] = (gate / (1.0 + jnp.exp(-gate)) * up).astype(jnp.bfloat16)
        rest = jnp.dot(x, wgu[:, pl.ds(2 * main, 128)], preferred_element_type=jnp.float32)
        turned = pltpu.roll(rest, half_lane, 1)
        where = lax.broadcasted_iota(jnp.int32, rest.shape, 1)
        tail = jnp.where(where < half_lane, rest / (1.0 + jnp.exp(-rest)) * turned, 0.0)
        hb[source, :, main : main + 128] = tail.astype(jnp.bfloat16)

    edge = jnp.where(inner, nears[0], part)
    order = nears + (part,)
    wide_cols = ranks * cols
    first_cols, later_cols = (1, 2), (0, 3)

    def pair_sum(b, place):
        landed(drv.at[b, place], dp_s, dp_r.at[b, place])
        return dsb[b, order[place], core].astype(jnp.float32) + drv[b, place].astype(jnp.float32)

    def onward(blocks, place, first):
        target = order[place]
        way = 1 - (target > part).astype(jnp.int32)
        for b in blocks:
            total = pair_sum(b, place)
            if not first:
                landed(dzb.at[b, way, target], fz_s, fz_r.at[b, way, target])
                total = total + dzb[b, way, target].astype(jnp.float32)
            ds2[b, target] = total.astype(jnp.bfloat16)
            send(
                ds2.at[b, target],
                dzb.at[b, way, target],
                fz_s,
                fz_r.at[b, way, target],
                (sp + ranks * (1 - 2 * way), core),
            )

    def stage(blocks, place):
        target = order[place]
        for b in blocks:
            block = jnp.dot(hb[target], wdn[:, b * wide_cols : (b + 1) * wide_cols], preferred_element_type=jnp.float32)
            dsb[b, target] = block.astype(jnp.bfloat16).reshape(2, share, wide_cols)
            send(dsb.at[b, target, other], drv.at[b, place], dp_s, dp_r.at[b, place], (sp, other))

    def ends_on(blocks, place):
        @pl.when(at_end)
        def _():
            onward(blocks, place, True)

    gu_halves(second)
    gu_pass(third)
    hop(0, outer)

    @pl.when(at_end)
    def _():
        down_to(nears[1])
        down_to(nears[2])

    gu_halves(third)
    dn_pass(nears[1])

    @pl.when(at_end)
    def _():
        dn_halves(nears[0])
        own_downs()

    @pl.when(inner)
    def _():
        dn_pass(nears[0])

    gu_own.wait()
    landed(gu_at(0, 0, ranks * depth), gh_s, gh_r)
    feed(nears[0])
    hop(0, across)
    feed(part)
    dn_halves(nears[1])
    locals_[1].wait()
    dn_done(jnp.where(inner, part, nears[0]))
    dn_done(nears[1])
    stage(first_cols, 0)
    stage(first_cols, 3)
    ends_on(first_cols, 0)
    hop(1)
    dn_halves(edge)
    dn_pass(nears[2])
    feed(nears[1])
    stage(first_cols, 1)
    ends_on(first_cols, 1)
    hop(2)
    feed(nears[2])
    stage(first_cols, 2)
    dn_halves(nears[2])
    ends_on(first_cols, 2)

    @pl.when(inner)
    def _():
        onward(first_cols, 1, False)

    dn_done(edge)
    dn_done(nears[2])
    stage(later_cols, 2)
    stage(later_cols, 1)
    ends_on(later_cols, 2)
    stage(later_cols, 0)
    ends_on(later_cols, 1)
    stage(later_cols, 3)
    ends_on(later_cols, 0)

    @pl.when(inner)
    def _():
        for blocks, place in ((first_cols, 2), (first_cols, 0), (later_cols, 2), (later_cols, 0), (later_cols, 1)):
            onward(blocks, place, False)

    for b in first_cols + later_cols:
        lanes = slice(b * wide_cols, (b + 1) * wide_cols)
        acc = pair_sum(b, last)
        base = st[:, lanes].astype(jnp.float32)

        def add(way, value, b=b):
            landed(dzb.at[b, way, part], fz_s, fz_r.at[b, way, part])
            return value + dzb[b, way, part].astype(jnp.float32)

        @pl.when(part == 0)
        def _():
            out_ref[:, lanes] = (base + 0.5 * add(1, acc)).astype(jnp.bfloat16)

        @pl.when(part == last)
        def _():
            out_ref[:, lanes] = (base + 0.5 * add(0, acc)).astype(jnp.bfloat16)

        @pl.when(inner)
        def _():
            out_ref[:, lanes] = (base + 0.5 * add(1, add(0, acc))).astype(jnp.bfloat16)

        pltpu.make_async_copy(out_ref.at[:, lanes], out_hbm.at[:, lanes], local_sem.at[7 + b]).start()

    left(kv_ref.at[pl.ds(0, last)], kvp_s, kvp_r.at[1])
    left(q_ref.at[pl.ds(0, last)], q_s, q_r.at[1])
    left(gu_ref.at[pl.ds(0, last)], gz_s, gz_r.at[0])
    left(down_ref.at[pl.ds(0, last * width)], dz_s, dz_r.at[0])
    left(gu_at(0, 0, 2 * ranks * depth), gx_s, gx_r.at[0, 0])
    left(gu_at(0, 0, ranks * depth), gh_s, gh_r)
    left(wdn.at[pl.ds(0, width), pl.ds(0, 2 * wide_cols)], dx_s, dx_r.at[0, 0])
    left(wdn.at[pl.ds(0, width), pl.ds(0, wide_cols)], dh_s, dh_r.at[0])
    left(prv, pj_s, pj_r)
    left(nb.at[:, 0], np_s, np_r.at[0])
    left(drv, dp_s, dp_r.at[0, 0])
    left(drv.at[pl.ds(0, last)], fz_s, fz_r.at[0, 0, 0])
    for way in (0, 1):
        for step in range(SPLIT - 1):
            source, there = present(way, step - 1)

            @pl.when(ways[way][0] & there)
            def _():
                left(nb.at[source, core], nz_s.at[way, step], nz_r.at[way, step])

            if step < 2:

                @pl.when(kv_ways[way] & there)
                def _():
                    for piece in range(ranks):
                        left(kvb.at[source, piece], kvz_s.at[way, step, piece], kvz_r.at[way, step, piece])

    @pl.when(at_end)
    def _():
        left(qb.at[0], qz_s, qz_r.at[0])

    @pl.when(inner)
    def _():
        for piece in range(ranks):
            left(asend.at[1, piece], at_s.at[1, piece], at_r.at[rank])
        for e in flips:
            left(asend.at[0, flip(e)], at_s.at[0, flip(e)], at_r.at[rank])

    for b in range(SPLIT):
        lanes = slice(b * wide_cols, (b + 1) * wide_cols)
        pltpu.make_async_copy(out_ref.at[:, lanes], out_hbm.at[:, lanes], local_sem.at[7 + b]).wait()


def run_layer(key, value, query, k_gain, q_gain, gate, up, down, out_weight, resid, gain, ranks):
    rows = query.shape[0]
    share = rows // 2
    model = resid.shape[1]
    width = down.shape[0] // SPLIT
    depth = gate.shape[0]
    head_dim = q_gain.shape[0]
    n_sp = ranks * SPLIT
    quarter = head_dim // 4
    steps = np.tile(np.arange(quarter, dtype=np.float32), 4)
    freq = jnp.asarray((np.float64(10000.0) ** (-steps / quarter)).astype(np.float32))[None, :]
    half = jnp.bfloat16
    dma = pltpu.SemaphoreType.DMA
    padded = -(-width // 128) * 128
    some = model // SPLIT
    anywhere = pl.BlockSpec(memory_space=pl.ANY)
    inside = pl.BlockSpec(memory_space=pltpu.VMEM)
    kv_shape = (SPLIT, rows, 2 * head_dim)
    q_shape = (SPLIT, rows, query.shape[1] // SPLIT)
    return pl.pallas_call(
        functools.partial(layer_kernel, ranks, head_dim),
        out_shape=jax.ShapeDtypeStruct((share, model), half),
        in_specs=[inside] * 6 + [anywhere] * 4 + [inside] * 2,
        out_specs=anywhere,
        scratch_shapes=[
            pltpu.VMEM((share, model), half),
            pltpu.VMEM((SPLIT, ranks, rows, 2 * head_dim), half),
            pltpu.VMEM((2, *q_shape), half),
            pltpu.VMEM((2, *q_shape), half),
            pltpu.VMEM(q_shape, half),
            pltpu.VMEM((n_sp * depth, 2 * width), half),
            pltpu.VMEM((padded, model), half),
            pltpu.VMEM((2, share, model), half),
            pltpu.VMEM((share, model), half),
            pltpu.VMEM((SPLIT, 2, share, model), half),
            pltpu.VMEM((share, model), half),
            pltpu.VMEM((SPLIT, rows, padded), half),
            pltpu.VMEM((SPLIT, SPLIT, 2, share, some), half),
            pltpu.VMEM((SPLIT, SPLIT, share, some), half),
            pltpu.VMEM((SPLIT, SPLIT, share, some), half),
            pltpu.VMEM((SPLIT, 2, SPLIT, share, some), half),
            pltpu.VMEM(kv_shape, half),
            pltpu.VMEM(q_shape, half),
            pltpu.VMEM((SPLIT, depth, 2 * width), half),
            pltpu.VMEM(gate.shape, half),
            pltpu.VMEM(up.shape, half),
            pltpu.VMEM(out_weight.shape, half),
            dma((7 + SPLIT,)),
        ]
        + [dma] * 15
        + [dma((SPLIT,))] * 8
        + [dma((SPLIT, 2))] * 2
        + [dma((SPLIT, SPLIT)), dma((2, SPLIT))]
        + [dma((2, 2, ranks))] * 2
        + [dma((2, SPLIT - 1))] * 2
        + [dma((SPLIT, 2, SPLIT))],
        compiler_params=pltpu.CompilerParams(
            collective_id=0, has_side_effects=True, vmem_limit_bytes=62 * 1024 * 1024
        ),
    )(
        key, value, query, k_gain[None, :], q_gain[None, :], freq, gate, up, down, out_weight, resid, gain[None, :]
    )


def in_kernel(n_sp, n_tp, kv_here, head_dim, width):
    return n_sp == 4 * SPLIT and n_tp == 2 and kv_here == SPLIT and head_dim == 128 and width % 128 == 64


def body(
    resid,
    query,
    key,
    value,
    q_gain,
    k_gain,
    out_weight,
    norm_gain,
    gate_weight,
    up_weight,
    down_weight,
):
    rows = query.shape[0]
    head_dim = q_gain.shape[0]
    heads_here = query.shape[1] // head_dim
    kv_here = key.shape[1] // head_dim
    n_sp = lax.axis_size("sp")
    if not fits(n_sp, kv_here, gate_weight.shape[1]):
        return whole_body(
            resid, query, key, value, q_gain, k_gain, out_weight, norm_gain, gate_weight, up_weight, down_weight
        )
    hidden_part = gate_weight.shape[1] // SPLIT
    ranks = n_sp // SPLIT
    if in_kernel(n_sp, lax.axis_size("tp"), kv_here, head_dim, hidden_part):
        return run_layer(
            key, value, query, k_gain, q_gain, gate_weight, up_weight, down_weight, out_weight, resid, norm_gain, ranks
        )
    tok_groups, hid_groups = groups_of(n_sp)
    ranks = n_sp // SPLIT
    group_size = heads_here // kv_here
    kv_part = kv_here // SPLIT

    def swap(array):
        return lax.all_to_all(array, "sp", 0, 0, axis_index_groups=tok_groups, tiled=True)

    def spread(array, axis):
        return lax.all_gather(array, "sp", axis=axis, axis_index_groups=hid_groups, tiled=True)

    positions = lax.axis_index("sp") * rows + jnp.arange(rows, dtype=jnp.int32)
    q_rot = prepare(query.reshape(rows, heads_here, head_dim), q_gain, positions)
    k_rot = prepare(key.reshape(rows, kv_here, head_dim), k_gain, positions)
    cut = lambda a: a.reshape(a.shape[0], SPLIT, -1).transpose(1, 0, 2).reshape(SPLIT * a.shape[0], -1)
    k_rot, val = cut(k_rot), cut(value)
    pair = swap(jnp.concatenate([k_rot, val], axis=1))
    pair = spread(pair, 0)
    q_mine = swap(cut(q_rot))
    width = kv_part * head_dim
    keys = pair[:, :width].reshape(-1, kv_part, head_dim)
    vals = pair[:, width:].reshape(-1, kv_part, head_dim)
    grouped = q_mine.reshape(SPLIT * rows, kv_part, group_size, head_dim)
    gate_up = spread(swap(jnp.concatenate([cut(gate_weight), cut(up_weight)], axis=1)), 0)
    depth = gate_weight.shape[0]
    gate_up = gate_up.reshape(ranks, SPLIT, depth, -1).transpose(1, 0, 2, 3).reshape(n_sp * depth, -1)
    down_w = swap(down_weight)
    part = down_weight.shape[0] // SPLIT
    down_w = down_w.reshape(SPLIT, part, -1)
    down_w = lax.all_gather(down_w, "sp", axis=1, axis_index_groups=hid_groups)
    down_w = jnp.transpose(down_w, (2, 0, 1, 3)).reshape(part, -1)
    scores = jnp.einsum("qkgd,skd->kgqs", grouped, keys, preferred_element_type=jnp.float32) * head_dim ** (-0.5)
    weights = jnp.exp(scores - jnp.max(scores, axis=-1, keepdims=True))
    totals = jnp.sum(weights, axis=-1)
    accum = jnp.einsum("kgqs,skd->kgqd", weights.astype(jnp.bfloat16), vals, preferred_element_type=jnp.float32)
    attn = jnp.transpose(accum / totals[..., None], (2, 0, 1, 3)).astype(jnp.bfloat16).reshape(SPLIT * rows, -1)
    attn = swap(attn).reshape(SPLIT, rows, -1).transpose(1, 0, 2).reshape(rows, -1)
    return finish(attn, resid, out_weight, norm_gain, gate_up, down_w, tok_groups)


def finish(attn, resid, out_weight, norm_gain, gate_up, down_w, tok_groups):
    rows = resid.shape[0]
    n_tp = lax.axis_size("tp")
    share = rows // n_tp
    my_first = lax.axis_index("tp") * share
    proj = lax.psum_scatter(
        jnp.dot(attn, out_weight, preferred_element_type=jnp.float32).astype(jnp.bfloat16),
        "tp",
        scatter_dimension=0,
        tiled=True,
    ).astype(jnp.float32)
    my_resid = lax.dynamic_slice_in_dim(resid, my_first, share, 0)
    my_stream = (my_resid.astype(jnp.float32) + proj).astype(jnp.bfloat16)
    normed = normalize(my_stream, norm_gain)
    normed = lax.all_gather(normed, "sp", axis=0, axis_index_groups=tok_groups, tiled=False)
    normed = lax.all_gather(normed, "tp", axis=0, tiled=False)
    normed = normed.reshape(n_tp * SPLIT * share, -1)
    both = jnp.dot(normed, gate_up, preferred_element_type=jnp.float32)
    gate, up_part = jnp.split(both, 2, axis=1)
    hidden = (jax.nn.silu(gate) * up_part).astype(jnp.bfloat16)
    down = jnp.dot(hidden, down_w, preferred_element_type=jnp.float32).astype(jnp.bfloat16)
    down = lax.psum_scatter(down, "tp", scatter_dimension=0, tiled=True)
    down = lax.all_to_all(
        down.reshape(SPLIT, share, -1), "sp", 0, 0, axis_index_groups=tok_groups, tiled=True
    )
    down = jnp.sum(down.astype(jnp.float32), axis=0)
    return (my_stream.astype(jnp.float32) + 0.5 * down).astype(jnp.bfloat16)


def solution(mesh):
    placed = (
        P("sp", None),
        P("sp", "tp"),
        P("sp", "tp"),
        P("sp", "tp"),
        P(),
        P(),
        P("tp", None),
        P(),
        P("sp", "tp"),
        P("sp", "tp"),
        P("tp", "sp"),
    )
    return jax.shard_map(
        body, mesh=mesh, in_specs=placed, out_specs=P(("sp", "tp"), None), check_vma=False
    )
```

```python
import functools
import math

import jax
import jax.numpy as jnp
import numpy as np
from jax import lax
from jax.experimental import pallas as pl
from jax.experimental.pallas import tpu as pltpu
from jax.sharding import PartitionSpec as P

GRID_W = 64


EPSILON = 1e-06


def rotate(values, positions):
    dim_size = values.shape[-1]
    half_dim = dim_size // 2
    quarter = half_dim // 2
    inverse = 10000.0 ** (-jnp.arange(quarter, dtype=jnp.float32) / quarter)
    outputs = []
    for axis_pos, coords in enumerate((positions // GRID_W, positions % GRID_W)):
        angles = coords.astype(jnp.float32)[:, None] * inverse[None, :]
        cosine = jnp.cos(angles)[:, None, :]
        sine = jnp.sin(angles)[:, None, :]
        section = values[..., axis_pos * half_dim : (axis_pos + 1) * half_dim]
        first_half = section[..., :quarter]
        second_half = section[..., quarter:]
        outputs += [
            first_half * cosine - second_half * sine,
            second_half * cosine + first_half * sine,
        ]
    return jnp.concatenate(outputs, axis=-1)


def prepare(projected, gain, positions):
    values = projected.astype(jnp.float32)
    normed = values * lax.rsqrt(jnp.mean(values * values, axis=-1, keepdims=True) + EPSILON) * gain
    return rotate(normed, positions).astype(jnp.bfloat16)


def normalize(stream, gain):
    values = stream.astype(jnp.float32)
    return (
        values * lax.rsqrt(jnp.mean(values * values, axis=-1, keepdims=True) + EPSILON) * gain
    ).astype(jnp.bfloat16)


def whole_body(
    resid,
    query,
    key,
    value,
    q_gain,
    k_gain,
    out_weight,
    norm_gain,
    gate_weight,
    up_weight,
    down_weight,
):
    rows_here = query.shape[0]
    head_dim = q_gain.shape[0]
    heads_here = query.shape[1] // head_dim
    kv_here = key.shape[1] // head_dim
    group_size = heads_here // kv_here
    score_scale = head_dim ** (-0.5)
    positions = lax.axis_index("sp") * rows_here + jnp.arange(rows_here, dtype=jnp.int32)
    q_rot = prepare(query.reshape(rows_here, heads_here, head_dim), q_gain, positions)
    k_rot = prepare(key.reshape(rows_here, kv_here, head_dim), k_gain, positions)
    val_rows = value.reshape(rows_here, kv_here, head_dim)
    grouped = q_rot.reshape(rows_here, kv_here, group_size, head_dim)

    def key_block(carry, block):
        maxima, totals, accum = carry
        block_keys, block_vals = block
        scores = (
            jnp.einsum("qkgd,skd->kgqs", grouped, block_keys, preferred_element_type=jnp.float32)
            * score_scale
        )
        new_max = jnp.maximum(maxima, jnp.max(scores, axis=-1))
        shrink = jnp.exp(maxima - new_max)
        weights = jnp.exp(scores - new_max[..., None])
        totals = totals * shrink + jnp.sum(weights, axis=-1)
        accum = accum * shrink[..., None] + jnp.einsum(
            "kgqs,skd->kgqd",
            weights.astype(jnp.bfloat16),
            block_vals,
            preferred_element_type=jnp.float32,
        )
        return ((new_max, totals, accum), None)

    start_max = jnp.full((kv_here, group_size, rows_here), -1e30, jnp.float32)
    start_total = jnp.zeros((kv_here, group_size, rows_here), jnp.float32)
    start_accum = jnp.zeros((kv_here, group_size, rows_here, head_dim), jnp.float32)
    carry = (start_max, start_total, start_accum)
    key_part = lax.all_gather(k_rot, "sp", axis=0, tiled=True)
    val_part = lax.all_gather(val_rows, "sp", axis=0, tiled=True)
    length = key_part.shape[0]
    factor = 4
    span = rows_here * factor
    turns = length // span
    key_blocks = key_part.reshape(turns, span, kv_here, head_dim)
    val_blocks = val_part.reshape(turns, span, kv_here, head_dim)
    carry, _ = lax.scan(key_block, carry, (key_blocks, val_blocks))
    maxima, totals, accum = carry
    attn = (
        jnp.transpose(accum / totals[..., None], (2, 0, 1, 3))
        .reshape(rows_here, heads_here * head_dim)
        .astype(jnp.bfloat16)
    )
    share = rows_here // lax.axis_size("tp")
    my_first = lax.axis_index("tp") * share
    proj = lax.psum_scatter(
        jnp.dot(attn, out_weight, preferred_element_type=jnp.float32).astype(jnp.bfloat16),
        "tp",
        scatter_dimension=0,
        tiled=True,
    ).astype(jnp.float32)
    my_resid = lax.dynamic_slice_in_dim(resid, my_first, share, 0)
    my_stream = (my_resid.astype(jnp.float32) + proj).astype(jnp.bfloat16)
    mixer_rows = lax.all_gather(normalize(my_stream, norm_gain), "tp", axis=0, tiled=True)

    def add_rows(shard_rows):
        return jnp.dot(mixer_rows, shard_rows, preferred_element_type=jnp.float32)

    gate = add_rows(lax.all_gather(gate_weight, "sp", axis=0, tiled=True))
    up_part = add_rows(lax.all_gather(up_weight, "sp", axis=0, tiled=True))
    hidden = (jax.nn.silu(gate) * up_part).astype(jnp.bfloat16)
    down_whole = lax.all_gather(down_weight, "sp", axis=1, tiled=True)
    down = lax.psum_scatter(
        jnp.dot(hidden, down_whole, preferred_element_type=jnp.float32).astype(jnp.bfloat16),
        "tp",
        scatter_dimension=0,
        tiled=True,
    ).astype(jnp.float32)
    return (my_stream.astype(jnp.float32) + 0.5 * down).astype(jnp.bfloat16)


SPLIT = 4


def fits(n_sp, kv_here, hidden_here):
    return n_sp % SPLIT == 0 and kv_here % SPLIT == 0 and hidden_here % (64 * SPLIT) == 0


def groups_of(n_sp):
    ranks = n_sp // SPLIT
    tokens = [[part * ranks + rank for part in range(SPLIT)] for rank in range(ranks)]
    hidden = [[part * ranks + rank for rank in range(ranks)] for part in range(SPLIT)]
    return tokens, hidden


MESH = pl.DeviceIdType.MESH


def layer_kernel(
    ranks,
    head_dim,
    key_ref,
    value_ref,
    query_ref,
    k_gain_ref,
    q_gain_ref,
    freq_ref,
    gate_hbm,
    up_hbm,
    down_ref,
    ow_hbm,
    resid_ref,
    gain_ref,
    out_hbm,
    out_ref,
    kvb,
    qb,
    asend,
    ab,
    wgu,
    wdn,
    pj,
    prv,
    nb,
    st,
    hb,
    dsb,
    drv,
    ds2,
    dzb,
    kv_ref,
    q_ref,
    gu_ref,
    gate_ref,
    up_ref,
    ow_ref,
    local_sem,
    kvp_s, q_s, qz_s, gz_s, dz_s, np_s, gx_s, dx_s, gh_s, dh_s, dp_s, fz_s, pj_s, pj_r, gh_r,
    kvp_r, q_r, qz_r, at_r, gz_r, dz_r, np_r, dh_r,
    gx_r, dx_r, dp_r, at_s, kvz_s, kvz_r, nz_s, nz_r, fz_r,
):
    sp = lax.axis_index("sp")
    core = lax.axis_index("tp")
    part = sp // ranks
    rank = sp % ranks
    rows = q_ref.shape[1]
    share = rows // 2
    depth = gu_ref.shape[1]
    width = down_ref.shape[0] // SPLIT
    cols = down_ref.shape[1]
    group = q_ref.shape[2] // head_dim
    other = 1 - core
    flips = (1, 2, 3)
    last = SPLIT - 1

    def flip(e):
        x = rank % 2
        y = rank // 2
        nx = 1 - x if e % 2 else x
        ny = 1 - y if e // 2 else y
        return ny * 2 + nx

    def near(e):
        return part * ranks + flip(e)

    def at_part(target):
        return target * ranks + rank

    def dn_own(index):
        return down_ref.at[pl.ds(pl.multiple_of(index * width, 16), width)]

    barrier = pltpu.get_barrier_semaphore()
    for dz in range(1, SPLIT):
        pl.semaphore_signal(barrier, inc=1, device_id=(at_part((part + dz) % SPLIT), core), device_id_type=MESH)
    for e in flips:
        pl.semaphore_signal(barrier, inc=1, device_id=(near(e), core), device_id_type=MESH)
    pl.semaphore_signal(barrier, inc=1, device_id=(sp, other), device_id_type=MESH)

    loads = [
        pltpu.make_async_copy(gate_hbm, gate_ref, local_sem.at[4]),
        pltpu.make_async_copy(up_hbm, up_ref, local_sem.at[5]),
        pltpu.make_async_copy(ow_hbm, ow_ref, local_sem.at[6]),
    ]
    for copy in loads:
        copy.start()

    lane = lax.broadcasted_iota(jnp.int32, (rows, head_dim), 1)
    spot = sp * rows + lax.broadcasted_iota(jnp.int32, (rows, head_dim), 0)
    grid_bits = GRID_W.bit_length() - 1
    coords = jnp.where(lane < head_dim // 2, spot >> grid_bits, spot & (GRID_W - 1))
    angles = coords.astype(jnp.float32) * freq_ref[...]
    first_half = (lane & (head_dim // 2 - 1)) < head_dim // 4
    cosine = jnp.cos(angles)
    sine = jnp.where(first_half, -jnp.sin(angles), jnp.sin(angles))

    def turn(ref, head, gain):
        x = ref[:, head * head_dim : (head + 1) * head_dim].astype(jnp.float32)
        x = x * lax.rsqrt(jnp.mean(x * x, axis=-1, keepdims=True) + EPSILON) * gain[...]
        quarter = head_dim // 4
        mate = jnp.where(first_half, pltpu.roll(x, head_dim - quarter, 1), pltpu.roll(x, quarter, 1))
        return (x * cosine + mate * sine).astype(jnp.bfloat16)

    def send(src, dst, s_sem, r_sem, target):
        copy = pltpu.make_async_remote_copy(
            src_ref=src, dst_ref=dst, send_sem=s_sem, recv_sem=r_sem, device_id=target, device_id_type=MESH
        )
        copy.start()

    def landed(dst, s_sem, r_sem):
        pltpu.make_async_remote_copy(
            src_ref=dst, dst_ref=dst, send_sem=s_sem, recv_sem=r_sem, device_id=(sp, other), device_id_type=MESH
        ).wait_recv()

    def left(src, s_sem, r_sem):
        pltpu.make_async_remote_copy(
            src_ref=src, dst_ref=src, send_sem=s_sem, recv_sem=r_sem, device_id=(sp, other), device_id_type=MESH
        ).wait_send()

    def gu_at(source, first=0, count=None):
        return wgu.at[pl.ds(pl.multiple_of(source * depth + first, 16), depth if count is None else count)]

    def dn_at(source, first=0, count=None):
        return wdn.at[pl.ds(first, width if count is None else count), pl.ds(pl.multiple_of(source * cols, cols), cols)]

    for index in range(SPLIT):
        kv_ref[index, :, 0:head_dim] = turn(key_ref, index, k_gain_ref)
        kv_ref[index, :, head_dim : 2 * head_dim] = value_ref[:, index * head_dim : (index + 1) * head_dim]

    pl.semaphore_wait(barrier, SPLIT - 1 + 3 + 1)

    ways = ((part < last, 1), (part > 0, -1))
    kv_ways = (part < last - 1, part > 1)
    at_end = (part == 0) | (part == last)
    inner = (part > 0) & (part < last)
    inward = jnp.where(part == 0, 1, last - 1)
    outward = jnp.where(part == 1, 0, last)

    def kv_on(way, step, source, piece, src=None):
        slot = kvb.at[source, piece]
        send(
            slot if src is None else src,
            slot,
            kvz_s.at[way, step, piece],
            kvz_r.at[way, step, piece],
            (sp + ranks * ways[way][1], core),
        )

    own_kv = kv_ref.at[rank]
    for e in flips:
        send(kv_ref.at[flip(e)], kvb.at[part, rank], kvp_s, kvp_r.at[e], (near(e), core))
    for way in (0, 1):

        @pl.when(kv_ways[way])
        def _():
            kv_on(way, 0, part, rank, own_kv)

    locals_ = [
        pltpu.make_async_copy(own_kv, kvb.at[part, rank], local_sem.at[0]),
        pltpu.make_async_copy(dn_own(part), dn_at(sp), local_sem.at[3]),
    ]
    for copy in locals_:
        copy.start()

    for index in range(SPLIT):
        for head in range(group):
            lanes = slice(head * head_dim, (head + 1) * head_dim)
            q_ref[index, :, lanes] = turn(query_ref, index * group + head, q_gain_ref)
    for e in flips:
        send(q_ref.at[flip(e)], qb.at[0, rank], q_s, q_r.at[e], (near(e), core))
    q_own = pltpu.make_async_copy(q_ref.at[rank], qb.at[0, rank], local_sem.at[1])
    q_own.start()

    loads[0].wait()
    loads[1].wait()
    whole_lanes = width // 128 * 128
    for index in range(SPLIT):
        start = index * width // 128 * 128
        skew = index * width - start
        rests = []
        for which, ref in enumerate((gate_ref, up_ref)):
            block = ref[:, start : start + whole_lanes + 128]
            if skew:
                block = pltpu.roll(block.astype(jnp.float32), whole_lanes + 128 - skew, 1).astype(jnp.bfloat16)
            gu_ref[index, :, which * whole_lanes : (which + 1) * whole_lanes] = block[:, :whole_lanes]
            rests.append(block[:, whole_lanes:].astype(jnp.float32))
        spread = lax.broadcasted_iota(jnp.int32, rests[0].shape, 1)
        tail = jnp.where(spread < width - whole_lanes, rests[0], pltpu.roll(rests[1], width - whole_lanes, 1))
        gu_ref[index, :, 2 * whole_lanes :] = tail.astype(jnp.bfloat16)
    gu_own = pltpu.make_async_copy(gu_ref.at[part], gu_at(sp), local_sem.at[2])
    gu_own.start()
    pad = wdn.shape[0] - width
    wdn[pl.ds(width, pad), :] = jnp.zeros((pad, wdn.shape[1]), wdn.dtype)
    for e in (1, 2):
        send(gu_ref.at[part], gu_at(sp), gx_s, gx_r.at[part, e - 1], (near(e), core))

    def own_downs():
        for e in (1, 2):
            send(dn_own(part), dn_at(sp), dx_s, dx_r.at[part, e - 1], (near(e), core))

    @pl.when(inner)
    def _():
        own_downs()


    def gate_to(target):
        @pl.when((target >= 0) & (target < SPLIT))
        def _():
            send(gu_ref.at[target], gu_at(sp), gz_s, gz_r.at[part], (at_part(target), core))

    def down_to(target):
        @pl.when((target >= 0) & (target < SPLIT))
        def _():
            send(dn_own(target), dn_at(sp), dz_s, dz_r.at[part], (at_part(target), core))

    def gu_pass(source):
        place = gu_at(at_part(source))
        landed(place, gz_s, gz_r.at[source])
        for e in (1, 2):
            send(place, place, gx_s, gx_r.at[source, e - 1], (near(e), core))

    def dn_pass(source):
        place = dn_at(at_part(source))
        landed(place, dz_s, dz_r.at[source])
        for e in (1, 2):
            send(place, place, dx_s, dx_r.at[source, e - 1], (near(e), core))

    def gu_halves(source):
        for e in (1, 2):
            origin = source * ranks + flip(e)
            landed(gu_at(origin), gx_s, gx_r.at[source, e - 1])
            half = gu_at(origin, (e - 1) * depth // 2, depth // 2)
            send(half, half, gh_s, gh_r, (near(3 - e), core))

    def dn_halves(source):
        for e in (1, 2):
            origin = source * ranks + flip(e)
            landed(dn_at(origin), dx_s, dx_r.at[source, e - 1])
            half = dn_at(origin, (e - 1) * width // 2, width // 2)
            send(half, half, dh_s, dh_r.at[source], (near(3 - e), core))

    def dn_done(source):
        landed(dn_at(source * ranks + flip(3)), dh_s, dh_r.at[source])

    high, odd = part // 2, part % 2
    nears = (part + 1 - 2 * odd, 2 - high, 3 - 3 * high)
    second, third = jnp.where(inner, nears[2], nears[1]), jnp.where(inner, nears[1], nears[2])

    def present(way, step):
        source = part - ways[way][1] * (step + 1)
        return source, (source >= 0) & (source < SPLIT)

    def kv_hop(step):
        for way in (0, 1):
            source, there = present(way, step)

            @pl.when(there & inner)
            def _():
                for piece in range(ranks):
                    landed(kvb.at[source, piece], kvz_s.at[way, step, piece], kvz_r.at[way, step, piece])
                    if step == 0:

                        @pl.when(kv_ways[way])
                        def _():
                            kv_on(way, 1, source, piece)

    @pl.when(inner)
    def _():
        gate_to(outward)
        down_to(outward)

    for e in flips:
        landed(kvb.at[part, flip(e)], kvp_s, kvp_r.at[e])
        for way in (0, 1):

            @pl.when(kv_ways[way])
            def _():
                kv_on(way, 0, part, flip(e))


    @pl.when(at_end)
    def _():
        gate_to(nears[0])

    locals_[0].wait()
    q_own.wait()
    for e in flips:
        landed(qb.at[0, flip(e)], q_s, q_r.at[e])

    factor = head_dim ** (-0.5) * math.log2(math.e)
    length = SPLIT * ranks * rows

    def attend(plane, piece, target):
        @pl.loop(0, group)
        def _(head):
            lanes = pl.ds(pl.multiple_of(head * head_dim, head_dim), head_dim)
            q = qb[plane, piece, :, lanes]
            keys = kvb[:, :, :, pl.ds(0, head_dim)].reshape(length, head_dim)
            scores = lax.dot_general(q, keys, (((1,), (1,)), ((), ())), preferred_element_type=jnp.float32)
            peak = jnp.max(scores, axis=-1, keepdims=True)
            weights = jnp.exp2((scores - peak) * factor)
            total = jnp.sum(weights, axis=-1, keepdims=True)
            vals = kvb[:, :, :, pl.ds(head_dim, head_dim)].reshape(length, head_dim)
            summed = jnp.dot(weights.astype(jnp.bfloat16), vals, preferred_element_type=jnp.float32)
            target[:, lanes] = (summed / total).astype(jnp.bfloat16)

    def attend_away(piece):
        attend(1, piece, asend.at[1, piece])
        send(
            asend.at[1, piece],
            ab.at[rank],
            at_s.at[1, piece],
            at_r.at[rank],
            (outward * ranks + piece, core),
        )


    @pl.when(at_end)
    def _():
        for piece in range(ranks):
            slot = qb.at[0, piece]
            send(slot, qb.at[1, piece], qz_s, qz_r.at[piece], (at_part(inward), core))
        gate_to(nears[1])
        gate_to(nears[2])
        down_to(nears[0])
        gu_pass(nears[0])
        gu_halves(part)
        gu_halves(nears[0])
        dn_pass(nears[0])
        gu_pass(second)

    @pl.when(inner)
    def _():
        kv_hop(0)
        gate_to(nears[2])
        gu_halves(part)
        dn_halves(part)
        kv_hop(1)
        def attend_near(turn_by):
            piece = (rank + turn_by) % ranks
            attend(0, piece, asend.at[0, piece])
            send(
                asend.at[0, piece],
                ab.at[rank],
                at_s.at[0, piece],
                at_r.at[rank],
                (part * ranks + piece, core),
            )

        gu_pass(nears[0])

        @pl.loop(1, 4)
        def _(turn_by):
            attend_near(turn_by)

        gate_to(nears[1])
        for piece in range(ranks):
            landed(qb.at[1, piece], qz_s, qz_r.at[piece])

        @pl.loop(0, 3)
        def _(piece):
            attend_away(piece)

        gu_halves(nears[0])
        gu_pass(second)
        down_to(nears[2])
        down_to(nears[1])
        attend_away(3)
        attend(0, rank, ab.at[rank])

    loads[2].wait()
    for e in flips:
        landed(ab.at[flip(e)], at_s.at[0, flip(e)], at_r.at[flip(e)])

    @pl.when(at_end)
    def _():
        landed(ab.at[rank], at_s.at[0, rank], at_r.at[rank])

    attn = jnp.concatenate([ab[index] for index in range(SPLIT)], axis=1)
    tile = 512
    for first in range(0, ow_ref.shape[1], tile):
        block = jnp.dot(attn, ow_ref[:, first : first + tile], preferred_element_type=jnp.float32)
        pj[:, :, first : first + tile] = block.astype(jnp.bfloat16).reshape(2, share, tile)
    send(pj.at[other], prv, pj_s, pj_r, (sp, other))
    landed(prv, pj_s, pj_r)
    proj = pj[core].astype(jnp.float32) + prv[...].astype(jnp.float32)
    stream = (resid_ref[pl.ds(pl.multiple_of(core * share, 16), share)].astype(jnp.float32) + proj).astype(jnp.bfloat16)
    st[...] = stream
    wide = stream.astype(jnp.float32)
    level = lax.rsqrt(jnp.mean(wide * wide, axis=-1, keepdims=True) + EPSILON)
    nb[part, core] = (wide * level * gain_ref[...]).astype(jnp.bfloat16)

    half_rows = share // 2

    def rows_of(source, piece):
        return nb.at[source, core, pl.ds(piece * half_rows, half_rows)]

    def step_on(source, step, way, piece):
        slot = rows_of(source, piece)

        @pl.when(ways[way][0])
        def _():
            send(slot, slot, nz_s.at[way, step, piece], nz_r.at[way, step, piece], (sp + ranks * ways[way][1], core))

    for piece in (0, 1):
        step_on(part, 0, 0, piece)
        step_on(part, 0, 1, piece)
    mine = nb.at[part, core]
    send(mine, mine, np_s, np_r.at[part], (sp, other))

    def hop(step, chosen=(True, True)):
        for way in (0, 1):
            source, there = present(way, step)

            @pl.when(there & chosen[way])
            def _():
                for piece in (0, 1):
                    landed(rows_of(source, piece), nz_s.at[way, step, piece], nz_r.at[way, step, piece])
                    if step < SPLIT - 2:
                        step_on(source, step + 1, way, piece)
                slot = nb.at[source, core]
                send(slot, slot, np_s, np_r.at[source], (sp, other))

    outer = (at_end | (high == 0), at_end | (high == 1))
    across = (inner & (high == 1), inner & (high == 0))

    main = width // 128 * 128
    half_lane = width - main

    def feed(source):
        landed(nb.at[source, other], np_s, np_r.at[source])
        x = nb[source].reshape(rows, nb.shape[-1])
        gate = jnp.dot(x, wgu[:, pl.ds(0, main)], preferred_element_type=jnp.float32)
        up = jnp.dot(x, wgu[:, pl.ds(main, main)], preferred_element_type=jnp.float32)
        hb[source, :, 0:main] = (gate / (1.0 + jnp.exp(-gate)) * up).astype(jnp.bfloat16)
        rest = jnp.dot(x, wgu[:, pl.ds(2 * main, 128)], preferred_element_type=jnp.float32)
        turned = pltpu.roll(rest, half_lane, 1)
        where = lax.broadcasted_iota(jnp.int32, rest.shape, 1)
        tail = jnp.where(where < half_lane, rest / (1.0 + jnp.exp(-rest)) * turned, 0.0)
        hb[source, :, main : main + 128] = tail.astype(jnp.bfloat16)

    edge = jnp.where(inner, nears[0], part)
    order = nears + (part,)
    wide_cols = ranks * cols
    planes = (jnp.where(inner, part, nears[0]), edge, nears[1], nears[2])

    def lanes_of(b):
        return pl.ds(pl.multiple_of(b * wide_cols, wide_cols), wide_cols)

    def pair_sum(b, place):
        landed(drv.at[b, place], dp_s, dp_r.at[b, place])
        return dsb[b, order[place], core].astype(jnp.float32) + drv[b, place].astype(jnp.float32)

    def onward(k, place, first):
        b = planes[k]
        target = order[place]
        way = 1 - (target > part).astype(jnp.int32)
        total = pair_sum(b, place)
        if not first:
            landed(dzb.at[b, way, target], fz_s, fz_r.at[b, way, target])
            total = total + dzb[b, way, target].astype(jnp.float32)
        ds2[b, target] = total.astype(jnp.bfloat16)
        send(
            ds2.at[b, target],
            dzb.at[b, way, target],
            fz_s,
            fz_r.at[b, way, target],
            (sp + ranks * (1 - 2 * way), core),
        )

    def stage(k, place):
        b = planes[k]
        target = order[place]
        block = jnp.dot(hb[target], wdn[:, lanes_of(b)], preferred_element_type=jnp.float32)
        dsb[b, target] = block.astype(jnp.bfloat16).reshape(2, share, wide_cols)
        send(dsb.at[b, target, other], drv.at[b, place], dp_s, dp_r.at[b, place], (sp, other))

    def ends_on(*steps):
        @pl.when(at_end)
        def _():
            for k, place in steps:
                onward(k, place, True)

    def inner_on(*steps):
        @pl.when(inner)
        def _():
            for k, place in steps:
                onward(k, place, False)

    gu_halves(second)
    gu_pass(third)
    hop(0, outer)

    @pl.when(at_end)
    def _():
        down_to(nears[1])
        down_to(nears[2])

    gu_halves(third)

    @pl.when(at_end)
    def _():
        dn_halves(nears[0])

    dn_pass(nears[1])

    @pl.when(inner)
    def _():
        dn_pass(nears[0])

    gu_own.wait()
    landed(gu_at(0, 0, ranks * depth), gh_s, gh_r)
    feed(nears[0])
    locals_[1].wait()
    dn_done(planes[0])
    stage(0, 0)
    hop(0, across)
    feed(part)
    dn_halves(nears[1])

    @pl.when(at_end)
    def _():
        own_downs()
        onward(0, 0, True)

    hop(1)
    dn_pass(nears[2])
    feed(nears[1])
    stage(0, 1)
    dn_halves(edge)
    dn_done(nears[1])
    stage(2, 0)
    ends_on((0, 1),)
    stage(2, 1)
    ends_on((2, 0), (2, 1))
    dn_halves(nears[2])
    hop(2)
    feed(nears[2])
    stage(0, 2)
    stage(2, 2)
    dn_done(edge)
    ends_on((0, 2), (2, 2))
    stage(1, 2)
    stage(1, 1)
    ends_on((1, 2),)
    stage(1, 0)
    inner_on((0, 1), (2, 1))
    dn_done(nears[2])
    stage(3, 2)
    stage(3, 1)
    ends_on((3, 2),)
    stage(3, 0)
    ends_on((1, 1), (3, 1))
    stage(0, 3)
    ends_on((1, 0), (3, 0))
    stage(1, 3)
    stage(2, 3)
    stage(3, 3)
    inner_on((0, 2), (2, 2), (2, 0), (0, 0), (1, 2), (3, 2), (3, 0), (1, 0), (1, 1), (3, 1))

    for k in (2, 0, 3, 1):
        b = planes[k]
        lanes = lanes_of(b)
        acc = pair_sum(b, last)
        base = st[:, lanes].astype(jnp.float32)

        def add(way, value, b=b):
            landed(dzb.at[b, way, part], fz_s, fz_r.at[b, way, part])
            return value + dzb[b, way, part].astype(jnp.float32)

        @pl.when(part == 0)
        def _():
            out_ref[:, lanes] = (base + 0.5 * add(1, acc)).astype(jnp.bfloat16)

        @pl.when(part == last)
        def _():
            out_ref[:, lanes] = (base + 0.5 * add(0, acc)).astype(jnp.bfloat16)

        @pl.when(inner)
        def _():
            out_ref[:, lanes] = (base + 0.5 * add(1, add(0, acc))).astype(jnp.bfloat16)

        pltpu.make_async_copy(out_ref.at[:, lanes], out_hbm.at[:, lanes], local_sem.at[7 + k]).start()

    left(kv_ref.at[pl.ds(0, last)], kvp_s, kvp_r.at[1])
    left(q_ref.at[pl.ds(0, last)], q_s, q_r.at[1])
    left(gu_ref.at[pl.ds(0, last)], gz_s, gz_r.at[0])
    left(down_ref.at[pl.ds(0, last * width)], dz_s, dz_r.at[0])
    left(gu_at(0, 0, 2 * ranks * depth), gx_s, gx_r.at[0, 0])
    left(gu_at(0, 0, ranks * depth), gh_s, gh_r)
    left(wdn.at[pl.ds(0, width), pl.ds(0, 2 * wide_cols)], dx_s, dx_r.at[0, 0])
    left(wdn.at[pl.ds(0, width), pl.ds(0, wide_cols)], dh_s, dh_r.at[0])
    left(prv, pj_s, pj_r)
    left(nb.at[:, 0], np_s, np_r.at[0])
    left(drv, dp_s, dp_r.at[0, 0])
    left(drv.at[pl.ds(0, last)], fz_s, fz_r.at[0, 0, 0])
    for way in (0, 1):
        for step in range(SPLIT - 1):
            source, there = present(way, step - 1)

            @pl.when(ways[way][0] & there)
            def _():
                for piece in (0, 1):
                    left(rows_of(source, piece), nz_s.at[way, step, piece], nz_r.at[way, step, piece])

            if step < 2:

                @pl.when(kv_ways[way] & there)
                def _():
                    for piece in range(ranks):
                        left(kvb.at[source, piece], kvz_s.at[way, step, piece], kvz_r.at[way, step, piece])

    @pl.when(at_end)
    def _():
        left(qb.at[0], qz_s, qz_r.at[0])

    @pl.when(inner)
    def _():
        for piece in range(ranks):
            left(asend.at[1, piece], at_s.at[1, piece], at_r.at[rank])
        for e in flips:
            left(asend.at[0, flip(e)], at_s.at[0, flip(e)], at_r.at[rank])

    for k in range(SPLIT):
        lanes = lanes_of(planes[k])
        pltpu.make_async_copy(out_ref.at[:, lanes], out_hbm.at[:, lanes], local_sem.at[7 + k]).wait()


def run_layer(key, value, query, k_gain, q_gain, gate, up, down, out_weight, resid, gain, ranks):
    rows = query.shape[0]
    share = rows // 2
    model = resid.shape[1]
    width = down.shape[0] // SPLIT
    depth = gate.shape[0]
    head_dim = q_gain.shape[0]
    n_sp = ranks * SPLIT
    quarter = head_dim // 4
    steps = np.tile(np.arange(quarter, dtype=np.float32), 4)
    freq = jnp.asarray((np.float64(10000.0) ** (-steps / quarter)).astype(np.float32))[None, :]
    half = jnp.bfloat16
    dma = pltpu.SemaphoreType.DMA
    padded = -(-width // 128) * 128
    some = model // SPLIT
    anywhere = pl.BlockSpec(memory_space=pl.ANY)
    inside = pl.BlockSpec(memory_space=pltpu.VMEM)
    kv_shape = (SPLIT, rows, 2 * head_dim)
    q_shape = (SPLIT, rows, query.shape[1] // SPLIT)
    return pl.pallas_call(
        functools.partial(layer_kernel, ranks, head_dim),
        out_shape=jax.ShapeDtypeStruct((share, model), half),
        in_specs=[inside] * 6 + [anywhere] * 4 + [inside] * 2,
        out_specs=anywhere,
        scratch_shapes=[
            pltpu.VMEM((share, model), half),
            pltpu.VMEM((SPLIT, ranks, rows, 2 * head_dim), half),
            pltpu.VMEM((2, *q_shape), half),
            pltpu.VMEM((2, *q_shape), half),
            pltpu.VMEM(q_shape, half),
            pltpu.VMEM((n_sp * depth, 2 * width), half),
            pltpu.VMEM((padded, model), half),
            pltpu.VMEM((2, share, model), half),
            pltpu.VMEM((share, model), half),
            pltpu.VMEM((SPLIT, 2, share, model), half),
            pltpu.VMEM((share, model), half),
            pltpu.VMEM((SPLIT, rows, padded), half),
            pltpu.VMEM((SPLIT, SPLIT, 2, share, some), half),
            pltpu.VMEM((SPLIT, SPLIT, share, some), half),
            pltpu.VMEM((SPLIT, SPLIT, share, some), half),
            pltpu.VMEM((SPLIT, 2, SPLIT, share, some), half),
            pltpu.VMEM(kv_shape, half),
            pltpu.VMEM(q_shape, half),
            pltpu.VMEM((SPLIT, depth, 2 * width), half),
            pltpu.VMEM(gate.shape, half),
            pltpu.VMEM(up.shape, half),
            pltpu.VMEM(out_weight.shape, half),
            dma((7 + SPLIT,)),
        ]
        + [dma] * 15
        + [dma((SPLIT,))] * 8
        + [dma((SPLIT, 2))] * 2
        + [dma((SPLIT, SPLIT)), dma((2, SPLIT))]
        + [dma((2, 2, ranks))] * 2
        + [dma((2, SPLIT - 1, 2))] * 2
        + [dma((SPLIT, 2, SPLIT))],
        compiler_params=pltpu.CompilerParams(
            collective_id=0, has_side_effects=True, vmem_limit_bytes=62 * 1024 * 1024
        ),
    )(
        key, value, query, k_gain[None, :], q_gain[None, :], freq, gate, up, down, out_weight, resid, gain[None, :]
    )


def in_kernel(n_sp, n_tp, kv_here, head_dim, width):
    return n_sp == 4 * SPLIT and n_tp == 2 and kv_here == SPLIT and head_dim == 128 and width % 128 == 64


def body(
    resid,
    query,
    key,
    value,
    q_gain,
    k_gain,
    out_weight,
    norm_gain,
    gate_weight,
    up_weight,
    down_weight,
):
    rows = query.shape[0]
    head_dim = q_gain.shape[0]
    heads_here = query.shape[1] // head_dim
    kv_here = key.shape[1] // head_dim
    n_sp = lax.axis_size("sp")
    if not fits(n_sp, kv_here, gate_weight.shape[1]):
        return whole_body(
            resid, query, key, value, q_gain, k_gain, out_weight, norm_gain, gate_weight, up_weight, down_weight
        )
    hidden_part = gate_weight.shape[1] // SPLIT
    ranks = n_sp // SPLIT
    if in_kernel(n_sp, lax.axis_size("tp"), kv_here, head_dim, hidden_part):
        return run_layer(
            key, value, query, k_gain, q_gain, gate_weight, up_weight, down_weight, out_weight, resid, norm_gain, ranks
        )
    tok_groups, hid_groups = groups_of(n_sp)
    ranks = n_sp // SPLIT
    group_size = heads_here // kv_here
    kv_part = kv_here // SPLIT

    def swap(array):
        return lax.all_to_all(array, "sp", 0, 0, axis_index_groups=tok_groups, tiled=True)

    def spread(array, axis):
        return lax.all_gather(array, "sp", axis=axis, axis_index_groups=hid_groups, tiled=True)

    positions = lax.axis_index("sp") * rows + jnp.arange(rows, dtype=jnp.int32)
    q_rot = prepare(query.reshape(rows, heads_here, head_dim), q_gain, positions)
    k_rot = prepare(key.reshape(rows, kv_here, head_dim), k_gain, positions)
    cut = lambda a: a.reshape(a.shape[0], SPLIT, -1).transpose(1, 0, 2).reshape(SPLIT * a.shape[0], -1)
    k_rot, val = cut(k_rot), cut(value)
    pair = swap(jnp.concatenate([k_rot, val], axis=1))
    pair = spread(pair, 0)
    q_mine = swap(cut(q_rot))
    width = kv_part * head_dim
    keys = pair[:, :width].reshape(-1, kv_part, head_dim)
    vals = pair[:, width:].reshape(-1, kv_part, head_dim)
    grouped = q_mine.reshape(SPLIT * rows, kv_part, group_size, head_dim)
    gate_up = spread(swap(jnp.concatenate([cut(gate_weight), cut(up_weight)], axis=1)), 0)
    depth = gate_weight.shape[0]
    gate_up = gate_up.reshape(ranks, SPLIT, depth, -1).transpose(1, 0, 2, 3).reshape(n_sp * depth, -1)
    down_w = swap(down_weight)
    part = down_weight.shape[0] // SPLIT
    down_w = down_w.reshape(SPLIT, part, -1)
    down_w = lax.all_gather(down_w, "sp", axis=1, axis_index_groups=hid_groups)
    down_w = jnp.transpose(down_w, (2, 0, 1, 3)).reshape(part, -1)
    scores = jnp.einsum("qkgd,skd->kgqs", grouped, keys, preferred_element_type=jnp.float32) * head_dim ** (-0.5)
    weights = jnp.exp(scores - jnp.max(scores, axis=-1, keepdims=True))
    totals = jnp.sum(weights, axis=-1)
    accum = jnp.einsum("kgqs,skd->kgqd", weights.astype(jnp.bfloat16), vals, preferred_element_type=jnp.float32)
    attn = jnp.transpose(accum / totals[..., None], (2, 0, 1, 3)).astype(jnp.bfloat16).reshape(SPLIT * rows, -1)
    attn = swap(attn).reshape(SPLIT, rows, -1).transpose(1, 0, 2).reshape(rows, -1)
    return finish(attn, resid, out_weight, norm_gain, gate_up, down_w, tok_groups)


def finish(attn, resid, out_weight, norm_gain, gate_up, down_w, tok_groups):
    rows = resid.shape[0]
    n_tp = lax.axis_size("tp")
    share = rows // n_tp
    my_first = lax.axis_index("tp") * share
    proj = lax.psum_scatter(
        jnp.dot(attn, out_weight, preferred_element_type=jnp.float32).astype(jnp.bfloat16),
        "tp",
        scatter_dimension=0,
        tiled=True,
    ).astype(jnp.float32)
    my_resid = lax.dynamic_slice_in_dim(resid, my_first, share, 0)
    my_stream = (my_resid.astype(jnp.float32) + proj).astype(jnp.bfloat16)
    normed = normalize(my_stream, norm_gain)
    normed = lax.all_gather(normed, "sp", axis=0, axis_index_groups=tok_groups, tiled=False)
    normed = lax.all_gather(normed, "tp", axis=0, tiled=False)
    normed = normed.reshape(n_tp * SPLIT * share, -1)
    both = jnp.dot(normed, gate_up, preferred_element_type=jnp.float32)
    gate, up_part = jnp.split(both, 2, axis=1)
    hidden = (jax.nn.silu(gate) * up_part).astype(jnp.bfloat16)
    down = jnp.dot(hidden, down_w, preferred_element_type=jnp.float32).astype(jnp.bfloat16)
    down = lax.psum_scatter(down, "tp", scatter_dimension=0, tiled=True)
    down = lax.all_to_all(
        down.reshape(SPLIT, share, -1), "sp", 0, 0, axis_index_groups=tok_groups, tiled=True
    )
    down = jnp.sum(down.astype(jnp.float32), axis=0)
    return (my_stream.astype(jnp.float32) + 0.5 * down).astype(jnp.bfloat16)


def solution(mesh):
    placed = (
        P("sp", None),
        P("sp", "tp"),
        P("sp", "tp"),
        P("sp", "tp"),
        P(),
        P(),
        P("tp", None),
        P(),
        P("sp", "tp"),
        P("sp", "tp"),
        P("tp", "sp"),
    )
    return jax.shard_map(
        body, mesh=mesh, in_specs=placed, out_specs=P(("sp", "tp"), None), check_vma=False
    )
```

```python
import functools
import math

import jax
import jax.numpy as jnp
import numpy as np
from jax import lax
from jax.experimental import pallas as pl
from jax.experimental.pallas import tpu as pltpu
from jax.sharding import PartitionSpec as P

GRID_W = 64


EPSILON = 1e-06


def rotate(values, positions):
    dim_size = values.shape[-1]
    half_dim = dim_size // 2
    quarter = half_dim // 2
    inverse = 10000.0 ** (-jnp.arange(quarter, dtype=jnp.float32) / quarter)
    outputs = []
    for axis_pos, coords in enumerate((positions // GRID_W, positions % GRID_W)):
        angles = coords.astype(jnp.float32)[:, None] * inverse[None, :]
        cosine = jnp.cos(angles)[:, None, :]
        sine = jnp.sin(angles)[:, None, :]
        section = values[..., axis_pos * half_dim : (axis_pos + 1) * half_dim]
        first_half = section[..., :quarter]
        second_half = section[..., quarter:]
        outputs += [
            first_half * cosine - second_half * sine,
            second_half * cosine + first_half * sine,
        ]
    return jnp.concatenate(outputs, axis=-1)


def prepare(projected, gain, positions):
    values = projected.astype(jnp.float32)
    normed = values * lax.rsqrt(jnp.mean(values * values, axis=-1, keepdims=True) + EPSILON) * gain
    return rotate(normed, positions).astype(jnp.bfloat16)


def normalize(stream, gain):
    values = stream.astype(jnp.float32)
    return (
        values * lax.rsqrt(jnp.mean(values * values, axis=-1, keepdims=True) + EPSILON) * gain
    ).astype(jnp.bfloat16)


def whole_body(
    resid,
    query,
    key,
    value,
    q_gain,
    k_gain,
    out_weight,
    norm_gain,
    gate_weight,
    up_weight,
    down_weight,
):
    rows_here = query.shape[0]
    head_dim = q_gain.shape[0]
    heads_here = query.shape[1] // head_dim
    kv_here = key.shape[1] // head_dim
    group_size = heads_here // kv_here
    score_scale = head_dim ** (-0.5)
    positions = lax.axis_index("sp") * rows_here + jnp.arange(rows_here, dtype=jnp.int32)
    q_rot = prepare(query.reshape(rows_here, heads_here, head_dim), q_gain, positions)
    k_rot = prepare(key.reshape(rows_here, kv_here, head_dim), k_gain, positions)
    val_rows = value.reshape(rows_here, kv_here, head_dim)
    grouped = q_rot.reshape(rows_here, kv_here, group_size, head_dim)

    def key_block(carry, block):
        maxima, totals, accum = carry
        block_keys, block_vals = block
        scores = (
            jnp.einsum("qkgd,skd->kgqs", grouped, block_keys, preferred_element_type=jnp.float32)
            * score_scale
        )
        new_max = jnp.maximum(maxima, jnp.max(scores, axis=-1))
        shrink = jnp.exp(maxima - new_max)
        weights = jnp.exp(scores - new_max[..., None])
        totals = totals * shrink + jnp.sum(weights, axis=-1)
        accum = accum * shrink[..., None] + jnp.einsum(
            "kgqs,skd->kgqd",
            weights.astype(jnp.bfloat16),
            block_vals,
            preferred_element_type=jnp.float32,
        )
        return ((new_max, totals, accum), None)

    start_max = jnp.full((kv_here, group_size, rows_here), -1e30, jnp.float32)
    start_total = jnp.zeros((kv_here, group_size, rows_here), jnp.float32)
    start_accum = jnp.zeros((kv_here, group_size, rows_here, head_dim), jnp.float32)
    carry = (start_max, start_total, start_accum)
    key_part = lax.all_gather(k_rot, "sp", axis=0, tiled=True)
    val_part = lax.all_gather(val_rows, "sp", axis=0, tiled=True)
    length = key_part.shape[0]
    factor = 4
    span = rows_here * factor
    turns = length // span
    key_blocks = key_part.reshape(turns, span, kv_here, head_dim)
    val_blocks = val_part.reshape(turns, span, kv_here, head_dim)
    carry, _ = lax.scan(key_block, carry, (key_blocks, val_blocks))
    maxima, totals, accum = carry
    attn = (
        jnp.transpose(accum / totals[..., None], (2, 0, 1, 3))
        .reshape(rows_here, heads_here * head_dim)
        .astype(jnp.bfloat16)
    )
    share = rows_here // lax.axis_size("tp")
    my_first = lax.axis_index("tp") * share
    proj = lax.psum_scatter(
        jnp.dot(attn, out_weight, preferred_element_type=jnp.float32).astype(jnp.bfloat16),
        "tp",
        scatter_dimension=0,
        tiled=True,
    ).astype(jnp.float32)
    my_resid = lax.dynamic_slice_in_dim(resid, my_first, share, 0)
    my_stream = (my_resid.astype(jnp.float32) + proj).astype(jnp.bfloat16)
    mixer_rows = lax.all_gather(normalize(my_stream, norm_gain), "tp", axis=0, tiled=True)

    def add_rows(shard_rows):
        return jnp.dot(mixer_rows, shard_rows, preferred_element_type=jnp.float32)

    gate = add_rows(lax.all_gather(gate_weight, "sp", axis=0, tiled=True))
    up_part = add_rows(lax.all_gather(up_weight, "sp", axis=0, tiled=True))
    hidden = (jax.nn.silu(gate) * up_part).astype(jnp.bfloat16)
    down_whole = lax.all_gather(down_weight, "sp", axis=1, tiled=True)
    down = lax.psum_scatter(
        jnp.dot(hidden, down_whole, preferred_element_type=jnp.float32).astype(jnp.bfloat16),
        "tp",
        scatter_dimension=0,
        tiled=True,
    ).astype(jnp.float32)
    return (my_stream.astype(jnp.float32) + 0.5 * down).astype(jnp.bfloat16)


SPLIT = 4


def fits(n_sp, kv_here, hidden_here):
    return n_sp % SPLIT == 0 and kv_here % SPLIT == 0 and hidden_here % (64 * SPLIT) == 0


def groups_of(n_sp):
    ranks = n_sp // SPLIT
    tokens = [[part * ranks + rank for part in range(SPLIT)] for rank in range(ranks)]
    hidden = [[part * ranks + rank for rank in range(ranks)] for part in range(SPLIT)]
    return tokens, hidden


MESH = pl.DeviceIdType.MESH


def layer_kernel(
    ranks,
    head_dim,
    key_ref,
    value_ref,
    query_ref,
    k_gain_ref,
    q_gain_ref,
    freq_ref,
    gate_hbm,
    up_hbm,
    down_ref,
    ow_hbm,
    resid_ref,
    gain_ref,
    out_hbm,
    out_ref,
    kvb,
    qb,
    asend,
    ab,
    wgu,
    wdn,
    pj,
    prv,
    nb,
    st,
    hb,
    dsb,
    drv,
    ds2,
    dzb,
    kv_ref,
    q_ref,
    gu_ref,
    gate_ref,
    up_ref,
    ow_ref,
    local_sem,
    kvp_s, q_s, qz_s, gz_s, dz_s, np_s, gx_s, dx_s, gh_s, dh_s, dp_s, fz_s, pj_s, pj_r, gh_r,
    kvp_r, q_r, qz_r, at_r, gz_r, dz_r, np_r, dh_r,
    gx_r, dx_r, dp_r, at_s, kvz_s, kvz_r, nz_s, nz_r, fz_r,
):
    sp = lax.axis_index("sp")
    core = lax.axis_index("tp")
    part = sp // ranks
    rank = sp % ranks
    rows = q_ref.shape[1]
    share = rows // 2
    depth = gu_ref.shape[1]
    width = down_ref.shape[0] // SPLIT
    cols = down_ref.shape[1]
    group = q_ref.shape[2] // head_dim
    other = 1 - core
    flips = (1, 2, 3)
    last = SPLIT - 1

    def flip(e):
        x = rank % 2
        y = rank // 2
        nx = 1 - x if e % 2 else x
        ny = 1 - y if e // 2 else y
        return ny * 2 + nx

    def near(e):
        return part * ranks + flip(e)

    def at_part(target):
        return target * ranks + rank

    def dn_own(index):
        return down_ref.at[pl.ds(pl.multiple_of(index * width, 16), width)]

    barrier = pltpu.get_barrier_semaphore()
    for dz in range(1, SPLIT):
        pl.semaphore_signal(barrier, inc=1, device_id=(at_part((part + dz) % SPLIT), core), device_id_type=MESH)
    for e in flips:
        pl.semaphore_signal(barrier, inc=1, device_id=(near(e), core), device_id_type=MESH)
    pl.semaphore_signal(barrier, inc=1, device_id=(sp, other), device_id_type=MESH)

    loads = [
        pltpu.make_async_copy(gate_hbm, gate_ref, local_sem.at[4]),
        pltpu.make_async_copy(up_hbm, up_ref, local_sem.at[5]),
        pltpu.make_async_copy(ow_hbm, ow_ref, local_sem.at[6]),
    ]
    for copy in loads:
        copy.start()

    lane = lax.broadcasted_iota(jnp.int32, (rows, head_dim), 1)
    spot = sp * rows + lax.broadcasted_iota(jnp.int32, (rows, head_dim), 0)
    grid_bits = GRID_W.bit_length() - 1
    coords = jnp.where(lane < head_dim // 2, spot >> grid_bits, spot & (GRID_W - 1))
    angles = coords.astype(jnp.float32) * freq_ref[...]
    first_half = (lane & (head_dim // 2 - 1)) < head_dim // 4
    cosine = jnp.cos(angles)
    sine = jnp.where(first_half, -jnp.sin(angles), jnp.sin(angles))

    def turn(ref, head, gain):
        x = ref[:, head * head_dim : (head + 1) * head_dim].astype(jnp.float32)
        x = x * lax.rsqrt(jnp.mean(x * x, axis=-1, keepdims=True) + EPSILON) * gain[...]
        quarter = head_dim // 4
        mate = jnp.where(first_half, pltpu.roll(x, head_dim - quarter, 1), pltpu.roll(x, quarter, 1))
        return (x * cosine + mate * sine).astype(jnp.bfloat16)

    def send(src, dst, s_sem, r_sem, target):
        copy = pltpu.make_async_remote_copy(
            src_ref=src, dst_ref=dst, send_sem=s_sem, recv_sem=r_sem, device_id=target, device_id_type=MESH
        )
        copy.start()

    def landed(dst, s_sem, r_sem):
        pltpu.make_async_remote_copy(
            src_ref=dst, dst_ref=dst, send_sem=s_sem, recv_sem=r_sem, device_id=(sp, other), device_id_type=MESH
        ).wait_recv()

    def left(src, s_sem, r_sem):
        pltpu.make_async_remote_copy(
            src_ref=src, dst_ref=src, send_sem=s_sem, recv_sem=r_sem, device_id=(sp, other), device_id_type=MESH
        ).wait_send()

    def gu_at(source, first=0, count=None):
        return wgu.at[pl.ds(pl.multiple_of(source * depth + first, 16), depth if count is None else count)]

    def dn_at(source, first=0, count=None):
        return wdn.at[pl.ds(first, width if count is None else count), pl.ds(pl.multiple_of(source * cols, cols), cols)]

    for index in range(SPLIT):
        kv_ref[index, :, 0:head_dim] = turn(key_ref, index, k_gain_ref)
        kv_ref[index, :, head_dim : 2 * head_dim] = value_ref[:, index * head_dim : (index + 1) * head_dim]

    pl.semaphore_wait(barrier, SPLIT - 1 + 3 + 1)

    ways = ((part < last, 1), (part > 0, -1))
    kv_ways = (part < last - 1, part > 1)
    at_end = (part == 0) | (part == last)
    inner = (part > 0) & (part < last)
    inward = jnp.where(part == 0, 1, last - 1)
    outward = jnp.where(part == 1, 0, last)

    def kv_on(way, step, source, piece, src=None):
        slot = kvb.at[source, piece]
        send(
            slot if src is None else src,
            slot,
            kvz_s.at[way, step, piece],
            kvz_r.at[way, step, piece],
            (sp + ranks * ways[way][1], core),
        )

    own_kv = kv_ref.at[rank]
    for e in flips:
        send(kv_ref.at[flip(e)], kvb.at[part, rank], kvp_s, kvp_r.at[e], (near(e), core))
    for way in (0, 1):

        @pl.when(kv_ways[way])
        def _():
            kv_on(way, 0, part, rank, own_kv)

    locals_ = [
        pltpu.make_async_copy(own_kv, kvb.at[part, rank], local_sem.at[0]),
        pltpu.make_async_copy(dn_own(part), dn_at(sp), local_sem.at[3]),
    ]
    for copy in locals_:
        copy.start()

    for index in range(SPLIT):
        for head in range(group):
            lanes = slice(head * head_dim, (head + 1) * head_dim)
            q_ref[index, :, lanes] = turn(query_ref, index * group + head, q_gain_ref)
    for e in flips:
        send(q_ref.at[flip(e)], qb.at[0, rank], q_s, q_r.at[e], (near(e), core))
    q_own = pltpu.make_async_copy(q_ref.at[rank], qb.at[0, rank], local_sem.at[1])
    q_own.start()

    loads[0].wait()
    loads[1].wait()
    whole_lanes = width // 128 * 128
    for index in range(SPLIT):
        start = index * width // 128 * 128
        skew = index * width - start
        rests = []
        for which, ref in enumerate((gate_ref, up_ref)):
            block = ref[:, start : start + whole_lanes + 128]
            if skew:
                block = pltpu.roll(block.astype(jnp.float32), whole_lanes + 128 - skew, 1).astype(jnp.bfloat16)
            gu_ref[index, :, which * whole_lanes : (which + 1) * whole_lanes] = block[:, :whole_lanes]
            rests.append(block[:, whole_lanes:].astype(jnp.float32))
        spread = lax.broadcasted_iota(jnp.int32, rests[0].shape, 1)
        tail = jnp.where(spread < width - whole_lanes, rests[0], pltpu.roll(rests[1], width - whole_lanes, 1))
        gu_ref[index, :, 2 * whole_lanes :] = tail.astype(jnp.bfloat16)
    gu_own = pltpu.make_async_copy(gu_ref.at[part], gu_at(sp), local_sem.at[2])
    gu_own.start()
    pad = wdn.shape[0] - width
    wdn[pl.ds(width, pad), :] = jnp.zeros((pad, wdn.shape[1]), wdn.dtype)
    for e in (1, 2):
        send(gu_ref.at[part], gu_at(sp), gx_s, gx_r.at[part, e - 1], (near(e), core))

    def own_downs():
        for e in (1, 2):
            send(dn_own(part), dn_at(sp), dx_s, dx_r.at[part, e - 1], (near(e), core))

    @pl.when(inner)
    def _():
        own_downs()


    def gate_to(target):
        @pl.when((target >= 0) & (target < SPLIT))
        def _():
            send(gu_ref.at[target], gu_at(sp), gz_s, gz_r.at[part], (at_part(target), core))

    def down_to(target):
        @pl.when((target >= 0) & (target < SPLIT))
        def _():
            send(dn_own(target), dn_at(sp), dz_s, dz_r.at[part], (at_part(target), core))

    def gu_pass(source):
        place = gu_at(at_part(source))
        landed(place, gz_s, gz_r.at[source])
        for e in (1, 2):
            send(place, place, gx_s, gx_r.at[source, e - 1], (near(e), core))

    def dn_pass(source):
        place = dn_at(at_part(source))
        landed(place, dz_s, dz_r.at[source])
        for e in (1, 2):
            send(place, place, dx_s, dx_r.at[source, e - 1], (near(e), core))

    def gu_halves(source):
        for e in (1, 2):
            origin = source * ranks + flip(e)
            landed(gu_at(origin), gx_s, gx_r.at[source, e - 1])
            half = gu_at(origin, (e - 1) * depth // 2, depth // 2)
            send(half, half, gh_s, gh_r, (near(3 - e), core))

    def dn_halves(source):
        for e in (1, 2):
            origin = source * ranks + flip(e)
            landed(dn_at(origin), dx_s, dx_r.at[source, e - 1])
            half = dn_at(origin, (e - 1) * width // 2, width // 2)
            send(half, half, dh_s, dh_r.at[source], (near(3 - e), core))

    def dn_done(source):
        landed(dn_at(source * ranks + flip(3)), dh_s, dh_r.at[source])

    high, odd = part // 2, part % 2
    nears = (part + 1 - 2 * odd, 2 - high, 3 - 3 * high)
    second, third = jnp.where(inner, nears[2], nears[1]), jnp.where(inner, nears[1], nears[2])

    def present(way, step):
        source = part - ways[way][1] * (step + 1)
        return source, (source >= 0) & (source < SPLIT)

    def kv_hop(step):
        for way in (0, 1):
            source, there = present(way, step)

            @pl.when(there & inner)
            def _():
                for piece in range(ranks):
                    landed(kvb.at[source, piece], kvz_s.at[way, step, piece], kvz_r.at[way, step, piece])
                    if step == 0:

                        @pl.when(kv_ways[way])
                        def _():
                            kv_on(way, 1, source, piece)

    @pl.when(inner)
    def _():
        gate_to(outward)
        down_to(outward)

    for e in flips:
        landed(kvb.at[part, flip(e)], kvp_s, kvp_r.at[e])
        for way in (0, 1):

            @pl.when(kv_ways[way])
            def _():
                kv_on(way, 0, part, flip(e))


    @pl.when(at_end)
    def _():
        gate_to(nears[0])

    locals_[0].wait()
    q_own.wait()
    for e in flips:
        landed(qb.at[0, flip(e)], q_s, q_r.at[e])

    factor = head_dim ** (-0.5) * math.log2(math.e)
    length = SPLIT * ranks * rows

    def attend(plane, piece, target):
        @pl.loop(0, group)
        def _(head):
            lanes = pl.ds(pl.multiple_of(head * head_dim, head_dim), head_dim)
            q = qb[plane, piece, :, lanes]
            keys = kvb[:, :, :, pl.ds(0, head_dim)].reshape(length, head_dim)
            scores = lax.dot_general(q, keys, (((1,), (1,)), ((), ())), preferred_element_type=jnp.float32)
            peak = jnp.max(scores, axis=-1, keepdims=True)
            weights = jnp.exp2((scores - peak) * factor)
            total = jnp.sum(weights, axis=-1, keepdims=True)
            vals = kvb[:, :, :, pl.ds(head_dim, head_dim)].reshape(length, head_dim)
            summed = jnp.dot(weights.astype(jnp.bfloat16), vals, preferred_element_type=jnp.float32)
            target[:, lanes] = (summed / total).astype(jnp.bfloat16)

    def attend_away(piece):
        attend(1, piece, asend.at[1, piece])
        send(
            asend.at[1, piece],
            ab.at[rank],
            at_s.at[1, piece],
            at_r.at[rank],
            (outward * ranks + piece, core),
        )


    @pl.when(at_end)
    def _():
        for piece in range(ranks):
            slot = qb.at[0, piece]
            send(slot, qb.at[1, piece], qz_s, qz_r.at[piece], (at_part(inward), core))
        gate_to(nears[1])
        gate_to(nears[2])
        down_to(nears[0])
        gu_pass(nears[0])
        gu_halves(part)
        gu_halves(nears[0])
        dn_pass(nears[0])
        gu_pass(second)

    @pl.when(inner)
    def _():
        kv_hop(0)
        gate_to(nears[2])
        gu_halves(part)
        dn_halves(part)
        kv_hop(1)
        def attend_near(turn_by):
            piece = (rank + turn_by) % ranks
            attend(0, piece, asend.at[0, piece])
            send(
                asend.at[0, piece],
                ab.at[rank],
                at_s.at[0, piece],
                at_r.at[rank],
                (part * ranks + piece, core),
            )

        gu_pass(nears[0])

        @pl.loop(1, 4)
        def _(turn_by):
            attend_near(turn_by)

        gate_to(nears[1])
        for piece in range(ranks):
            landed(qb.at[1, piece], qz_s, qz_r.at[piece])

        @pl.loop(0, 3)
        def _(piece):
            attend_away(piece)

        gu_halves(nears[0])
        gu_pass(second)
        down_to(nears[2])
        down_to(nears[1])
        attend_away(3)
        attend(0, rank, ab.at[rank])

    loads[2].wait()
    for e in flips:
        landed(ab.at[flip(e)], at_s.at[0, flip(e)], at_r.at[flip(e)])

    @pl.when(at_end)
    def _():
        landed(ab.at[rank], at_s.at[0, rank], at_r.at[rank])

    attn = jnp.concatenate([ab[index] for index in range(SPLIT)], axis=1)
    tile = 512
    for first in range(0, ow_ref.shape[1], tile):
        block = jnp.dot(attn, ow_ref[:, first : first + tile], preferred_element_type=jnp.float32)
        pj[:, :, first : first + tile] = block.astype(jnp.bfloat16).reshape(2, share, tile)
    send(pj.at[other], prv, pj_s, pj_r, (sp, other))
    landed(prv, pj_s, pj_r)
    proj = pj[core].astype(jnp.float32) + prv[...].astype(jnp.float32)
    stream = (resid_ref[pl.ds(pl.multiple_of(core * share, 16), share)].astype(jnp.float32) + proj).astype(jnp.bfloat16)
    st[...] = stream
    wide = stream.astype(jnp.float32)
    level = lax.rsqrt(jnp.mean(wide * wide, axis=-1, keepdims=True) + EPSILON)
    nb[part, core] = (wide * level * gain_ref[...]).astype(jnp.bfloat16)

    half_rows = share // 2

    def rows_of(source, piece):
        return nb.at[source, core, pl.ds(piece * half_rows, half_rows)]

    def step_on(source, step, way, piece):
        slot = rows_of(source, piece)

        @pl.when(ways[way][0])
        def _():
            send(slot, slot, nz_s.at[way, step, piece], nz_r.at[way, step, piece], (sp + ranks * ways[way][1], core))

    for piece in (0, 1):
        step_on(part, 0, 0, piece)
        step_on(part, 0, 1, piece)
    mine = nb.at[part, core]
    send(mine, mine, np_s, np_r.at[part], (sp, other))

    def hop(step, chosen=(True, True)):
        for way in (0, 1):
            source, there = present(way, step)

            @pl.when(there & chosen[way])
            def _():
                for piece in (0, 1):
                    landed(rows_of(source, piece), nz_s.at[way, step, piece], nz_r.at[way, step, piece])
                    if step < SPLIT - 2:
                        step_on(source, step + 1, way, piece)
                slot = nb.at[source, core]
                send(slot, slot, np_s, np_r.at[source], (sp, other))

    outer = (at_end | (high == 0), at_end | (high == 1))
    across = (inner & (high == 1), inner & (high == 0))

    main = width // 128 * 128
    half_lane = width - main

    def feed(source):
        landed(nb.at[source, other], np_s, np_r.at[source])
        x = nb[source].reshape(rows, nb.shape[-1])
        gate = jnp.dot(x, wgu[:, pl.ds(0, main)], preferred_element_type=jnp.float32)
        up = jnp.dot(x, wgu[:, pl.ds(main, main)], preferred_element_type=jnp.float32)
        hb[source, :, 0:main] = (gate / (1.0 + jnp.exp(-gate)) * up).astype(jnp.bfloat16)
        rest = jnp.dot(x, wgu[:, pl.ds(2 * main, 128)], preferred_element_type=jnp.float32)
        turned = pltpu.roll(rest, half_lane, 1)
        where = lax.broadcasted_iota(jnp.int32, rest.shape, 1)
        tail = jnp.where(where < half_lane, rest / (1.0 + jnp.exp(-rest)) * turned, 0.0)
        hb[source, :, main : main + 128] = tail.astype(jnp.bfloat16)

    edge = jnp.where(inner, nears[0], part)
    order = nears + (part,)
    wide_cols = ranks * cols
    planes = (jnp.where(inner, part, nears[0]), edge, nears[1], nears[2])

    def lanes_of(b):
        return pl.ds(pl.multiple_of(b * wide_cols, wide_cols), wide_cols)

    def pair_sum(b, place):
        landed(drv.at[b, place], dp_s, dp_r.at[b, place])
        return dsb[b, order[place], core].astype(jnp.float32) + drv[b, place].astype(jnp.float32)

    def onward(k, place, first):
        b = planes[k]
        target = order[place]
        way = 1 - (target > part).astype(jnp.int32)
        total = pair_sum(b, place)
        if not first:
            landed(dzb.at[b, way, target], fz_s, fz_r.at[b, way, target])
            total = total + dzb[b, way, target].astype(jnp.float32)
        ds2[b, target] = total.astype(jnp.bfloat16)
        send(
            ds2.at[b, target],
            dzb.at[b, way, target],
            fz_s,
            fz_r.at[b, way, target],
            (sp + ranks * (1 - 2 * way), core),
        )

    def stage(k, place):
        b = planes[k]
        target = order[place]
        block = jnp.dot(hb[target], wdn[:, lanes_of(b)], preferred_element_type=jnp.float32)
        dsb[b, target] = block.astype(jnp.bfloat16).reshape(2, share, wide_cols)
        send(dsb.at[b, target, other], drv.at[b, place], dp_s, dp_r.at[b, place], (sp, other))

    def ends_on(*steps):
        @pl.when(at_end)
        def _():
            for k, place in steps:
                onward(k, place, True)

    def inner_on(*steps):
        @pl.when(inner)
        def _():
            for k, place in steps:
                onward(k, place, False)

    gu_halves(second)
    gu_pass(third)
    hop(0, outer)

    @pl.when(at_end)
    def _():
        down_to(nears[1])
        down_to(nears[2])

    gu_halves(third)

    @pl.when(at_end)
    def _():
        dn_halves(nears[0])

    dn_pass(nears[1])

    @pl.when(inner)
    def _():
        dn_pass(nears[0])

    gu_own.wait()
    landed(gu_at(0, 0, ranks * depth), gh_s, gh_r)
    feed(nears[0])
    locals_[1].wait()
    dn_done(planes[0])
    stage(0, 0)
    hop(0, across)
    feed(part)
    dn_halves(nears[1])

    @pl.when(at_end)
    def _():
        own_downs()
        onward(0, 0, True)

    hop(1)
    dn_pass(nears[2])
    feed(nears[1])
    stage(0, 1)
    dn_halves(edge)
    dn_done(nears[1])
    stage(2, 0)
    ends_on((0, 1),)
    stage(2, 1)
    ends_on((2, 0), (2, 1))
    dn_halves(nears[2])
    hop(2)
    feed(nears[2])
    stage(0, 2)
    stage(2, 2)
    dn_done(edge)
    ends_on((0, 2), (2, 2))
    stage(1, 2)
    stage(1, 1)
    ends_on((1, 2),)
    stage(1, 0)
    inner_on((0, 1), (2, 1))
    dn_done(nears[2])
    stage(3, 2)
    stage(3, 1)
    ends_on((3, 2),)
    stage(3, 0)
    ends_on((1, 1), (3, 1))
    stage(0, 3)
    ends_on((1, 0), (3, 0))
    stage(1, 3)
    stage(2, 3)
    stage(3, 3)
    inner_on((0, 2), (2, 2), (1, 2), (2, 0), (3, 2), (0, 0), (1, 1), (3, 0), (3, 1), (1, 0))

    for k in (2, 0, 3, 1):
        b = planes[k]
        lanes = lanes_of(b)
        acc = pair_sum(b, last)
        base = st[:, lanes].astype(jnp.float32)

        def add(way, value, b=b):
            landed(dzb.at[b, way, part], fz_s, fz_r.at[b, way, part])
            return value + dzb[b, way, part].astype(jnp.float32)

        @pl.when(part == 0)
        def _():
            out_ref[:, lanes] = (base + 0.5 * add(1, acc)).astype(jnp.bfloat16)

        @pl.when(part == last)
        def _():
            out_ref[:, lanes] = (base + 0.5 * add(0, acc)).astype(jnp.bfloat16)

        @pl.when(inner)
        def _():
            out_ref[:, lanes] = (base + 0.5 * add(1, add(0, acc))).astype(jnp.bfloat16)

        pltpu.make_async_copy(out_ref.at[:, lanes], out_hbm.at[:, lanes], local_sem.at[7 + k]).start()

    left(kv_ref.at[pl.ds(0, last)], kvp_s, kvp_r.at[1])
    left(q_ref.at[pl.ds(0, last)], q_s, q_r.at[1])
    left(gu_ref.at[pl.ds(0, last)], gz_s, gz_r.at[0])
    left(down_ref.at[pl.ds(0, last * width)], dz_s, dz_r.at[0])
    left(gu_at(0, 0, 2 * ranks * depth), gx_s, gx_r.at[0, 0])
    left(gu_at(0, 0, ranks * depth), gh_s, gh_r)
    left(wdn.at[pl.ds(0, width), pl.ds(0, 2 * wide_cols)], dx_s, dx_r.at[0, 0])
    left(wdn.at[pl.ds(0, width), pl.ds(0, wide_cols)], dh_s, dh_r.at[0])
    left(prv, pj_s, pj_r)
    left(nb.at[:, 0], np_s, np_r.at[0])
    left(drv, dp_s, dp_r.at[0, 0])
    left(drv.at[pl.ds(0, last)], fz_s, fz_r.at[0, 0, 0])
    for way in (0, 1):
        for step in range(SPLIT - 1):
            source, there = present(way, step - 1)

            @pl.when(ways[way][0] & there)
            def _():
                for piece in (0, 1):
                    left(rows_of(source, piece), nz_s.at[way, step, piece], nz_r.at[way, step, piece])

            if step < 2:

                @pl.when(kv_ways[way] & there)
                def _():
                    for piece in range(ranks):
                        left(kvb.at[source, piece], kvz_s.at[way, step, piece], kvz_r.at[way, step, piece])

    @pl.when(at_end)
    def _():
        left(qb.at[0], qz_s, qz_r.at[0])

    @pl.when(inner)
    def _():
        for piece in range(ranks):
            left(asend.at[1, piece], at_s.at[1, piece], at_r.at[rank])
        for e in flips:
            left(asend.at[0, flip(e)], at_s.at[0, flip(e)], at_r.at[rank])

    for k in range(SPLIT):
        lanes = lanes_of(planes[k])
        pltpu.make_async_copy(out_ref.at[:, lanes], out_hbm.at[:, lanes], local_sem.at[7 + k]).wait()


def run_layer(key, value, query, k_gain, q_gain, gate, up, down, out_weight, resid, gain, ranks):
    rows = query.shape[0]
    share = rows // 2
    model = resid.shape[1]
    width = down.shape[0] // SPLIT
    depth = gate.shape[0]
    head_dim = q_gain.shape[0]
    n_sp = ranks * SPLIT
    quarter = head_dim // 4
    steps = np.tile(np.arange(quarter, dtype=np.float32), 4)
    freq = jnp.asarray((np.float64(10000.0) ** (-steps / quarter)).astype(np.float32))[None, :]
    half = jnp.bfloat16
    dma = pltpu.SemaphoreType.DMA
    padded = -(-width // 128) * 128
    some = model // SPLIT
    anywhere = pl.BlockSpec(memory_space=pl.ANY)
    inside = pl.BlockSpec(memory_space=pltpu.VMEM)
    kv_shape = (SPLIT, rows, 2 * head_dim)
    q_shape = (SPLIT, rows, query.shape[1] // SPLIT)
    return pl.pallas_call(
        functools.partial(layer_kernel, ranks, head_dim),
        out_shape=jax.ShapeDtypeStruct((share, model), half),
        in_specs=[inside] * 6 + [anywhere] * 4 + [inside] * 2,
        out_specs=anywhere,
        scratch_shapes=[
            pltpu.VMEM((share, model), half),
            pltpu.VMEM((SPLIT, ranks, rows, 2 * head_dim), half),
            pltpu.VMEM((2, *q_shape), half),
            pltpu.VMEM((2, *q_shape), half),
            pltpu.VMEM(q_shape, half),
            pltpu.VMEM((n_sp * depth, 2 * width), half),
            pltpu.VMEM((padded, model), half),
            pltpu.VMEM((2, share, model), half),
            pltpu.VMEM((share, model), half),
            pltpu.VMEM((SPLIT, 2, share, model), half),
            pltpu.VMEM((share, model), half),
            pltpu.VMEM((SPLIT, rows, padded), half),
            pltpu.VMEM((SPLIT, SPLIT, 2, share, some), half),
            pltpu.VMEM((SPLIT, SPLIT, share, some), half),
            pltpu.VMEM((SPLIT, SPLIT, share, some), half),
            pltpu.VMEM((SPLIT, 2, SPLIT, share, some), half),
            pltpu.VMEM(kv_shape, half),
            pltpu.VMEM(q_shape, half),
            pltpu.VMEM((SPLIT, depth, 2 * width), half),
            pltpu.VMEM(gate.shape, half),
            pltpu.VMEM(up.shape, half),
            pltpu.VMEM(out_weight.shape, half),
            dma((7 + SPLIT,)),
        ]
        + [dma] * 15
        + [dma((SPLIT,))] * 8
        + [dma((SPLIT, 2))] * 2
        + [dma((SPLIT, SPLIT)), dma((2, SPLIT))]
        + [dma((2, 2, ranks))] * 2
        + [dma((2, SPLIT - 1, 2))] * 2
        + [dma((SPLIT, 2, SPLIT))],
        compiler_params=pltpu.CompilerParams(
            collective_id=0, has_side_effects=True, vmem_limit_bytes=62 * 1024 * 1024
        ),
    )(
        key, value, query, k_gain[None, :], q_gain[None, :], freq, gate, up, down, out_weight, resid, gain[None, :]
    )


def in_kernel(n_sp, n_tp, kv_here, head_dim, width):
    return n_sp == 4 * SPLIT and n_tp == 2 and kv_here == SPLIT and head_dim == 128 and width % 128 == 64


def body(
    resid,
    query,
    key,
    value,
    q_gain,
    k_gain,
    out_weight,
    norm_gain,
    gate_weight,
    up_weight,
    down_weight,
):
    rows = query.shape[0]
    head_dim = q_gain.shape[0]
    heads_here = query.shape[1] // head_dim
    kv_here = key.shape[1] // head_dim
    n_sp = lax.axis_size("sp")
    if not fits(n_sp, kv_here, gate_weight.shape[1]):
        return whole_body(
            resid, query, key, value, q_gain, k_gain, out_weight, norm_gain, gate_weight, up_weight, down_weight
        )
    hidden_part = gate_weight.shape[1] // SPLIT
    ranks = n_sp // SPLIT
    if in_kernel(n_sp, lax.axis_size("tp"), kv_here, head_dim, hidden_part):
        return run_layer(
            key, value, query, k_gain, q_gain, gate_weight, up_weight, down_weight, out_weight, resid, norm_gain, ranks
        )
    tok_groups, hid_groups = groups_of(n_sp)
    ranks = n_sp // SPLIT
    group_size = heads_here // kv_here
    kv_part = kv_here // SPLIT

    def swap(array):
        return lax.all_to_all(array, "sp", 0, 0, axis_index_groups=tok_groups, tiled=True)

    def spread(array, axis):
        return lax.all_gather(array, "sp", axis=axis, axis_index_groups=hid_groups, tiled=True)

    positions = lax.axis_index("sp") * rows + jnp.arange(rows, dtype=jnp.int32)
    q_rot = prepare(query.reshape(rows, heads_here, head_dim), q_gain, positions)
    k_rot = prepare(key.reshape(rows, kv_here, head_dim), k_gain, positions)
    cut = lambda a: a.reshape(a.shape[0], SPLIT, -1).transpose(1, 0, 2).reshape(SPLIT * a.shape[0], -1)
    k_rot, val = cut(k_rot), cut(value)
    pair = swap(jnp.concatenate([k_rot, val], axis=1))
    pair = spread(pair, 0)
    q_mine = swap(cut(q_rot))
    width = kv_part * head_dim
    keys = pair[:, :width].reshape(-1, kv_part, head_dim)
    vals = pair[:, width:].reshape(-1, kv_part, head_dim)
    grouped = q_mine.reshape(SPLIT * rows, kv_part, group_size, head_dim)
    gate_up = spread(swap(jnp.concatenate([cut(gate_weight), cut(up_weight)], axis=1)), 0)
    depth = gate_weight.shape[0]
    gate_up = gate_up.reshape(ranks, SPLIT, depth, -1).transpose(1, 0, 2, 3).reshape(n_sp * depth, -1)
    down_w = swap(down_weight)
    part = down_weight.shape[0] // SPLIT
    down_w = down_w.reshape(SPLIT, part, -1)
    down_w = lax.all_gather(down_w, "sp", axis=1, axis_index_groups=hid_groups)
    down_w = jnp.transpose(down_w, (2, 0, 1, 3)).reshape(part, -1)
    scores = jnp.einsum("qkgd,skd->kgqs", grouped, keys, preferred_element_type=jnp.float32) * head_dim ** (-0.5)
    weights = jnp.exp(scores - jnp.max(scores, axis=-1, keepdims=True))
    totals = jnp.sum(weights, axis=-1)
    accum = jnp.einsum("kgqs,skd->kgqd", weights.astype(jnp.bfloat16), vals, preferred_element_type=jnp.float32)
    attn = jnp.transpose(accum / totals[..., None], (2, 0, 1, 3)).astype(jnp.bfloat16).reshape(SPLIT * rows, -1)
    attn = swap(attn).reshape(SPLIT, rows, -1).transpose(1, 0, 2).reshape(rows, -1)
    return finish(attn, resid, out_weight, norm_gain, gate_up, down_w, tok_groups)


def finish(attn, resid, out_weight, norm_gain, gate_up, down_w, tok_groups):
    rows = resid.shape[0]
    n_tp = lax.axis_size("tp")
    share = rows // n_tp
    my_first = lax.axis_index("tp") * share
    proj = lax.psum_scatter(
        jnp.dot(attn, out_weight, preferred_element_type=jnp.float32).astype(jnp.bfloat16),
        "tp",
        scatter_dimension=0,
        tiled=True,
    ).astype(jnp.float32)
    my_resid = lax.dynamic_slice_in_dim(resid, my_first, share, 0)
    my_stream = (my_resid.astype(jnp.float32) + proj).astype(jnp.bfloat16)
    normed = normalize(my_stream, norm_gain)
    normed = lax.all_gather(normed, "sp", axis=0, axis_index_groups=tok_groups, tiled=False)
    normed = lax.all_gather(normed, "tp", axis=0, tiled=False)
    normed = normed.reshape(n_tp * SPLIT * share, -1)
    both = jnp.dot(normed, gate_up, preferred_element_type=jnp.float32)
    gate, up_part = jnp.split(both, 2, axis=1)
    hidden = (jax.nn.silu(gate) * up_part).astype(jnp.bfloat16)
    down = jnp.dot(hidden, down_w, preferred_element_type=jnp.float32).astype(jnp.bfloat16)
    down = lax.psum_scatter(down, "tp", scatter_dimension=0, tiled=True)
    down = lax.all_to_all(
        down.reshape(SPLIT, share, -1), "sp", 0, 0, axis_index_groups=tok_groups, tiled=True
    )
    down = jnp.sum(down.astype(jnp.float32), axis=0)
    return (my_stream.astype(jnp.float32) + 0.5 * down).astype(jnp.bfloat16)


def solution(mesh):
    placed = (
        P("sp", None),
        P("sp", "tp"),
        P("sp", "tp"),
        P("sp", "tp"),
        P(),
        P(),
        P("tp", None),
        P(),
        P("sp", "tp"),
        P("sp", "tp"),
        P("tp", "sp"),
    )
    return jax.shard_map(
        body, mesh=mesh, in_specs=placed, out_specs=P(("sp", "tp"), None), check_vma=False
    )
```
